512 devices in a mesh: ep: 128 (over z, x, core), tp: 4 (over y).
Axes of the slice: x: 4, y: 4, z: 16, core: 2. Of those that a mesh axis runs over, the one named last changes fastest.
Arguments:
- hidden_in: bfloat16 [2048, 256], P('ep'), may hold values from -24 to 24
- attn_gain: float32 [2048], replicated, may hold values from 0.1 to 1.9
- w_query: bfloat16 [2048, 1536], P('ep', 'tp'), may hold values from -32 to 32
- w_latent: bfloat16 [2048, 512], P('ep'), may hold values from -0.125 to 0.125
- w_rotkey: bfloat16 [32, 2048], replicated, may hold values from -32 to 32
- latent_gain: float32 [512], replicated, may hold values from 0.1 to 1.9
- w_key_up: bfloat16 [512, 1024], P(None, 'tp'), may hold values from -0.75 to 0.75
- w_value_up: bfloat16 [512, 1024], P(None, 'tp'), may hold values from -0.75 to 0.75
- w_attn_out: bfloat16 [2048, 1024], P('ep'), may hold values from -0.1875 to 0.1875
- cache_latent: bfloat16 [256, 1024, 512], P('ep'), may hold values from -6 to 6
- cache_rotkey: bfloat16 [256, 32, 1024], P('ep'), may hold values from -6 to 6
- lengths: int32 [256], P('ep'), may hold values from 128 to 1023
- ffn_gain: float32 [2048], replicated, may hold values from 0.1 to 1.9
- route_ids: int32 [256, 4], replicated, may hold values from 0 to 127, all different within a row; in each aligned block of 256 rows (0 to 255, 256 to 511, ...) at most 16 rows name the same one
- route_scores: float32 [256, 4], replicated, may hold values from 0.05 to 1
- w_exp_gate: bfloat16 [128, 2048, 512], P('ep', None, 'tp'), may hold values from -0.125 to 0.125
- w_exp_up: bfloat16 [128, 2048, 512], P('ep', None, 'tp'), may hold values from -0.125 to 0.125
- w_exp_down: bfloat16 [128, 512, 2048], P('ep', 'tp'), may hold values from -0.25 to 0.25
- w_shared_gate: bfloat16 [2048, 512], P('ep', 'tp'), may hold values from -0.125 to 0.125
- w_shared_up: bfloat16 [2048, 512], P('ep', 'tp'), may hold values from -0.125 to 0.125
- w_shared_out: bfloat16 [2048, 512], P('ep', 'tp'), may hold values from -0.25 to 0.25
Outputs:
- mixed_out: bfloat16 [2048, 256], P('ep', 'tp')
- new_latent: bfloat16 [256, 512], P('ep')
- new_rotkey: bfloat16 [256, 32], P('ep')
The draws below stay inside these ranges and needn't reach their ends.
Inputs may be any that keep to these rules, and one draw needn't show every extreme that they name: `route_ids`: each row names 4 different experts; in the whole batch no expert is named by more than 16 rows, a bound that some block reaches.
All inputs are finite; a program needn't handle non-finite values.
Results may differ from the reference program's by a relative error of at most 0.015.
Values may be sent and summed in bfloat16 or wider, within the bound.
A program may use at most 64 MiB of HBM per device.

```python
import math
import jax
import jax.numpy as jnp
import numpy as np
from jax import lax

D = 2048
HEADS = 16
HEAD_KEY = 64
HEAD_ROT = 32
HEAD_VAL = 64
LATENT = 512
EXPERT_W = 512
SHARED_W = 512
TOP_K = 4
CACHE_LEN = 1024
BATCH = 256
EXPERTS = 128
SLOTS = 16
SPLITS = 4


def rotary_base(key):
    base = jax.random.normal(jax.random.fold_in(key, 11), (HEAD_ROT, D), jnp.float32)
    return jnp.clip(base, -6.0, 6.0) * D ** (-0.5)


def draw_w_rotkey(key, part):
    return rotary_base(key).astype(jnp.bfloat16)


def draw_w_query(key, part):
    per_head = HEAD_KEY + HEAD_ROT
    main = jax.random.normal(jax.random.fold_in(key, 12), (D, HEADS * per_head), jnp.float32)
    main = jnp.clip(main, -6.0, 6.0) * D ** (-0.5)
    return main.astype(jnp.bfloat16)


def place_ends(drawn, key, smallest, high):
    place = [jax.random.randint(jax.random.fold_in(key, axis), (), 0, length) for axis, length in enumerate(drawn.shape)]
    widest = drawn.shape.index(max(drawn.shape))
    next_to = place[:widest] + [(place[widest] + 1) % drawn.shape[widest]] + place[widest + 1:]
    return drawn.at[tuple(place)].set(smallest).at[tuple(next_to)].set(high)


def raised(result, key, source, target, shards_of, factor):
    owner, partner = [(jnp.arange(result.shape[axis_at]) // (result.shape[axis_at] // shards_of)).reshape([-1 if axis == axis_at else 1 for axis in range(result.ndim)]) for axis_at in (source, target)]
    chosen = jax.random.permutation(key, shards_of)[partner]
    strong = (owner == chosen) | (owner == (partner + shards_of // 2) % shards_of)
    return jnp.where(strong, factor * result, result)


def block_scale(rng, shape, cuts, smallest, high):
    gain = 1.0
    for position, parts in cuts:
        heights = jax.random.uniform(jax.random.fold_in(jax.random.fold_in(rng, 6), position), (parts,), jnp.float32, smallest / len(cuts), high / len(cuts))
        gain = gain * jnp.repeat(jnp.exp(heights), shape[position] // parts).reshape((-1,) + (1,) * (len(shape) - 1 - position))
    return gain


def deal_out(key, own, number, rows, count, top, most, slope):
    sequence = jax.random.permutation(key, count)
    crowded, usual = shares(count, rows * top, most, slope, True), shares(count, rows * top, most, slope, False)
    places = jnp.arange(count)

    def named(sizes, turn):
        used = int((sizes > 0).sum())
        fixed = max(1, used // 4)
        shifted = fixed + (places - fixed + turn * (used - fixed)) % max(1, count - fixed)
        return jnp.zeros((count,), jnp.int32).at[sequence[jnp.where(places < fixed, places, shifted)]].set(jnp.asarray(sizes, jnp.int32))

    sizes = jnp.where(number % 4 == 0, named(crowded, number // 4), named(usual, number - number // 4 - 1))
    mixed = jax.random.permutation(jax.random.fold_in(own, 3), count)
    donor, receiver = mixed[0:count // 2 * 2:2], mixed[1:count // 2 * 2:2]
    room = jnp.minimum(sizes[donor] - 1, most - sizes[receiver]) // 2
    room = jnp.where((donor == sequence[0]) | (receiver == sequence[0]) | (sizes[receiver] == 0), 0, jnp.maximum(room, 0))
    shifted = jax.random.randint(jax.random.fold_in(own, 4), (count // 2,), 0, 1 << 20) % (room + 1)
    sizes = sizes.at[donor].add(-shifted).at[receiver].add(shifted)
    items = jnp.searchsorted(jnp.cumsum(sizes), jnp.arange(rows * top), side="right").astype(jnp.int32)
    listing = items.reshape(top, rows).T
    listing = listing[jax.random.permutation(jax.random.fold_in(own, 1), rows)]
    turn = jax.random.randint(jax.random.fold_in(own, 2), (rows, 1), 0, top)
    return jnp.take_along_axis(listing, (jnp.arange(top)[None, :] + turn) % top, axis=1)


def shares(count, total, limit, lean, full):
    portions = [(1 << 20) // math.isqrt(grade ** lean) + 1 for grade in range(1, count + 1)]
    largest = limit if full else min(limit, max(-(-total // count), total * portions[0] // sum(portions)))
    least = 1 if total - largest >= count - 1 else 0
    counts, rest = [largest] + [least] * (count - 1), total - largest - least * (count - 1)
    while rest > 0:
        candidates = [i for i in range(1, count) if counts[i] < largest] or [i for i in range(1, count) if counts[i] < limit]
        pool, remaining = sum([portions[i] for i in candidates]), rest
        for i in candidates:
            extra = min(limit - counts[i], max(1, remaining * portions[i] // pool), rest)
            counts[i] = counts[i] + extra
            rest = rest - extra
    return np.array(counts)


def bell_draw(rng, extent, width, bound, split=(), held_as=jnp.bfloat16):
    loudness = block_scale(rng, extent, split, -0.22, 0.18) if split else 1.0
    array = jax.random.normal(rng, extent, jnp.float32) * width * loudness
    return jnp.minimum(jnp.maximum(array, -bound), bound).astype(held_as)


def gaussian_with(stream_key, dims, scale, bound, pieces, heavy, kind=jnp.bfloat16):
    array = scale * jax.random.normal(stream_key, dims, jnp.float32)
    if pieces:
        array = array * block_scale(stream_key, dims, pieces, -0.22, 0.18)
    return jnp.clip(raised(array, jax.random.fold_in(stream_key, 3), *heavy), -bound, bound).astype(kind)


def setup_inputs(seed: int = 0) -> dict:
    key_of = jax.random.split(jax.random.key(seed), 22)
    hidden_in = gaussian_with(key_of[0], (D, BATCH), 1.0, 24.0, ((0, 128),), (0, 1, 128, 5.5))
    attn_gain = jnp.clip(1.0 + 0.18 * jax.random.normal(key_of[1], (D,), jnp.float32), 0.1, 1.9)
    w_query = draw_w_query(jax.random.fold_in(key_of[21], 71), 0)
    w_latent = bell_draw(key_of[3], (D, LATENT), D ** -0.5, 0.125, ((0, 128),))
    w_rotkey = draw_w_rotkey(jax.random.fold_in(key_of[21], 71), 0)
    latent_gain = jnp.clip(1.0 + 0.18 * jax.random.normal(key_of[5], (LATENT,), jnp.float32), 0.1, 1.9)
    w_key_up = bell_draw(key_of[6], (LATENT, HEADS * HEAD_KEY), HEAD_KEY ** -0.5, 0.75, ((1, 4),))
    w_value_up = bell_draw(key_of[7], (LATENT, HEADS * HEAD_VAL), HEAD_VAL ** -0.5, 0.75, ((1, 4),))
    w_attn_out = bell_draw(key_of[8], (D, HEADS * HEAD_VAL), (HEADS * HEAD_VAL) ** -0.5, 0.1875, ((0, 128),))
    cache_latent = bell_draw(key_of[9], (BATCH, CACHE_LEN, LATENT), 1.0, 6.0, ((0, 128),))
    cache_rotkey = bell_draw(key_of[10], (BATCH, HEAD_ROT, CACHE_LEN), 1.0, 6.0, ((0, 128),))
    lengths = place_ends(jax.random.randint(key_of[11], (BATCH,), CACHE_LEN // 8, CACHE_LEN), jax.random.fold_in(key_of[11], 1), CACHE_LEN // 8, CACHE_LEN - 1).astype(jnp.int32)
    ffn_gain = jnp.clip(1.0 + 0.18 * jax.random.normal(key_of[12], (D,), jnp.float32), 0.1, 1.9)
    route_ids_keys = jax.random.split(jax.random.fold_in(key_of[13], 1), BATCH // BATCH)
    route_ids_turns = jax.random.permutation(jax.random.fold_in(key_of[13], 3), BATCH // BATCH)
    route_ids = jax.vmap(lambda own, number: deal_out(jax.random.fold_in(key_of[13], 2), own, number, BATCH, EXPERTS, TOP_K, SLOTS, 2))(route_ids_keys, route_ids_turns).reshape((BATCH, TOP_K))
    route_scores = jnp.clip(jax.random.uniform(key_of[14], (BATCH, TOP_K), jnp.float32, 0.05, 1.0), 0.05, 1.0)
    w_exp_gate = bell_draw(key_of[15], (EXPERTS, D, EXPERT_W), D ** -0.5, 0.125, ((0, 128), (2, 4)))
    w_exp_up = bell_draw(key_of[16], (EXPERTS, D, EXPERT_W), D ** -0.5, 0.125, ((0, 128), (2, 4)))
    w_exp_down = bell_draw(key_of[17], (EXPERTS, EXPERT_W, D), EXPERT_W ** -0.5, 0.25, ((0, 128), (1, 4)))
    w_shared_gate = bell_draw(key_of[18], (D, SHARED_W), D ** -0.5, 0.125, ((0, 128), (1, 4)))
    w_shared_up = bell_draw(key_of[19], (D, SHARED_W), D ** -0.5, 0.125, ((0, 128), (1, 4)))
    w_shared_out = bell_draw(key_of[20], (D, SHARED_W), SHARED_W ** -0.5, 0.25, ((0, 128), (1, 4)))
    return dict(hidden_in=hidden_in, attn_gain=attn_gain, w_query=w_query, w_latent=w_latent, w_rotkey=w_rotkey, latent_gain=latent_gain, w_key_up=w_key_up, w_value_up=w_value_up, w_attn_out=w_attn_out, cache_latent=cache_latent, cache_rotkey=cache_rotkey, lengths=lengths, ffn_gain=ffn_gain, route_ids=route_ids, route_scores=route_scores, w_exp_gate=w_exp_gate, w_exp_up=w_exp_up, w_exp_down=w_exp_down, w_shared_gate=w_shared_gate, w_shared_up=w_shared_up, w_shared_out=w_shared_out)


EPSILON = 1e-06
THETA_BASE = 10000.0
ROUTED_SCALE = 2.5
HIGHEST = lax.Precision.HIGHEST

def rotate(lower, upper, angles):
    cosine_part = jnp.cos(angles)
    sine_part = jnp.sin(angles)
    return (lower * cosine_part - upper * sine_part, lower * sine_part + upper * cosine_part)

def rounded(values):
    return lax.optimization_barrier(values.astype(jnp.bfloat16)).astype(jnp.float32)

def slot_tables(route_ids):
    flat_ids = route_ids.reshape(-1).astype(jnp.int32)
    hit_table = (flat_ids[:, None] == jnp.arange(EXPERTS, dtype=jnp.int32)[None, :]).astype(jnp.int32)
    earlier = (jnp.cumsum(hit_table, axis=0) - hit_table).astype(jnp.int32)
    slot_rank = lax.optimization_barrier(jnp.sum(earlier * hit_table, axis=1)).astype(jnp.int32)
    slot_of = (flat_ids * SLOTS + slot_rank).astype(jnp.int32)
    owners = (jnp.arange(BATCH * TOP_K, dtype=jnp.int32) // TOP_K).astype(jnp.int32)
    slot_row = jnp.full((EXPERTS * SLOTS,), BATCH, jnp.int32).at[slot_of].set(owners)
    return (slot_of, slot_row)

def reference(hidden_in, attn_gain, w_query, w_latent, w_rotkey, latent_gain, w_key_up, w_value_up, w_attn_out, cache_latent, cache_rotkey, lengths, ffn_gain, route_ids, route_scores, w_exp_gate, w_exp_up, w_exp_down, w_shared_gate, w_shared_up, w_shared_out):
    rows_in = hidden_in.astype(jnp.float32).T
    scaled_in = (rows_in * attn_gain[None, :]).astype(jnp.bfloat16)
    in_scale = lax.rsqrt(lax.optimization_barrier(jnp.mean(rows_in * rows_in, axis=1, keepdims=True)) + EPSILON)
    query = (in_scale * jnp.dot(scaled_in, w_query, preferred_element_type=jnp.float32)).astype(jnp.bfloat16)
    latent_raw = (in_scale * jnp.dot(scaled_in, w_latent, preferred_element_type=jnp.float32)).astype(jnp.bfloat16)
    new_rotkey = (in_scale * jnp.dot(scaled_in, w_rotkey.T, preferred_element_type=jnp.float32)).astype(jnp.bfloat16)
    raw_values = latent_raw.astype(jnp.float32)
    new_latent = (raw_values * lax.rsqrt(lax.optimization_barrier(jnp.mean(raw_values * raw_values, axis=1, keepdims=True)) + EPSILON) * latent_gain[None, :]).astype(jnp.bfloat16)
    per_head = HEAD_KEY + HEAD_ROT
    query_heads = query.astype(jnp.float32).reshape(BATCH, HEADS, per_head)
    key_up = w_key_up.astype(jnp.float32).reshape(LATENT, HEADS, HEAD_KEY)
    absorbed = jnp.einsum('bhn,chn->bhc', query_heads[:, :, :HEAD_KEY], key_up).astype(jnp.bfloat16)
    half_rot = HEAD_ROT // 2
    frequency = THETA_BASE ** (-jnp.arange(half_rot, dtype=jnp.float32) / half_rot)
    new_angles = lengths.astype(jnp.float32)[:, None] * frequency[None, :]
    query_rot = query_heads[:, :, HEAD_KEY:]
    query_low, query_high = rotate(query_rot[..., :half_rot], query_rot[..., half_rot:], new_angles[:, None, :])
    own_key = new_rotkey.astype(jnp.float32)
    own_low, own_high = rotate(own_key[:, :half_rot], own_key[:, half_rot:], new_angles)
    cache_angles = frequency[:, None] * jnp.arange(CACHE_LEN, dtype=jnp.float32)[None, :]
    value_up = w_value_up.astype(jnp.float32).reshape(LATENT, HEADS, HEAD_VAL)
    score_scale = per_head ** (-0.5)
    positions = jnp.arange(CACHE_LEN, dtype=jnp.int32)

    def one_sequence(items):
        latent_rows, rot_rows, absorb, low_query, high_query, low_own, high_own, fresh, length = items
        latent_values = latent_rows.astype(jnp.float32)
        rot_values = rot_rows.astype(jnp.float32)
        key_low, key_high = rotate(rot_values[:half_rot], rot_values[half_rot:], cache_angles)
        absorb_values = absorb.astype(jnp.float32)
        fresh_values = fresh.astype(jnp.float32)
        latent_score = jnp.dot(absorb_values, latent_values.T, precision=HIGHEST)
        rot_score = jnp.dot(low_query, key_low, precision=HIGHEST) + jnp.dot(high_query, key_high, precision=HIGHEST)
        cache_score = jnp.where((positions < length)[None, :], score_scale * (latent_score + rot_score), -1e+30)
        own_score = score_scale * (jnp.dot(absorb_values, fresh_values, precision=HIGHEST) + lax.optimization_barrier(jnp.sum(low_query * low_own[None, :] + high_query * high_own[None, :], axis=1)))
        top_score = jnp.maximum(lax.optimization_barrier(jnp.max(cache_score, axis=1)), own_score)
        cache_weight = jnp.exp(cache_score - top_score[:, None])
        own_weight = jnp.exp(own_score - top_score)
        denominator = lax.optimization_barrier(jnp.sum(cache_weight, axis=1)) + own_weight
        cache_prob = rounded(cache_weight / denominator[:, None])
        own_prob = rounded(own_weight / denominator)
        context = (jnp.dot(cache_prob, latent_values, precision=HIGHEST) + own_prob[:, None] * fresh_values[None, :]).astype(jnp.bfloat16)
        heads = jnp.einsum('hc,chv->hv', context.astype(jnp.float32), value_up)
        return heads.astype(jnp.bfloat16).reshape(HEADS * HEAD_VAL)
    heads_out = lax.map(one_sequence, (cache_latent, cache_rotkey, absorbed, query_low, query_high, own_low, own_high, new_latent, lengths))
    attn = jnp.dot(heads_out, w_attn_out.T, preferred_element_type=jnp.float32).astype(jnp.bfloat16)
    mid = (rows_in + attn.astype(jnp.float32)).astype(jnp.bfloat16)
    mid_values = mid.astype(jnp.float32)
    mid_scale = lax.rsqrt(lax.optimization_barrier(jnp.mean(mid_values * mid_values, axis=1)) + EPSILON)
    ffn_in = (mid_values * ffn_gain[None, :]).astype(jnp.bfloat16)
    shared_gate = mid_scale[:, None] * jnp.dot(ffn_in, w_shared_gate, preferred_element_type=jnp.float32)
    shared_up = mid_scale[:, None] * jnp.dot(ffn_in, w_shared_up, preferred_element_type=jnp.float32)
    shared_act = (jax.nn.silu(shared_gate) * shared_up).astype(jnp.bfloat16)
    slot_of, slot_row = slot_tables(route_ids)
    ffn_pad = jnp.concatenate([ffn_in, jnp.zeros((1, D), jnp.bfloat16)], axis=0)
    scale_pad = jnp.concatenate([mid_scale, jnp.ones((1,), jnp.float32)])
    block_width = EXPERT_W // SPLITS

    def one_expert(items):
        gate_weight, up_weight, down_weight, slot_rows = items
        expert_in = jnp.take(ffn_pad, slot_rows, axis=0)
        row_scale = jnp.take(scale_pad, slot_rows)[:, None]
        gate_value = row_scale * jnp.dot(expert_in, gate_weight, preferred_element_type=jnp.float32)
        up_value = row_scale * jnp.dot(expert_in, up_weight, preferred_element_type=jnp.float32)
        activation = (jax.nn.silu(gate_value) * up_value).astype(jnp.bfloat16)
        partials = jnp.einsum('stj,tjd->tsd', activation.astype(jnp.float32).reshape(SLOTS, SPLITS, block_width), down_weight.astype(jnp.float32).reshape(SPLITS, block_width, D))
        return partials.astype(jnp.bfloat16)
    expert_parts = lax.map(one_expert, (w_exp_gate, w_exp_up, w_exp_down, slot_row.reshape(EXPERTS, SLOTS)))
    flat_parts = jnp.transpose(expert_parts, (1, 0, 2, 3)).reshape(SPLITS, EXPERTS * SLOTS, D)
    picked = jnp.take(flat_parts, slot_of, axis=1).reshape(SPLITS, BATCH, TOP_K, D).astype(jnp.float32)
    route_weight = ROUTED_SCALE * route_scores / lax.optimization_barrier(jnp.sum(route_scores, axis=1, keepdims=True))
    routed = jnp.einsum('tbkd,bk->tbd', picked, route_weight, precision=HIGHEST)
    shared_blocks = shared_act.astype(jnp.float32).reshape(BATCH, SPLITS, SHARED_W // SPLITS)
    out_blocks = w_shared_out.astype(jnp.float32).reshape(D, SPLITS, SHARED_W // SPLITS)
    shared = jnp.einsum('btj,dtj->tbd', shared_blocks, out_blocks)
    block_total = rounded(shared + routed)
    mixed_out = (mid_values + lax.optimization_barrier(jnp.sum(block_total, axis=0))).astype(jnp.bfloat16)
    return (mixed_out.T, new_latent, new_rotkey)
```

```python
import functools

import jax
import jax.numpy as jnp
import numpy as np
from jax import lax
from jax.experimental import pallas as pl
from jax.experimental.pallas import tpu as pltpu
from jax.sharding import Mesh
from jax.sharding import PartitionSpec as P

MESH = pl.DeviceIdType.MESH
F32 = jnp.float32
BF16 = jnp.bfloat16
HIGHEST = lax.Precision.HIGHEST
NN = (((1,), (0,)), ((), ()))
NT = (((1,), (1,)), ((), ()))
TN = (((0,), (0,)), ((), ()))

LOCAL_HEADS = 4
HEAD_KEY = 64
HEAD_ROT = 32
HEAD_VAL = 64
PER_HEAD = HEAD_KEY + HEAD_ROT
LATENT = 512
CACHE = 1024
HIDDEN = 128
SLOTS = 16
FEATS = 16
SEQS = 2
EPSILON = 1e-06
THETA_BASE = 10000.0
ROUTED_SCALE = 2.5
QW = LOCAL_HEADS * PER_HEAD
HV = LOCAL_HEADS * HEAD_VAL


def dot(a, b, dims=NN, precision=None):
    return lax.dot_general(a, b, dims, precision=precision, preferred_element_type=F32)


def iota(shape, axis):
    return lax.broadcasted_iota(jnp.int32, shape, axis)


def ones_where(mask, dtype=BF16):
    return jnp.where(mask, 1.0, 0.0).astype(dtype)


def rounded(v):
    return v.astype(BF16).astype(F32)


def log2(n):
    return n.bit_length() - 1


def kernel(nz, nx, nc, nt, *refs):
    (
        hidden, attn_gain, w_query, w_latent, w_rotkey, latent_gain, w_key_up, w_value_up, w_attn_out, cache_latent, cache_rotkey,
        lengths, ffn_gain, route_ids, route_scores, w_exp_gate, w_exp_up, w_exp_down, w_shared_gate, w_shared_up, w_shared_out,
        trig, freq,
        o_mixed, o_latent, o_rotkey,
        crit, back, rotw, again, fgain, lgain, fr, keyup, valup, cache, crot, lens, ids, scores, wgu, wd, trg,
        za_s, za_r, yb, zd, ye, midx, zf_s, zf_r, zg_s, zg_r, zh_s, zh_r, zs, xr_s, xr_r, yo_s, yo_r,
        ka, krot, sel_p, wt, ht, h32, s32, pall, shf,
        lsem, ssem, rsem,
    ) = refs
    ncol = nx * nc
    pf = FEATS * ncol
    rows = SEQS * nz
    batch = rows * ncol
    width = pf * nz
    lq = LATENT // nt
    nslot = nz * SLOTS
    ob = batch // nt
    hl = 2 * ob
    z, x, c, y = (lax.axis_index(a) for a in ("z", "x", "c", "y"))
    col = x * nc + c

    z_order = sorted(range(1, nz), key=lambda d: -min(d, nz - d))
    z_peers = [(lax.rem(z + d, nz),) for d in z_order]

    def zdev(p):
        return {"z": p}

    def xdev(p):
        return {"x": lax.div(p, nc), "c": lax.rem(p, nc)}

    def ydev(p):
        return {"y": p}

    x_peers = [lax.rem(col + d, ncol) for d in range(1, ncol)]
    y_peers = [lax.rem(y + d, nt) for d in range(1, nt)]
    z_peers = [p for (p,) in z_peers]

    bar = pltpu.get_barrier_semaphore()
    for p in z_peers:
        pl.semaphore_signal(bar, inc=1, device_id=zdev(p), device_id_type=MESH)
    for p in x_peers:
        pl.semaphore_signal(bar, inc=1, device_id=xdev(p), device_id_type=MESH)
    for p in y_peers:
        pl.semaphore_signal(bar, inc=1, device_id=ydev(p), device_id_type=MESH)

    def loads(sem, pairs):
        copies = [pltpu.make_async_copy(s, d, lsem.at[sem + i]) for i, (s, d) in enumerate(pairs)]
        for cp in copies:
            cp.start()
        return copies

    def done(copies):
        for cp in copies:
            cp.wait()

    own_lq = pl.ds(pl.multiple_of(y * lq, lq), lq)
    own_hv = pl.ds(pl.multiple_of(y * HV, HV), HV)
    own_pf = pl.ds(pl.multiple_of(z * pf, pf), pf)
    half = HEAD_ROT // 2
    l_crit = loads(0, [
        (w_query, crit.at[col, :, pl.ds(0, QW)]),
        (w_latent.at[:, own_lq], crit.at[col, :, pl.ds(QW, lq)]),
        (hidden, crit.at[col, :, pl.ds(QW + lq, batch)]),
    ])
    l_rot = loads(3, [
        (w_rotkey.at[:, own_pf], rotw.at[pl.ds(0, HEAD_ROT)]),
        (w_rotkey.at[pl.ds(half, half), own_pf], rotw.at[pl.ds(64, half)]),
        (w_rotkey.at[pl.ds(0, half), own_pf], rotw.at[pl.ds(64 + half, half)]),
        (attn_gain, again),
        (ffn_gain, fgain),
        (latent_gain, lgain),
        (freq, fr),
        (lengths, lens),
    ])
    l_back = loads(11, [
        (w_attn_out.at[:, own_hv], back.at[col, :, pl.ds(0, HV)]),
        (w_shared_gate, back.at[col, :, pl.ds(HV, HIDDEN)]),
        (w_shared_up, back.at[col, :, pl.ds(HV + HIDDEN, HIDDEN)]),
        (w_shared_out, back.at[col, :, pl.ds(HV + 2 * HIDDEN, HIDDEN)]),
    ])
    l_tab = loads(15, [
        (w_key_up, keyup), (cache_rotkey, crot), (trig, trg), (route_ids, ids), (route_scores, scores),
    ])
    l_att = loads(20, [(cache_latent, cache), (w_value_up, valup)])
    l_exp = loads(22, [
        (w_exp_gate.at[0], wgu.at[:, pl.ds(0, HIDDEN)]),
        (w_exp_up.at[0], wgu.at[:, pl.ds(HIDDEN, HIDDEN)]),
        (w_exp_down.at[0], wd),
    ])

    def send(src, dst, k, dev):
        cp = pltpu.make_async_remote_copy(
            src_ref=src, dst_ref=dst, send_sem=ssem.at[k], recv_sem=rsem.at[k], device_id=dev, device_id_type=MESH
        )
        cp.start()

    def arrived(buf, n, k):
        part = buf.at[pl.ds(0, n)]
        pltpu.make_async_copy(part, part, rsem.at[k]).wait()

    pending = []

    def sent(buf, n, k):
        pending.append((buf, n, k))

    done(l_crit)
    pl.semaphore_wait(bar, len(z_peers) + len(x_peers) + len(y_peers))
    for p in x_peers:
        send(crit.at[col], crit.at[col], 0, xdev(p))
    sent(crit, ncol - 1, 0)
    done(l_back)
    for p in x_peers:
        send(back.at[col], back.at[col], 1, xdev(p))
    sent(back, ncol - 1, 1)

    done(l_rot)
    done(l_tab)
    cos_t, sin_t = trg[0], trg[1]
    for s in range(SEQS):
        low = crot[s, pl.ds(0, half), :].astype(F32)
        high = crot[s, pl.ds(half, half), :].astype(F32)
        krot[s, pl.ds(0, half), :] = low * cos_t - high * sin_t
        krot[s, pl.ds(half, half), :] = low * sin_t + high * cos_t
    spread_r = iota((LOCAL_HEADS * HEAD_KEY, QW), 0)
    spread = ones_where(iota((LOCAL_HEADS * HEAD_KEY, QW), 1) == spread_r + HEAD_ROT * (spread_r >> log2(HEAD_KEY)))
    ka[pl.ds(0, LATENT), :] = dot(keyup[...], spread).astype(BF16)
    lane_q = iota((256, QW), 1)
    head_q = ones_where(lane_q >= PER_HEAD, jnp.int32)
    for h in range(2, LOCAL_HEADS):
        head_q = head_q + ones_where(lane_q >= h * PER_HEAD, jnp.int32)
    within = lane_q - PER_HEAD * head_q - HEAD_KEY
    row_q = iota((256, QW), 0)
    want = jnp.where(row_q < 128, row_q, (row_q - 128) ^ half)
    limit = jnp.where(row_q < 128, row_q, row_q - 128)
    ka[pl.ds(LATENT, 256), :] = ones_where((within == want) & (limit < HEAD_ROT))
    rot_rows = iota((128, pf), 0)
    rot_w = jnp.where((rot_rows & 63) < HEAD_ROT, rotw[...].astype(F32), 0.0).astype(BF16)

    arrived(crit, ncol - 1, 0)
    r_i, b_i = iota((rows, batch), 0), iota((rows, batch), 1)
    sel_a = ones_where(b_i == (r_i >> 1) * (ncol * SEQS) + col * SEQS + (r_i & 1))
    hid = crit[:, :, pl.ds(QW + lq, batch)].reshape(pf, batch)
    h_t = dot(sel_a, hid, NT)
    ht[...] = h_t
    scaled = (h_t * again[pl.ds(z, 1), :]).astype(BF16)
    main = dot(scaled, crit[:, :, pl.ds(0, QW + lq)].reshape(pf, QW + lq))
    rot = dot(scaled, rot_w, NT)
    square = jnp.sum(h_t * h_t, axis=1, keepdims=True)
    rot = jnp.where(iota((rows, 128), 1) == HEAD_ROT, square, rot)
    aw = QW + lq + 128
    pall[:, pl.ds(0, QW + lq)] = main
    pall[:, pl.ds(QW + lq, 128)] = rot
    for i in range(nz):
        za_s[i] = pall[pl.ds(SEQS * i, SEQS), :]
    for p in z_peers:
        send(za_s.at[p], za_r.at[z], 2, zdev(p))
    sent(za_s, nz - 1, 2)
    za_r[pl.ds(z, 1)] = za_s[pl.ds(z, 1)]

    rs = scores[...]
    rw = ROUTED_SCALE * rs / jnp.sum(rs, axis=1, keepdims=True)
    idv = ids[...]
    target = iota((batch, 128), 1) * ncol + col
    hit = jnp.zeros((batch, 128), F32)
    wgt = jnp.zeros((batch, 128), F32)
    for k in range(4):
        same = idv[:, k : k + 1] == target
        hit = jnp.where(same, 1.0, hit)
        wgt = jnp.where(same, rw[:, k : k + 1], wgt)
    before = ones_where(iota((batch, batch), 1) < iota((batch, batch), 0))
    rank = dot(before, hit.astype(BF16))
    val = jnp.where(hit > 0.0, rank, -1.0).astype(BF16)
    expand = ones_where(iota((nslot, 128), 1) == (iota((nslot, 128), 0) >> log2(SLOTS)))
    slot_i = (iota((nslot, batch), 0) & (SLOTS - 1)).astype(F32)
    in_slot = dot(expand, val, NT) == slot_i
    w_hi = wgt.astype(BF16)
    w_lo = (wgt - w_hi.astype(F32)).astype(BF16)
    wt[pl.ds(0, nslot), :] = jnp.where(in_slot, dot(expand, w_hi, NT), 0.0).astype(BF16)
    wt[pl.ds(nslot, nslot), :] = jnp.where(in_slot, dot(expand, w_lo, NT), 0.0).astype(BF16)

    def natural(p):
        return ((p >> 1) & (nz - 1)) * (ncol * SEQS) + (p >> log2(rows)) * SEQS + (p & 1)

    perm = ones_where(iota((batch, batch), 0) == natural(iota((batch, batch), 1)))
    sel_p[...] = dot(ones_where(in_slot), perm).astype(BF16)

    arrived(za_r, nz - 1, 2)
    tot = za_r[0]
    for i in range(1, nz):
        tot = tot + za_r[i]
    lane2 = iota((SEQS, 128), 1)
    tail = tot[:, QW + lq : aw]
    sq = jnp.sum(jnp.where(lane2 == HEAD_ROT, tail, 0.0), axis=1, keepdims=True)
    scale = lax.rsqrt(sq / width + EPSILON)
    yb[pl.ds(y, 1)] = rounded(tot[:, QW : QW + lq] * scale).reshape(1, SEQS, lq)
    for p in y_peers:
        send(yb.at[y], yb.at[y], 3, ydev(p))
    sent(yb, nt - 1, 3)
    q = rounded(tot[:, :QW] * scale)
    nrows = SEQS * LOCAL_HEADS
    r8 = iota((nrows, 128), 0)
    first8 = r8 < LOCAL_HEADS

    def per_row(v):
        top = iota((nrows, v.shape[1]), 0) < LOCAL_HEADS
        return jnp.where(top, v[0:1, :], v[1:2, :])

    lane_8 = iota((nrows, QW), 1)
    first = (iota((nrows, QW), 0) & (LOCAL_HEADS - 1)) * PER_HEAD
    q8 = jnp.where((lane_8 >= first) & (lane_8 < first + PER_HEAD), per_row(q), 0.0).astype(BF16)
    qa = dot(q8, ka[...], NT)
    absorbed = qa[:, :LATENT].astype(BF16)
    len8 = jnp.where(first8, lens[0], lens[1])
    angle = len8.astype(F32) * fr[...]
    cos8 = jnp.cos(angle)
    lane8 = iota((nrows, 128), 1)
    sin8 = jnp.where((lane8 & half) == 0, -jnp.sin(angle), jnp.sin(angle))
    q_rot = qa[:, LATENT : LATENT + 128] * cos8 + qa[:, LATENT + 128 : LATENT + 256] * sin8

    done(l_att)
    q32 = q_rot[:, :HEAD_ROT]
    per_seq = [dot(absorbed, cache[s], NT) + dot(q32, krot[s], NN, HIGHEST) for s in range(SEQS)]
    top_rows = iota((nrows, CACHE), 0) < LOCAL_HEADS
    score_scale = PER_HEAD**-0.5
    live = iota((nrows, CACHE), 1) < jnp.where(top_rows, lens[0], lens[1])
    cache_score = jnp.where(live, score_scale * jnp.where(top_rows, per_seq[0], per_seq[1]), -1e30)
    best = jnp.max(cache_score, axis=1, keepdims=True)

    new_rot = rounded(tail * scale)
    o_rotkey[...] = new_rot[:, :HEAD_ROT].astype(BF16)
    new_swap = pltpu.roll(new_rot, 64, 1)
    own_rot = jnp.where(lane8 < HEAD_ROT, per_row(new_rot) * cos8 + per_row(new_swap) * sin8, 0.0)

    arrived(yb, nt - 1, 3)
    raw = jnp.concatenate([yb[i] for i in range(nt)], axis=1)
    new_latent = (
        raw * lax.rsqrt(jnp.mean(raw * raw, axis=1, keepdims=True) + EPSILON) * lgain[...]
    ).astype(BF16)
    o_latent[...] = new_latent
    lat8 = per_row(new_latent.astype(F32))
    own_score = score_scale * (
        jnp.sum(absorbed.astype(F32) * lat8, axis=1, keepdims=True)
        + jnp.sum(q_rot * own_rot, axis=1, keepdims=True)
    )
    top_score = jnp.maximum(best, own_score)
    cache_weight = jnp.exp(cache_score - top_score)
    own_weight = jnp.exp(own_score - top_score)
    denominator = jnp.sum(cache_weight, axis=1, keepdims=True) + own_weight
    prob = (cache_weight / denominator).astype(BF16)
    own_prob = rounded(own_weight / denominator)
    ctx = [dot(prob, cache[s]) for s in range(SEQS)]
    top_rows = iota((nrows, LATENT), 0) < LOCAL_HEADS
    context = jnp.where(top_rows, ctx[0], ctx[1]) + own_prob * lat8
    ho = dot(context.astype(BF16), valup[...])
    r_h = iota((nrows, HV), 0)
    ho = jnp.where((iota((nrows, HV), 1) >> log2(HEAD_VAL)) == (r_h & (LOCAL_HEADS - 1)), ho, 0.0)
    h0 = jnp.sum(jnp.where(r_h < LOCAL_HEADS, ho, 0.0), axis=0, keepdims=True)
    h1 = jnp.sum(jnp.where(r_h < LOCAL_HEADS, 0.0, ho), axis=0, keepdims=True)
    heads = rounded(jnp.where(iota((SEQS, HV), 0) == 0, h0, h1))
    zd[pl.ds(z, 1)] = heads.reshape(1, SEQS, HV)
    for p in z_peers:
        send(zd.at[z], zd.at[z], 4, zdev(p))
    sent(zd, nz - 1, 4)

    arrived(back, ncol - 1, 1)
    arrived(zd, nz - 1, 4)
    for i in range(nz):
        h32[pl.ds(SEQS * i, SEQS), :] = zd[i]
    part = dot(h32[...].astype(BF16), back[:, :, pl.ds(0, HV)].reshape(pf, HV), NT)
    ye[pl.ds(y, 1)] = part.reshape(1, rows, pf)
    for p in y_peers:
        send(ye.at[y], ye.at[y], 5, ydev(p))
    sent(ye, nt - 1, 5)
    arrived(ye, nt - 1, 5)
    attn = ye[0]
    for i in range(1, nt):
        attn = attn + ye[i]
    mid = (ht[...] + rounded(attn)).astype(BF16)
    midx[pl.ds(col, 1)] = mid.reshape(1, rows, pf)
    for p in x_peers:
        send(midx.at[col], midx.at[col], 6, xdev(p))
    sent(midx, ncol - 1, 6)
    mid_v = mid.astype(F32)
    ffn = (mid_v * fgain[pl.ds(z, 1), :]).astype(BF16)
    shf[:, pl.ds(0, 2 * HIDDEN)] = dot(ffn, back[:, :, pl.ds(HV, 2 * HIDDEN)].reshape(pf, 2 * HIDDEN))
    shf[:, pl.ds(2 * HIDDEN, 128)] = jnp.broadcast_to(jnp.sum(mid_v * mid_v, axis=1, keepdims=True), (rows, 128))
    for i in range(nz):
        zf_s[i] = shf[pl.ds(SEQS * i, SEQS), :]
    for p in z_peers:
        send(zf_s.at[p], zf_r.at[z], 7, zdev(p))
    sent(zf_s, nz - 1, 7)
    zf_r[pl.ds(z, 1)] = zf_s[pl.ds(z, 1)]

    arrived(midx, ncol - 1, 6)
    mid_all = midx[...].reshape(batch, pf)
    zg_s[...] = dot(sel_p[...], mid_all).astype(BF16).reshape(nz, SLOTS, pf)
    for p in z_peers:
        send(zg_s.at[p], zg_r.at[z], 8, zdev(p))
    sent(zg_s, nz - 1, 8)
    zg_r[pl.ds(z, 1)] = zg_s[pl.ds(z, 1)]
    own_f = ones_where(iota((FEATS, pf), 1) == iota((FEATS, pf), 0) + col * FEATS)
    mid_t = dot(own_f, mid_all, NT).astype(BF16)
    to_half = ones_where(natural(iota((batch, hl), 0)) == iota((batch, hl), 1) + (y >> 1) * hl)
    mid_own = dot(mid_t, to_half)

    arrived(zf_r, nz - 1, 7)
    tot = zf_r[0]
    for i in range(1, nz):
        tot = tot + zf_r[i]
    scale = lax.rsqrt(tot[:, 2 * HIDDEN : 2 * HIDDEN + 1] / width + EPSILON)
    gate = scale * tot[:, :HIDDEN]
    act = rounded(gate / (1.0 + jnp.exp(-gate)) * (scale * tot[:, HIDDEN : 2 * HIDDEN]))
    zs[pl.ds(z, 1)] = act.reshape(1, SEQS, HIDDEN)
    for p in z_peers:
        send(zs.at[z], zs.at[z], 9, zdev(p))
    sent(zs, nz - 1, 9)

    done(l_exp)
    arrived(zg_r, nz - 1, 8)
    pieces = []
    sq = jnp.zeros((SLOTS, 1), F32)
    for i in range(nz):
        v = zg_r[i].astype(F32)
        sq = sq + jnp.sum(v * v, axis=1, keepdims=True)
        pieces.append((v * fgain[pl.ds(i, 1), :]).astype(BF16))
    gu = dot(jnp.concatenate(pieces, axis=1), wgu[...])
    scale = lax.rsqrt(sq / width + EPSILON)
    gate = scale * gu[:, :HIDDEN]
    act = (gate / (1.0 + jnp.exp(-gate)) * (scale * gu[:, HIDDEN:])).astype(BF16)
    out = dot(act, wd[...])
    for i in range(nz):
        zh_s[i] = out[:, pf * i : pf * (i + 1)].astype(BF16)
    for p in z_peers:
        send(zh_s.at[p], zh_r.at[z], 10, zdev(p))
    sent(zh_s, nz - 1, 10)
    zh_r[pl.ds(z, 1)] = zh_s[pl.ds(z, 1)]

    arrived(zs, nz - 1, 9)
    for i in range(nz):
        s32[pl.ds(SEQS * i, SEQS), :] = zs[i]
    place = ones_where(
        iota((batch, rows), 0) == (iota((batch, rows), 1) >> 1) * (ncol * SEQS) + col * SEQS + (iota((batch, rows), 1) & 1)
    )
    spread_act = dot(place, s32[...].astype(BF16)).astype(BF16)
    total = dot(back[:, :, pl.ds(HV + 2 * HIDDEN, HIDDEN)].reshape(pf, HIDDEN), spread_act, NT)
    arrived(zh_r, nz - 1, 10)
    parts = zh_r[...].reshape(nslot, pf)
    total = total + dot(parts, wt[pl.ds(0, nslot), :], TN) + dot(parts, wt[pl.ds(nslot, nslot), :], TN)
    xr_s[...] = total.reshape(ncol, FEATS, batch)
    for p in x_peers:
        send(xr_s.at[p], xr_r.at[col], 11, xdev(p))
    sent(xr_s, ncol - 1, 11)
    xr_r[pl.ds(col, 1)] = xr_s[pl.ds(col, 1)]
    arrived(xr_r, ncol - 1, 11)
    tot = xr_r[0]
    for i in range(1, ncol):
        tot = tot + xr_r[i]
    for i in range(nt // 2):
        yo_s[i] = tot[:, hl * i : hl * (i + 1)].astype(BF16)
    for p in y_peers:
        send(yo_s.at[p >> 1], yo_r.at[y], 12, ydev(p))
    sent(yo_r, nt - 1, 12)
    yo_r[pl.ds(y, 1)] = yo_s[pl.ds(y >> 1, 1)]
    arrived(yo_r, nt - 1, 12)
    tot = yo_r[0].astype(F32)
    for i in range(1, nt):
        tot = tot + yo_r[i].astype(F32)
    res = mid_own + tot
    res = jnp.where((y & 1) == 1, pltpu.roll(res, ob, 1), res)
    o_mixed[...] = res[:, :ob].astype(BF16)

    for buf, n, k in pending:
        part = buf.at[pl.ds(0, n)]
        pltpu.make_async_copy(part, part, ssem.at[k]).wait()


def body(nz, nx, nc, nt, *args):
    args = list(args)
    ncol = nx * nc
    pf = FEATS * ncol
    rows = SEQS * nz
    batch = rows * ncol
    lq = LATENT // nt
    nslot = nz * SLOTS
    hl = 2 * (batch // nt)
    aw = QW + lq + 128
    for i in (1, 12):
        args[i] = args[i].reshape(nz, pf)
    args[5] = args[5].reshape(1, LATENT)
    half = HEAD_ROT // 2
    frequency = THETA_BASE ** (-np.arange(half, dtype=np.float64) / half)
    angles = frequency.astype(np.float32)[:, None] * np.arange(CACHE, dtype=np.float32)[None, :]
    trig = jnp.asarray(np.stack([np.cos(angles.astype(np.float64)), np.sin(angles.astype(np.float64))]).astype(np.float32))
    freq = jnp.asarray(np.tile(frequency.astype(np.float32), 128 // half)[None, :])
    vm = pltpu.VMEM
    scratch = [
        vm((ncol, FEATS, QW + lq + batch), BF16),
        vm((ncol, FEATS, HV + 3 * HIDDEN), BF16),
        vm((128, pf), BF16),
        vm((nz, pf), F32), vm((nz, pf), F32), vm((1, LATENT), F32), vm((1, 128), F32),
        vm((LATENT, LOCAL_HEADS * HEAD_KEY), BF16), vm((LATENT, HV), BF16),
        vm((SEQS, CACHE, LATENT), BF16), vm((SEQS, HEAD_ROT, CACHE), BF16),
        pltpu.SMEM((SEQS,), jnp.int32),
        vm((batch, 4), jnp.int32), vm((batch, 4), F32),
        vm((pf * nz, 2 * HIDDEN), BF16), vm((HIDDEN, pf * nz), BF16),
        vm((2, half, CACHE), F32),
        vm((nz, SEQS, aw), F32), vm((nz, SEQS, aw), F32),
        vm((nt, SEQS, lq), F32),
        vm((nz, SEQS, HV), F32),
        vm((nt, rows, pf), F32),
        vm((ncol, rows, pf), BF16),
        vm((nz, SEQS, 2 * HIDDEN + 128), F32), vm((nz, SEQS, 2 * HIDDEN + 128), F32),
        vm((nz, SLOTS, pf), BF16), vm((nz, SLOTS, pf), BF16),
        vm((nz, SLOTS, pf), BF16), vm((nz, SLOTS, pf), BF16),
        vm((nz, SEQS, HIDDEN), F32),
        vm((ncol, FEATS, batch), F32), vm((ncol, FEATS, batch), F32),
        vm((nt // 2, FEATS, hl), BF16), vm((nt, FEATS, hl), BF16),
        vm((LATENT + 256, QW), BF16),
        vm((SEQS, HEAD_ROT, CACHE), F32),
        vm((nslot, batch), BF16),
        vm((2 * nslot, batch), BF16),
        vm((rows, pf), F32),
        vm((rows, HV), F32),
        vm((rows, HIDDEN), F32),
        vm((rows, aw), F32),
        vm((rows, 2 * HIDDEN + 128), F32),
        pltpu.SemaphoreType.DMA((25,)),
        pltpu.SemaphoreType.DMA((13,)),
        pltpu.SemaphoreType.DMA((13,)),
    ]
    anywhere = pl.BlockSpec(memory_space=pl.ANY)
    return pl.pallas_call(
        functools.partial(kernel, nz, nx, nc, nt),
        out_shape=(
            jax.ShapeDtypeStruct((FEATS, batch // nt), BF16),
            jax.ShapeDtypeStruct((SEQS, LATENT), BF16),
            jax.ShapeDtypeStruct((SEQS, HEAD_ROT), BF16),
        ),
        in_specs=[anywhere] * 23,
        out_specs=(pl.BlockSpec(memory_space=pltpu.VMEM),) * 3,
        scratch_shapes=scratch,
        compiler_params=pltpu.CompilerParams(collective_id=0, has_side_effects=True, vmem_limit_bytes=40 * 2**20),
        name="layer",
    )(*args, trig, freq)


EP = ("z", "x", "c")


def build(devices):
    split = Mesh(devices, ("z", "x", "c", "y"))
    return jax.shard_map(
        functools.partial(body, *devices.shape),
        mesh=split,
        in_specs=(
            P(EP, None),
            P(),
            P(EP, "y"),
            P(EP, None),
            P(),
            P(),
            P(None, "y"),
            P(None, "y"),
            P(EP, None),
            P(EP, None, None),
            P(EP, None, None),
            P(EP),
            P(),
            P(),
            P(),
            P(EP, None, "y"),
            P(EP, None, "y"),
            P(EP, "y", None),
            P(EP, "y"),
            P(EP, "y"),
            P(EP, "y"),
        ),
        out_specs=(P(EP, "y"), P(EP, None), P(EP, None)),
        check_vma=False,
    )


def solution(mesh):
    return build(mesh.devices.reshape(16, 4, 2, mesh.shape["tp"]))
```

```python
import functools

import jax
import jax.numpy as jnp
import numpy as np
from jax import lax
from jax.experimental import pallas as pl
from jax.experimental.pallas import tpu as pltpu
from jax.sharding import Mesh
from jax.sharding import PartitionSpec as P

MESH = pl.DeviceIdType.MESH
F32 = jnp.float32
BF16 = jnp.bfloat16
HIGHEST = lax.Precision.HIGHEST
NN = (((1,), (0,)), ((), ()))
NT = (((1,), (1,)), ((), ()))
TN = (((0,), (0,)), ((), ()))

LOCAL_HEADS = 4
HEAD_KEY = 64
HEAD_ROT = 32
HEAD_VAL = 64
PER_HEAD = HEAD_KEY + HEAD_ROT
LATENT = 512
CACHE = 1024
HIDDEN = 128
SLOTS = 16
FEATS = 16
SEQS = 2
EPSILON = 1e-06
THETA_BASE = 10000.0
ROUTED_SCALE = 2.5
QW = LOCAL_HEADS * PER_HEAD
HV = LOCAL_HEADS * HEAD_VAL


def dot(a, b, dims=NN, precision=None):
    return lax.dot_general(a, b, dims, precision=precision, preferred_element_type=F32)


def iota(shape, axis):
    return lax.broadcasted_iota(jnp.int32, shape, axis)


def ones_where(mask, dtype=BF16):
    return jnp.where(mask, 1.0, 0.0).astype(dtype)


def rounded(v):
    return v.astype(BF16).astype(F32)


def log2(n):
    return n.bit_length() - 1


def kernel(nz, nx, nc, nt, *refs):
    (
        hidden, attn_gain, w_query, w_latent, w_rotkey, latent_gain, w_key_up, w_value_up, w_attn_out, cache_latent, cache_rotkey,
        lengths, ffn_gain, route_ids, route_scores, w_exp_gate, w_exp_up, w_exp_down, w_shared_gate, w_shared_up, w_shared_out,
        trig, freq,
        o_mixed, o_latent, o_rotkey,
        crit, back, rotw, again, fgain, lgain, fr, keyup, valup, cache, crot, lens, ids, scores, wgu, wd, trg,
        za_s, za_r, yb, zd, ye, midx, zf_s, zf_r, zg_s, zg_r, zh_s, zh_r, zs, xr_s, xr_r, yo_s, yo_r,
        ka, krot, sel_p, wt, ht, h32, s32, pall, shf,
        lsem, ssem, rsem,
    ) = refs
    ncol = nx * nc
    pf = FEATS * ncol
    rows = SEQS * nz
    batch = rows * ncol
    width = pf * nz
    lq = LATENT // nt
    nslot = nz * SLOTS
    ob = batch // nt
    hl = 2 * ob
    z, x, c, y = (lax.axis_index(a) for a in ("z", "x", "c", "y"))
    col = x * nc + c

    z_order = sorted(range(1, nz), key=lambda d: -min(d, nz - d))
    z_peers = [(lax.rem(z + d, nz),) for d in z_order]

    def zdev(p):
        return {"z": p}

    def xdev(p):
        return {"x": lax.div(p, nc), "c": lax.rem(p, nc)}

    def ydev(p):
        return {"y": p}

    x_peers = [lax.rem(col + d, ncol) for d in range(1, ncol)]
    y_peers = [lax.rem(y + d, nt) for d in range(1, nt)]
    z_peers = [p for (p,) in z_peers]

    bar = pltpu.get_barrier_semaphore()
    for p in z_peers:
        pl.semaphore_signal(bar, inc=1, device_id=zdev(p), device_id_type=MESH)
    for p in x_peers:
        pl.semaphore_signal(bar, inc=1, device_id=xdev(p), device_id_type=MESH)
    for p in y_peers:
        pl.semaphore_signal(bar, inc=1, device_id=ydev(p), device_id_type=MESH)

    def loads(sem, pairs):
        copies = [pltpu.make_async_copy(s, d, lsem.at[sem + i]) for i, (s, d) in enumerate(pairs)]
        for cp in copies:
            cp.start()
        return copies

    def done(copies):
        for cp in copies:
            cp.wait()

    own_lq = pl.ds(pl.multiple_of(y * lq, lq), lq)
    own_hv = pl.ds(pl.multiple_of(y * HV, HV), HV)
    own_pf = pl.ds(pl.multiple_of(z * pf, pf), pf)
    half = HEAD_ROT // 2
    l_crit = loads(0, [
        (w_query, crit.at[col, :, pl.ds(0, QW)]),
        (w_latent.at[:, own_lq], crit.at[col, :, pl.ds(QW, lq)]),
        (hidden, crit.at[col, :, pl.ds(QW + lq, batch)]),
    ])
    l_rot = loads(3, [
        (w_rotkey.at[:, own_pf], rotw.at[pl.ds(0, HEAD_ROT)]),
        (w_rotkey.at[pl.ds(half, half), own_pf], rotw.at[pl.ds(64, half)]),
        (w_rotkey.at[pl.ds(0, half), own_pf], rotw.at[pl.ds(64 + half, half)]),
        (attn_gain, again),
        (ffn_gain, fgain),
        (latent_gain, lgain),
        (freq, fr),
        (lengths, lens),
    ])
    l_back = loads(11, [
        (w_attn_out.at[:, own_hv], back.at[col, :, pl.ds(0, HV)]),
        (w_shared_gate, back.at[col, :, pl.ds(HV, HIDDEN)]),
        (w_shared_up, back.at[col, :, pl.ds(HV + HIDDEN, HIDDEN)]),
        (w_shared_out, back.at[col, :, pl.ds(HV + 2 * HIDDEN, HIDDEN)]),
    ])
    l_tab = loads(15, [
        (w_key_up, keyup), (cache_rotkey, crot), (trig, trg), (route_ids, ids), (route_scores, scores),
    ])
    l_att = loads(20, [(cache_latent, cache), (w_value_up, valup)])
    l_exp = loads(22, [
        (w_exp_gate.at[0], wgu.at[:, pl.ds(0, HIDDEN)]),
        (w_exp_up.at[0], wgu.at[:, pl.ds(HIDDEN, HIDDEN)]),
        (w_exp_down.at[0], wd),
    ])

    def send(src, dst, k, dev):
        cp = pltpu.make_async_remote_copy(
            src_ref=src, dst_ref=dst, send_sem=ssem.at[k], recv_sem=rsem.at[k], device_id=dev, device_id_type=MESH
        )
        cp.start()

    def arrived(buf, n, k):
        part = buf.at[pl.ds(0, n)]
        pltpu.make_async_copy(part, part, rsem.at[k]).wait()

    pending = []

    def sent(buf, n, k):
        pending.append((buf, n, k))

    done(l_crit)
    pl.semaphore_wait(bar, len(z_peers) + len(x_peers) + len(y_peers))
    for p in x_peers:
        send(crit.at[col], crit.at[col], 0, xdev(p))
    sent(crit, ncol - 1, 0)
    done(l_back)
    for p in x_peers:
        send(back.at[col], back.at[col], 1, xdev(p))
    sent(back, ncol - 1, 1)

    done(l_rot)
    done(l_tab)
    cos_t, sin_t = trg[0], trg[1]
    for s in range(SEQS):
        low = crot[s, pl.ds(0, half), :].astype(F32)
        high = crot[s, pl.ds(half, half), :].astype(F32)
        krot[s, pl.ds(0, half), :] = low * cos_t - high * sin_t
        krot[s, pl.ds(half, half), :] = low * sin_t + high * cos_t
    spread_r = iota((LOCAL_HEADS * HEAD_KEY, QW), 0)
    spread = ones_where(iota((LOCAL_HEADS * HEAD_KEY, QW), 1) == spread_r + HEAD_ROT * (spread_r >> log2(HEAD_KEY)))
    ka[pl.ds(0, LATENT), :] = dot(keyup[...], spread).astype(BF16)
    lane_q = iota((256, QW), 1)
    head_q = ones_where(lane_q >= PER_HEAD, jnp.int32)
    for h in range(2, LOCAL_HEADS):
        head_q = head_q + ones_where(lane_q >= h * PER_HEAD, jnp.int32)
    within = lane_q - PER_HEAD * head_q - HEAD_KEY
    row_q = iota((256, QW), 0)
    want = jnp.where(row_q < 128, row_q, (row_q - 128) ^ half)
    limit = jnp.where(row_q < 128, row_q, row_q - 128)
    ka[pl.ds(LATENT, 256), :] = ones_where((within == want) & (limit < HEAD_ROT))
    rot_rows = iota((128, pf), 0)
    rot_w = jnp.where((rot_rows & 63) < HEAD_ROT, rotw[...].astype(F32), 0.0).astype(BF16)

    arrived(crit, ncol - 1, 0)
    r_i, b_i = iota((rows, batch), 0), iota((rows, batch), 1)
    sel_a = ones_where(b_i == (r_i >> 1) * (ncol * SEQS) + col * SEQS + (r_i & 1))
    hid = crit[:, :, pl.ds(QW + lq, batch)].reshape(pf, batch)
    h_t = dot(sel_a, hid, NT)
    ht[...] = h_t
    scaled = (h_t * again[pl.ds(z, 1), :]).astype(BF16)
    main = dot(scaled, crit[:, :, pl.ds(0, QW + lq)].reshape(pf, QW + lq))
    rot = dot(scaled, rot_w, NT)
    square = jnp.sum(h_t * h_t, axis=1, keepdims=True)
    rot = jnp.where(iota((rows, 128), 1) == HEAD_ROT, square, rot)
    aw = QW + lq + 128
    pall[:, pl.ds(0, QW + lq)] = main
    pall[:, pl.ds(QW + lq, 128)] = rot
    for i in range(nz):
        za_s[i] = pall[pl.ds(SEQS * i, SEQS), :]
    for p in z_peers:
        send(za_s.at[p], za_r.at[z], 2, zdev(p))
    sent(za_s, nz - 1, 2)
    za_r[pl.ds(z, 1)] = za_s[pl.ds(z, 1)]

    rs = scores[...]
    rw = ROUTED_SCALE * rs / jnp.sum(rs, axis=0, keepdims=True)
    idv = ids[...]
    target = iota((nz, batch), 0) * ncol + col
    hit = jnp.zeros((nz, batch), F32)
    wgt = jnp.zeros((nz, batch), F32)
    for k in range(4):
        same = idv[k : k + 1, :] == target
        hit = jnp.where(same, 1.0, hit)
        wgt = jnp.where(same, rw[k : k + 1, :], wgt)
    before = ones_where(iota((batch, batch), 0) < iota((batch, batch), 1))
    rank = dot(hit.astype(BF16), before)
    val = jnp.where(hit > 0.0, rank, -1.0).astype(BF16)
    expand = ones_where(iota((nslot, nz), 1) == (iota((nslot, nz), 0) >> log2(SLOTS)))
    slot_i = (iota((nslot, batch), 0) & (SLOTS - 1)).astype(F32)
    in_slot = dot(expand, val) == slot_i
    w_hi = wgt.astype(BF16)
    w_lo = (wgt - w_hi.astype(F32)).astype(BF16)
    wt[pl.ds(0, nslot), :] = jnp.where(in_slot, dot(expand, w_hi), 0.0).astype(BF16)
    wt[pl.ds(nslot, nslot), :] = jnp.where(in_slot, dot(expand, w_lo), 0.0).astype(BF16)

    def natural(p):
        return ((p >> 1) & (nz - 1)) * (ncol * SEQS) + (p >> log2(rows)) * SEQS + (p & 1)

    perm = ones_where(iota((batch, batch), 0) == natural(iota((batch, batch), 1)))
    sel_p[...] = dot(ones_where(in_slot), perm).astype(BF16)

    arrived(za_r, nz - 1, 2)
    tot = za_r[0]
    for i in range(1, nz):
        tot = tot + za_r[i]
    lane2 = iota((SEQS, 128), 1)
    tail = tot[:, QW + lq : aw]
    sq = jnp.sum(jnp.where(lane2 == HEAD_ROT, tail, 0.0), axis=1, keepdims=True)
    scale = lax.rsqrt(sq / width + EPSILON)
    yb[pl.ds(y, 1)] = rounded(tot[:, QW : QW + lq] * scale).reshape(1, SEQS, lq)
    for p in y_peers:
        send(yb.at[y], yb.at[y], 3, ydev(p))
    sent(yb, nt - 1, 3)
    q = rounded(tot[:, :QW] * scale)
    nrows = SEQS * LOCAL_HEADS
    r8 = iota((nrows, 128), 0)
    first8 = r8 < LOCAL_HEADS

    def per_row(v):
        top = iota((nrows, v.shape[1]), 0) < LOCAL_HEADS
        return jnp.where(top, v[0:1, :], v[1:2, :])

    lane_8 = iota((nrows, QW), 1)
    first = (iota((nrows, QW), 0) & (LOCAL_HEADS - 1)) * PER_HEAD
    q8 = jnp.where((lane_8 >= first) & (lane_8 < first + PER_HEAD), per_row(q), 0.0).astype(BF16)
    qa = dot(q8, ka[...], NT)
    absorbed = qa[:, :LATENT].astype(BF16)
    len8 = jnp.where(first8, lens[0], lens[1])
    angle = len8.astype(F32) * fr[...]
    cos8 = jnp.cos(angle)
    lane8 = iota((nrows, 128), 1)
    sin8 = jnp.where((lane8 & half) == 0, -jnp.sin(angle), jnp.sin(angle))
    q_rot = qa[:, LATENT : LATENT + 128] * cos8 + qa[:, LATENT + 128 : LATENT + 256] * sin8

    done(l_att)
    q32 = q_rot[:, :HEAD_ROT]
    per_seq = [dot(absorbed, cache[s], NT) + dot(q32, krot[s], NN, HIGHEST) for s in range(SEQS)]
    top_rows = iota((nrows, CACHE), 0) < LOCAL_HEADS
    score_scale = PER_HEAD**-0.5
    live = iota((nrows, CACHE), 1) < jnp.where(top_rows, lens[0], lens[1])
    cache_score = jnp.where(live, score_scale * jnp.where(top_rows, per_seq[0], per_seq[1]), -1e30)
    best = jnp.max(cache_score, axis=1, keepdims=True)

    new_rot = rounded(tail * scale)
    o_rotkey[...] = new_rot[:, :HEAD_ROT].astype(BF16)
    new_swap = pltpu.roll(new_rot, 64, 1)
    own_rot = jnp.where(lane8 < HEAD_ROT, per_row(new_rot) * cos8 + per_row(new_swap) * sin8, 0.0)

    arrived(yb, nt - 1, 3)
    raw = jnp.concatenate([yb[i] for i in range(nt)], axis=1)
    new_latent = (
        raw * lax.rsqrt(jnp.mean(raw * raw, axis=1, keepdims=True) + EPSILON) * lgain[...]
    ).astype(BF16)
    o_latent[...] = new_latent
    lat8 = per_row(new_latent.astype(F32))
    own_score = score_scale * (
        jnp.sum(absorbed.astype(F32) * lat8, axis=1, keepdims=True)
        + jnp.sum(q_rot * own_rot, axis=1, keepdims=True)
    )
    top_score = jnp.maximum(best, own_score)
    cache_weight = jnp.exp(cache_score - top_score)
    own_weight = jnp.exp(own_score - top_score)
    denominator = jnp.sum(cache_weight, axis=1, keepdims=True) + own_weight
    prob = (cache_weight / denominator).astype(BF16)
    own_prob = rounded(own_weight / denominator)
    ctx = [dot(prob, cache[s]) for s in range(SEQS)]
    top_rows = iota((nrows, LATENT), 0) < LOCAL_HEADS
    context = jnp.where(top_rows, ctx[0], ctx[1]) + own_prob * lat8
    ho = dot(context.astype(BF16), valup[...])
    r_h = iota((nrows, HV), 0)
    ho = jnp.where((iota((nrows, HV), 1) >> log2(HEAD_VAL)) == (r_h & (LOCAL_HEADS - 1)), ho, 0.0)
    h0 = jnp.sum(jnp.where(r_h < LOCAL_HEADS, ho, 0.0), axis=0, keepdims=True)
    h1 = jnp.sum(jnp.where(r_h < LOCAL_HEADS, 0.0, ho), axis=0, keepdims=True)
    heads = rounded(jnp.where(iota((SEQS, HV), 0) == 0, h0, h1))
    zd[pl.ds(z, 1)] = heads.reshape(1, SEQS, HV)
    for p in z_peers:
        send(zd.at[z], zd.at[z], 4, zdev(p))
    sent(zd, nz - 1, 4)

    arrived(back, ncol - 1, 1)
    arrived(zd, nz - 1, 4)
    for i in range(nz):
        h32[pl.ds(SEQS * i, SEQS), :] = zd[i]
    part = dot(h32[...].astype(BF16), back[:, :, pl.ds(0, HV)].reshape(pf, HV), NT)
    ye[pl.ds(y, 1)] = part.reshape(1, rows, pf)
    for p in y_peers:
        send(ye.at[y], ye.at[y], 5, ydev(p))
    sent(ye, nt - 1, 5)
    arrived(ye, nt - 1, 5)
    attn = ye[0]
    for i in range(1, nt):
        attn = attn + ye[i]
    mid = (ht[...] + rounded(attn)).astype(BF16)
    midx[pl.ds(col, 1)] = mid.reshape(1, rows, pf)
    for p in x_peers:
        send(midx.at[col], midx.at[col], 6, xdev(p))
    sent(midx, ncol - 1, 6)
    mid_v = mid.astype(F32)
    ffn = (mid_v * fgain[pl.ds(z, 1), :]).astype(BF16)
    shf[:, pl.ds(0, 2 * HIDDEN)] = dot(ffn, back[:, :, pl.ds(HV, 2 * HIDDEN)].reshape(pf, 2 * HIDDEN))
    shf[:, pl.ds(2 * HIDDEN, 128)] = jnp.broadcast_to(jnp.sum(mid_v * mid_v, axis=1, keepdims=True), (rows, 128))
    for i in range(nz):
        zf_s[i] = shf[pl.ds(SEQS * i, SEQS), :]
    for p in z_peers:
        send(zf_s.at[p], zf_r.at[z], 7, zdev(p))
    sent(zf_s, nz - 1, 7)
    zf_r[pl.ds(z, 1)] = zf_s[pl.ds(z, 1)]

    arrived(midx, ncol - 1, 6)
    mid_all = midx[...].reshape(batch, pf)
    zg_s[...] = dot(sel_p[...], mid_all).astype(BF16).reshape(nz, SLOTS, pf)
    for p in z_peers:
        send(zg_s.at[p], zg_r.at[z], 8, zdev(p))
    sent(zg_s, nz - 1, 8)
    zg_r[pl.ds(z, 1)] = zg_s[pl.ds(z, 1)]
    own_f = ones_where(iota((FEATS, pf), 1) == iota((FEATS, pf), 0) + col * FEATS)
    mid_t = dot(own_f, mid_all, NT).astype(BF16)
    to_half = ones_where(natural(iota((batch, hl), 0)) == iota((batch, hl), 1) + (y >> 1) * hl)
    mid_own = dot(mid_t, to_half)

    arrived(zf_r, nz - 1, 7)
    tot = zf_r[0]
    for i in range(1, nz):
        tot = tot + zf_r[i]
    scale = lax.rsqrt(tot[:, 2 * HIDDEN : 2 * HIDDEN + 1] / width + EPSILON)
    gate = scale * tot[:, :HIDDEN]
    act = rounded(gate / (1.0 + jnp.exp(-gate)) * (scale * tot[:, HIDDEN : 2 * HIDDEN]))
    zs[pl.ds(z, 1)] = act.reshape(1, SEQS, HIDDEN)
    for p in z_peers:
        send(zs.at[z], zs.at[z], 9, zdev(p))
    sent(zs, nz - 1, 9)

    done(l_exp)
    arrived(zg_r, nz - 1, 8)
    pieces = []
    sq = jnp.zeros((SLOTS, 1), F32)
    for i in range(nz):
        v = zg_r[i].astype(F32)
        sq = sq + jnp.sum(v * v, axis=1, keepdims=True)
        pieces.append((v * fgain[pl.ds(i, 1), :]).astype(BF16))
    gu = dot(jnp.concatenate(pieces, axis=1), wgu[...])
    scale = lax.rsqrt(sq / width + EPSILON)
    gate = scale * gu[:, :HIDDEN]
    act = (gate / (1.0 + jnp.exp(-gate)) * (scale * gu[:, HIDDEN:])).astype(BF16)
    out = dot(act, wd[...])
    for i in range(nz):
        zh_s[i] = out[:, pf * i : pf * (i + 1)].astype(BF16)
    for p in z_peers:
        send(zh_s.at[p], zh_r.at[z], 10, zdev(p))
    sent(zh_s, nz - 1, 10)
    zh_r[pl.ds(z, 1)] = zh_s[pl.ds(z, 1)]

    arrived(zs, nz - 1, 9)
    for i in range(nz):
        s32[pl.ds(SEQS * i, SEQS), :] = zs[i]
    place = ones_where(
        iota((batch, rows), 0) == (iota((batch, rows), 1) >> 1) * (ncol * SEQS) + col * SEQS + (iota((batch, rows), 1) & 1)
    )
    spread_act = dot(place, s32[...].astype(BF16)).astype(BF16)
    total = dot(back[:, :, pl.ds(HV + 2 * HIDDEN, HIDDEN)].reshape(pf, HIDDEN), spread_act, NT)
    arrived(zh_r, nz - 1, 10)
    parts = zh_r[...].reshape(nslot, pf)
    total = total + dot(parts, wt[pl.ds(0, nslot), :], TN) + dot(parts, wt[pl.ds(nslot, nslot), :], TN)
    xr_s[...] = total.reshape(ncol, FEATS, batch)
    for p in x_peers:
        send(xr_s.at[p], xr_r.at[col], 11, xdev(p))
    sent(xr_s, ncol - 1, 11)
    xr_r[pl.ds(col, 1)] = xr_s[pl.ds(col, 1)]
    arrived(xr_r, ncol - 1, 11)
    tot = xr_r[0]
    for i in range(1, ncol):
        tot = tot + xr_r[i]
    for i in range(nt // 2):
        yo_s[i] = tot[:, hl * i : hl * (i + 1)].astype(BF16)
    for p in y_peers:
        send(yo_s.at[p >> 1], yo_r.at[y], 12, ydev(p))
    sent(yo_r, nt - 1, 12)
    yo_r[pl.ds(y, 1)] = yo_s[pl.ds(y >> 1, 1)]
    arrived(yo_r, nt - 1, 12)
    tot = yo_r[0].astype(F32)
    for i in range(1, nt):
        tot = tot + yo_r[i].astype(F32)
    res = mid_own + tot
    res = jnp.where((y & 1) == 1, pltpu.roll(res, ob, 1), res)
    o_mixed[...] = res[:, :ob].astype(BF16)

    for buf, n, k in pending:
        part = buf.at[pl.ds(0, n)]
        pltpu.make_async_copy(part, part, ssem.at[k]).wait()


def body(nz, nx, nc, nt, *args):
    args = list(args)
    ncol = nx * nc
    pf = FEATS * ncol
    rows = SEQS * nz
    batch = rows * ncol
    lq = LATENT // nt
    nslot = nz * SLOTS
    hl = 2 * (batch // nt)
    aw = QW + lq + 128
    for i in (1, 12):
        args[i] = args[i].reshape(nz, pf)
    args[5] = args[5].reshape(1, LATENT)
    args[13], args[14] = args[13].T, args[14].T
    half = HEAD_ROT // 2
    frequency = THETA_BASE ** (-np.arange(half, dtype=np.float64) / half)
    angles = frequency.astype(np.float32)[:, None] * np.arange(CACHE, dtype=np.float32)[None, :]
    trig = jnp.asarray(np.stack([np.cos(angles.astype(np.float64)), np.sin(angles.astype(np.float64))]).astype(np.float32))
    freq = jnp.asarray(np.tile(frequency.astype(np.float32), 128 // half)[None, :])
    vm = pltpu.VMEM
    scratch = [
        vm((ncol, FEATS, QW + lq + batch), BF16),
        vm((ncol, FEATS, HV + 3 * HIDDEN), BF16),
        vm((128, pf), BF16),
        vm((nz, pf), F32), vm((nz, pf), F32), vm((1, LATENT), F32), vm((1, 128), F32),
        vm((LATENT, LOCAL_HEADS * HEAD_KEY), BF16), vm((LATENT, HV), BF16),
        vm((SEQS, CACHE, LATENT), BF16), vm((SEQS, HEAD_ROT, CACHE), BF16),
        pltpu.SMEM((SEQS,), jnp.int32),
        vm((4, batch), jnp.int32), vm((4, batch), F32),
        vm((pf * nz, 2 * HIDDEN), BF16), vm((HIDDEN, pf * nz), BF16),
        vm((2, half, CACHE), F32),
        vm((nz, SEQS, aw), F32), vm((nz, SEQS, aw), F32),
        vm((nt, SEQS, lq), F32),
        vm((nz, SEQS, HV), F32),
        vm((nt, rows, pf), F32),
        vm((ncol, rows, pf), BF16),
        vm((nz, SEQS, 2 * HIDDEN + 128), F32), vm((nz, SEQS, 2 * HIDDEN + 128), F32),
        vm((nz, SLOTS, pf), BF16), vm((nz, SLOTS, pf), BF16),
        vm((nz, SLOTS, pf), BF16), vm((nz, SLOTS, pf), BF16),
        vm((nz, SEQS, HIDDEN), F32),
        vm((ncol, FEATS, batch), F32), vm((ncol, FEATS, batch), F32),
        vm((nt // 2, FEATS, hl), BF16), vm((nt, FEATS, hl), BF16),
        vm((LATENT + 256, QW), BF16),
        vm((SEQS, HEAD_ROT, CACHE), F32),
        vm((nslot, batch), BF16),
        vm((2 * nslot, batch), BF16),
        vm((rows, pf), F32),
        vm((rows, HV), F32),
        vm((rows, HIDDEN), F32),
        vm((rows, aw), F32),
        vm((rows, 2 * HIDDEN + 128), F32),
        pltpu.SemaphoreType.DMA((25,)),
        pltpu.SemaphoreType.DMA((13,)),
        pltpu.SemaphoreType.DMA((13,)),
    ]
    anywhere = pl.BlockSpec(memory_space=pltpu.HBM)
    return pl.pallas_call(
        functools.partial(kernel, nz, nx, nc, nt),
        out_shape=(
            jax.ShapeDtypeStruct((FEATS, batch // nt), BF16),
            jax.ShapeDtypeStruct((SEQS, LATENT), BF16),
            jax.ShapeDtypeStruct((SEQS, HEAD_ROT), BF16),
        ),
        in_specs=[anywhere] * 23,
        out_specs=(pl.BlockSpec(memory_space=pltpu.VMEM),) * 3,
        scratch_shapes=scratch,
        compiler_params=pltpu.CompilerParams(collective_id=0, has_side_effects=True, vmem_limit_bytes=67043328),
        name="layer",
    )(*args, trig, freq)


EP = ("z", "x", "c")


def build(devices):
    split = Mesh(devices, ("z", "x", "c", "y"))
    return jax.shard_map(
        functools.partial(body, *devices.shape),
        mesh=split,
        in_specs=(
            P(EP, None),
            P(),
            P(EP, "y"),
            P(EP, None),
            P(),
            P(),
            P(None, "y"),
            P(None, "y"),
            P(EP, None),
            P(EP, None, None),
            P(EP, None, None),
            P(EP),
            P(),
            P(),
            P(),
            P(EP, None, "y"),
            P(EP, None, "y"),
            P(EP, "y", None),
            P(EP, "y"),
            P(EP, "y"),
            P(EP, "y"),
        ),
        out_specs=(P(EP, "y"), P(EP, None), P(EP, None)),
        check_vma=False,
    )


def solution(mesh):
    return build(mesh.devices.reshape(16, 4, 2, mesh.shape["tp"]))
```

```python
import functools

import jax
import jax.numpy as jnp
import numpy as np
from jax import lax
from jax.experimental import pallas as pl
from jax.experimental.pallas import tpu as pltpu
from jax.sharding import Mesh
from jax.sharding import PartitionSpec as P

MESH = pl.DeviceIdType.MESH
F32 = jnp.float32
BF16 = jnp.bfloat16
HIGHEST = lax.Precision.HIGHEST
NN = (((1,), (0,)), ((), ()))
NT = (((1,), (1,)), ((), ()))
TN = (((0,), (0,)), ((), ()))

LOCAL_HEADS = 4
HEAD_KEY = 64
HEAD_ROT = 32
HEAD_VAL = 64
PER_HEAD = HEAD_KEY + HEAD_ROT
LATENT = 512
CACHE = 1024
HIDDEN = 128
SLOTS = 16
FEATS = 16
SEQS = 2
EPSILON = 1e-06
THETA_BASE = 10000.0
ROUTED_SCALE = 2.5
QW = LOCAL_HEADS * PER_HEAD
HV = LOCAL_HEADS * HEAD_VAL


def dot(a, b, dims=NN, precision=None):
    return lax.dot_general(a, b, dims, precision=precision, preferred_element_type=F32)


def iota(shape, axis):
    return lax.broadcasted_iota(jnp.int32, shape, axis)


def ones_where(mask, dtype=BF16):
    return jnp.where(mask, 1.0, 0.0).astype(dtype)


def rounded(v):
    return v.astype(BF16).astype(F32)


def log2(n):
    return n.bit_length() - 1


def kernel(nz, nx, nc, nt, *refs):
    (
        hidden, attn_gain, w_query, w_latent, w_rotkey, latent_gain, w_key_up, w_value_up, w_attn_out, cache_latent, cache_rotkey,
        lengths, ffn_gain, route_ids, route_scores, w_exp_gate, w_exp_up, w_exp_down, w_shared_gate, w_shared_up, w_shared_out,
        trig, freq,
        o_mixed, o_latent, o_rotkey,
        crit, back, rotw, again, fgain, lgain, fr, keyup, valup, cache, crot, lens, ids, scores, wgu, wd, trg,
        za_s, za_r, yb, hs, zd, midx, zf_s, zf_r, zg_s, zg_r, zh_s, zh_r, zs, pd_s, pd_r,
        ka, krot, sel_p, wt, ht, h32, s32, pall, shf,
        lsem, ssem, rsem, ok,
    ) = refs
    ncol = nx * nc
    pf = FEATS * ncol
    rows = SEQS * nz
    batch = rows * ncol
    width = pf * nz
    lq = LATENT // nt
    nslot = nz * SLOTS
    ob = batch // nt
    hl = 2 * ob
    aow = nt * HV
    zy = nz // nt
    z, x, c, y = (lax.axis_index(a) for a in ("z", "x", "c", "y"))
    col = x * nc + c

    z_order = sorted(range(1, nz), key=lambda d: -min(d, nz - d))
    z_peers = [(lax.rem(z + d, nz),) for d in z_order]

    def zdev(p):
        return {"z": p}

    def xdev(p):
        return {"x": lax.div(p, nc), "c": lax.rem(p, nc)}

    def ydev(p):
        return {"y": p}

    x_order = sorted(range(1, ncol), key=lambda d: -min(d, ncol - d))
    x_peers = [lax.rem(col + d, ncol) for d in x_order]
    y_peers = [lax.rem(y + d, nt) for d in range(1, nt)]
    z_peers = [p for (p,) in z_peers]
    plane_order = sorted(
        [(dx, dc, dy) for dx in range(nx) for dc in range(nc) for dy in range(nt) if dx or dc or dy],
        key=lambda t: -(min(t[0], nx - t[0]) + min(t[2], nt - t[2])),
    )
    plane_peers = [
        {"x": lax.rem(x + dx, nx), "c": lax.rem(c + dc, nc), "y": lax.rem(y + dy, nt)} for dx, dc, dy in plane_order
    ]

    bar = pltpu.get_barrier_semaphore()

    def signal(sem, dev):
        pl.semaphore_signal(sem, inc=1, device_id=dev, device_id_type=MESH)

    for d in range(nx - 1, 0, -1):
        signal(bar, {"x": lax.rem(x + d, nx), "c": 0})

    @pl.when(c == 1)
    def _():
        signal(bar, {"c": 0})

    for p in z_peers:
        signal(bar, {"z": p, "c": 1})
    for p in y_peers:
        signal(bar, {"y": p, "c": 1})

    def loads(sem, pairs):
        copies = [pltpu.make_async_copy(s, d, lsem.at[sem + i]) for i, (s, d) in enumerate(pairs)]
        for cp in copies:
            cp.start()
        return copies

    def done(copies):
        for cp in copies:
            cp.wait()

    own_lq = pl.ds(pl.multiple_of(y * lq, lq), lq)
    own_pf = pl.ds(pl.multiple_of(z * pf, pf), pf)
    half = HEAD_ROT // 2
    l_crit = loads(0, [
        (w_query, crit.at[col, :, pl.ds(0, QW)]),
        (w_latent.at[:, own_lq], crit.at[col, :, pl.ds(QW, lq)]),
        (hidden, crit.at[col, :, pl.ds(QW + lq, batch)]),
    ])
    l_rot = loads(3, [
        (w_rotkey.at[:, own_pf], rotw.at[pl.ds(0, HEAD_ROT)]),
        (w_rotkey.at[pl.ds(half, half), own_pf], rotw.at[pl.ds(64, half)]),
        (w_rotkey.at[pl.ds(0, half), own_pf], rotw.at[pl.ds(64 + half, half)]),
        (attn_gain, again),
        (ffn_gain, fgain),
        (latent_gain, lgain),
        (freq, fr),
        (lengths, lens),
    ])
    l_back = loads(11, [
        (w_attn_out, back.at[col, :, pl.ds(0, aow)]),
        (w_shared_gate, back.at[col, :, pl.ds(aow, HIDDEN)]),
        (w_shared_up, back.at[col, :, pl.ds(aow + HIDDEN, HIDDEN)]),
        (w_shared_out, back.at[col, :, pl.ds(aow + 2 * HIDDEN, HIDDEN)]),
    ])
    l_tab = loads(15, [
        (w_key_up, keyup), (cache_rotkey, crot), (trig, trg), (route_ids, ids), (route_scores, scores),
    ])
    l_att = loads(20, [(cache_latent, cache), (w_value_up, valup)])
    l_exp = loads(22, [
        (w_exp_gate.at[0], wgu.at[:, pl.ds(0, HIDDEN)]),
        (w_exp_up.at[0], wgu.at[:, pl.ds(HIDDEN, HIDDEN)]),
        (w_exp_down.at[0], wd),
    ])

    def send(src, dst, k, dev):
        cp = pltpu.make_async_remote_copy(
            src_ref=src, dst_ref=dst, send_sem=ssem.at[k], recv_sem=rsem.at[k], device_id=dev, device_id_type=MESH
        )
        cp.start()

    def arrived(buf, n, k):
        part = buf.at[pl.ds(0, n)]
        pltpu.make_async_copy(part, part, rsem.at[k]).wait()

    pending, late = [], []

    def sent(buf, n, k):
        pending.append((buf, n, k))

    done(l_crit)

    @pl.when(c == 0)
    def _():
        pl.semaphore_wait(bar, nc * nx - 1)
        signal(ok.at[0], {"c": 1})

    @pl.when(c == 1)
    def _():
        pl.semaphore_wait(ok.at[0], 1)

    for p in x_peers:
        send(crit.at[col], crit.at[col], 0, xdev(p))
    sent(crit, ncol - 1, 0)

    done(l_rot)
    done(l_tab)
    cos_t, sin_t = trg[0], trg[1]
    for s in range(SEQS):
        low = crot[s, pl.ds(0, half), :].astype(F32)
        high = crot[s, pl.ds(half, half), :].astype(F32)
        krot[s, pl.ds(0, half), :] = low * cos_t - high * sin_t
        krot[s, pl.ds(half, half), :] = low * sin_t + high * cos_t
    spread_r = iota((LOCAL_HEADS * HEAD_KEY, QW), 0)
    spread = ones_where(iota((LOCAL_HEADS * HEAD_KEY, QW), 1) == spread_r + HEAD_ROT * (spread_r >> log2(HEAD_KEY)))
    ka[pl.ds(0, LATENT), :] = dot(keyup[...], spread).astype(BF16)
    lane_q = iota((256, QW), 1)
    head_q = ones_where(lane_q >= PER_HEAD, jnp.int32)
    for h in range(2, LOCAL_HEADS):
        head_q = head_q + ones_where(lane_q >= h * PER_HEAD, jnp.int32)
    within = lane_q - PER_HEAD * head_q - HEAD_KEY
    row_q = iota((256, QW), 0)
    want = jnp.where(row_q < 128, row_q, (row_q - 128) ^ half)
    limit = jnp.where(row_q < 128, row_q, row_q - 128)
    ka[pl.ds(LATENT, 256), :] = ones_where((within == want) & (limit < HEAD_ROT))
    rot_rows = iota((128, pf), 0)
    rot_w = jnp.where((rot_rows & 63) < HEAD_ROT, rotw[...].astype(F32), 0.0).astype(BF16)

    arrived(crit, ncol - 1, 0)
    r_i, b_i = iota((rows, batch), 0), iota((rows, batch), 1)
    sel_a = ones_where(b_i == (r_i >> 1) * (ncol * SEQS) + col * SEQS + (r_i & 1))
    hid = crit[:, :, pl.ds(QW + lq, batch)].reshape(pf, batch)
    h_t = dot(sel_a, hid, NT)
    ht[...] = h_t
    scaled = (h_t * again[pl.ds(z, 1), :]).astype(BF16)
    main = dot(scaled, crit[:, :, pl.ds(0, QW + lq)].reshape(pf, QW + lq))
    rot = dot(scaled, rot_w, NT)
    square = jnp.sum(h_t * h_t, axis=1, keepdims=True)
    rot = jnp.where(iota((rows, 128), 1) == HEAD_ROT, square, rot)
    aw = QW + lq + 128
    pall[:, pl.ds(0, QW + lq)] = main
    pall[:, pl.ds(QW + lq, 128)] = rot
    for i in range(nz):
        za_s[i] = pall[pl.ds(SEQS * i, SEQS), :]

    @pl.when(c == 1)
    def _():
        pl.semaphore_wait(bar, nc * (nz - 1) + nc * (nt - 1))
        signal(ok.at[1], {"c": 0})

    @pl.when(c == 0)
    def _():
        pl.semaphore_wait(ok.at[1], 1)

    for p in z_peers:
        send(za_s.at[p], za_r.at[z], 2, zdev(p))
    sent(za_s, nz - 1, 2)
    za_r[pl.ds(z, 1)] = za_s[pl.ds(z, 1)]
    done(l_back)
    for p in x_peers:
        send(back.at[col], back.at[col], 1, xdev(p))
    sent(back, ncol - 1, 1)

    rs = scores[...]
    rw = ROUTED_SCALE * rs / jnp.sum(rs, axis=0, keepdims=True)
    idv = ids[...]
    target = iota((nz, batch), 0) * ncol + col
    hit = jnp.zeros((nz, batch), F32)
    wgt = jnp.zeros((nz, batch), F32)
    for k in range(4):
        same = idv[k : k + 1, :] == target
        hit = jnp.where(same, 1.0, hit)
        wgt = jnp.where(same, rw[k : k + 1, :], wgt)
    before = ones_where(iota((batch, batch), 0) < iota((batch, batch), 1))
    rank = dot(hit.astype(BF16), before)
    val = jnp.where(hit > 0.0, rank, -1.0).astype(BF16)
    expand = ones_where(iota((nslot, nz), 1) == (iota((nslot, nz), 0) >> log2(SLOTS)))
    slot_i = (iota((nslot, batch), 0) & (SLOTS - 1)).astype(F32)
    in_slot = dot(expand, val) == slot_i
    w_hi = wgt.astype(BF16)
    w_lo = (wgt - w_hi.astype(F32)).astype(BF16)
    wt[pl.ds(0, nslot), :] = jnp.where(in_slot, dot(expand, w_hi), 0.0).astype(BF16)
    wt[pl.ds(nslot, nslot), :] = jnp.where(in_slot, dot(expand, w_lo), 0.0).astype(BF16)

    def natural(p):
        return ((p >> 1) & (nz - 1)) * (ncol * SEQS) + (p >> log2(rows)) * SEQS + (p & 1)

    perm = ones_where(iota((batch, batch), 0) == natural(iota((batch, batch), 1)))
    sel_p[...] = dot(ones_where(in_slot), perm).astype(BF16)

    arrived(za_r, nz - 1, 2)
    tot = za_r[0]
    for i in range(1, nz):
        tot = tot + za_r[i]
    lane2 = iota((SEQS, 128), 1)
    tail = tot[:, QW + lq : aw]
    sq = jnp.sum(jnp.where(lane2 == HEAD_ROT, tail, 0.0), axis=1, keepdims=True)
    scale = lax.rsqrt(sq / width + EPSILON)
    yb[pl.ds(y, 1)] = rounded(tot[:, QW : QW + lq] * scale).reshape(1, SEQS, lq)
    for p in y_peers:
        send(yb.at[y], yb.at[y], 3, ydev(p))
    sent(yb, nt - 1, 3)
    q = rounded(tot[:, :QW] * scale)
    nrows = SEQS * LOCAL_HEADS
    r8 = iota((nrows, 128), 0)
    first8 = r8 < LOCAL_HEADS

    def per_row(v):
        top = iota((nrows, v.shape[1]), 0) < LOCAL_HEADS
        return jnp.where(top, v[0:1, :], v[1:2, :])

    lane_8 = iota((nrows, QW), 1)
    first = (iota((nrows, QW), 0) & (LOCAL_HEADS - 1)) * PER_HEAD
    q8 = jnp.where((lane_8 >= first) & (lane_8 < first + PER_HEAD), per_row(q), 0.0).astype(BF16)
    qa = dot(q8, ka[...], NT)
    absorbed = qa[:, :LATENT].astype(BF16)
    len8 = jnp.where(first8, lens[0], lens[1])
    angle = len8.astype(F32) * fr[...]
    cos8 = jnp.cos(angle)
    lane8 = iota((nrows, 128), 1)
    sin8 = jnp.where((lane8 & half) == 0, -jnp.sin(angle), jnp.sin(angle))
    q_rot = qa[:, LATENT : LATENT + 128] * cos8 + qa[:, LATENT + 128 : LATENT + 256] * sin8

    done(l_att)
    q32 = q_rot[:, :HEAD_ROT]
    per_seq = [dot(absorbed, cache[s], NT) + dot(q32, krot[s], NN, HIGHEST) for s in range(SEQS)]
    top_rows = iota((nrows, CACHE), 0) < LOCAL_HEADS
    score_scale = PER_HEAD**-0.5
    live = iota((nrows, CACHE), 1) < jnp.where(top_rows, lens[0], lens[1])
    cache_score = jnp.where(live, score_scale * jnp.where(top_rows, per_seq[0], per_seq[1]), -1e30)
    best = jnp.max(cache_score, axis=1, keepdims=True)

    new_rot = rounded(tail * scale)
    o_rotkey[...] = new_rot[:, :HEAD_ROT].astype(BF16)
    new_swap = pltpu.roll(new_rot, 64, 1)
    own_rot = jnp.where(lane8 < HEAD_ROT, per_row(new_rot) * cos8 + per_row(new_swap) * sin8, 0.0)

    arrived(yb, nt - 1, 3)
    raw = jnp.concatenate([yb[i] for i in range(nt)], axis=1)
    new_latent = (
        raw * lax.rsqrt(jnp.mean(raw * raw, axis=1, keepdims=True) + EPSILON) * lgain[...]
    ).astype(BF16)
    o_latent[...] = new_latent
    lat8 = per_row(new_latent.astype(F32))
    own_score = score_scale * (
        jnp.sum(absorbed.astype(F32) * lat8, axis=1, keepdims=True)
        + jnp.sum(q_rot * own_rot, axis=1, keepdims=True)
    )
    top_score = jnp.maximum(best, own_score)
    cache_weight = jnp.exp(cache_score - top_score)
    own_weight = jnp.exp(own_score - top_score)
    denominator = jnp.sum(cache_weight, axis=1, keepdims=True) + own_weight
    prob = (cache_weight / denominator).astype(BF16)
    own_prob = rounded(own_weight / denominator)
    ctx = [dot(prob, cache[s]) for s in range(SEQS)]
    top_rows = iota((nrows, LATENT), 0) < LOCAL_HEADS
    context = jnp.where(top_rows, ctx[0], ctx[1]) + own_prob * lat8
    ho = dot(context.astype(BF16), valup[...])
    r_h = iota((nrows, HV), 0)
    ho = jnp.where((iota((nrows, HV), 1) >> log2(HEAD_VAL)) == (r_h & (LOCAL_HEADS - 1)), ho, 0.0)
    h0 = jnp.sum(jnp.where(r_h < LOCAL_HEADS, ho, 0.0), axis=0, keepdims=True)
    h1 = jnp.sum(jnp.where(r_h < LOCAL_HEADS, 0.0, ho), axis=0, keepdims=True)
    heads = rounded(jnp.where(iota((SEQS, HV), 0) == 0, h0, h1))
    hs[...] = heads
    y_to = lax.div(z, zy)
    spot = lax.rem(z, zy) * nt + y
    to = zd.at[spot]
    for p in z_peers:
        send(hs, to, 4, {"z": p, "y": y_to})

    @pl.when(y_to == y)
    def _():
        zd[pl.ds(spot, 1)] = heads.reshape(1, SEQS, HV)

    @pl.when(y_to != y)
    def _():
        send(hs, to, 4, {"y": y_to})

    def heads_wait(sems):
        for remote in (True, False):

            @pl.when((y_to != y) if remote else (y_to == y))
            def _():
                part = zd.at[pl.ds(0, nz if remote else nz - 1)]
                pltpu.make_async_copy(part, part, sems.at[4]).wait()

    late.append(lambda: heads_wait(ssem))
    arrived(back, ncol - 1, 1)
    heads_wait(rsem)
    for j in range(zy):
        for i in range(nt):
            h32[pl.ds(SEQS * j, SEQS), pl.ds(HV * i, HV)] = zd[j * nt + i]
    group = SEQS * zy
    attn = dot(h32[...].astype(BF16), back[:, :, pl.ds(0, aow)].reshape(pf, aow), NT)
    mid = rounded(ht[pl.ds(pl.multiple_of(group * y, group), group), :] + rounded(attn))
    place_of = col * nt + y
    midx[pl.ds(place_of, 1)] = mid.reshape(1, group, pf)
    for dev in plane_peers:
        send(midx.at[place_of], midx.at[place_of], 6, dev)
    sent(midx, ncol * nt - 1, 6)

    arrived(midx, ncol * nt - 1, 6)
    mid_all = midx[...].reshape(batch, pf).astype(BF16)
    zg_s[...] = dot(sel_p[...], mid_all).astype(BF16).reshape(nz, SLOTS, pf)
    for p in z_peers:
        send(zg_s.at[p], zg_r.at[z], 8, zdev(p))
    sent(zg_s, nz - 1, 8)
    zg_r[pl.ds(z, 1)] = zg_s[pl.ds(z, 1)]
    mid_v = midx[pl.ds(pl.multiple_of(col * nt, nt), nt)].reshape(rows, pf)
    ffn = (mid_v * fgain[pl.ds(z, 1), :]).astype(BF16)
    shf[:, pl.ds(0, 2 * HIDDEN)] = dot(ffn, back[:, :, pl.ds(aow, 2 * HIDDEN)].reshape(pf, 2 * HIDDEN))
    shf[:, pl.ds(2 * HIDDEN, 128)] = jnp.broadcast_to(jnp.sum(mid_v * mid_v, axis=1, keepdims=True), (rows, 128))
    for i in range(nz):
        zf_s[i] = shf[pl.ds(SEQS * i, SEQS), :]
    for p in z_peers:
        send(zf_s.at[p], zf_r.at[z], 7, zdev(p))
    sent(zf_s, nz - 1, 7)
    zf_r[pl.ds(z, 1)] = zf_s[pl.ds(z, 1)]
    own_f = ones_where(iota((FEATS, pf), 1) == iota((FEATS, pf), 0) + col * FEATS)
    mid_t = dot(own_f, mid_all, NT).astype(BF16)
    to_own = ones_where(natural(iota((batch, hl), 0)) == (iota((batch, hl), 1) & (ob - 1)) + y * ob)
    mid_own = dot(mid_t, to_own)
    mid_own = jnp.where(iota((FEATS // 2, hl), 1) < ob, mid_own[: FEATS // 2], mid_own[FEATS // 2 :])

    arrived(zg_r, nz - 1, 8)
    arrived(zf_r, nz - 1, 7)
    tot = zf_r[0]
    for i in range(1, nz):
        tot = tot + zf_r[i]
    scale = lax.rsqrt(tot[:, 2 * HIDDEN : 2 * HIDDEN + 1] / width + EPSILON)
    gate = scale * tot[:, :HIDDEN]
    act = rounded(gate / (1.0 + jnp.exp(-gate)) * (scale * tot[:, HIDDEN : 2 * HIDDEN]))
    zs[pl.ds(z, 1)] = act.reshape(1, SEQS, HIDDEN)
    for p in z_peers:
        send(zs.at[z], zs.at[z], 9, zdev(p))
    sent(zs, nz - 1, 9)

    done(l_exp)
    pieces = []
    sq = jnp.zeros((SLOTS, 1), F32)
    for i in range(nz):
        v = zg_r[i].astype(F32)
        sq = sq + jnp.sum(v * v, axis=1, keepdims=True)
        pieces.append((v * fgain[pl.ds(i, 1), :]).astype(BF16))
    gu = dot(jnp.concatenate(pieces, axis=1), wgu[...])
    scale = lax.rsqrt(sq / width + EPSILON)
    gate = scale * gu[:, :HIDDEN]
    act = (gate / (1.0 + jnp.exp(-gate)) * (scale * gu[:, HIDDEN:])).astype(BF16)
    out = dot(act, wd[...])
    for i in range(nz):
        zh_s[i] = out[:, pf * i : pf * (i + 1)].astype(BF16)
    for p in z_peers:
        send(zh_s.at[p], zh_r.at[z], 10, zdev(p))
    sent(zh_s, nz - 1, 10)
    zh_r[pl.ds(z, 1)] = zh_s[pl.ds(z, 1)]

    arrived(zs, nz - 1, 9)
    for i in range(nz):
        s32[pl.ds(SEQS * i, SEQS), :] = zs[i]
    place = ones_where(
        iota((batch, rows), 0) == (iota((batch, rows), 1) >> 1) * (ncol * SEQS) + col * SEQS + (iota((batch, rows), 1) & 1)
    )
    spread_act = dot(place, s32[...].astype(BF16)).astype(BF16)
    total = dot(back[:, :, pl.ds(aow + 2 * HIDDEN, HIDDEN)].reshape(pf, HIDDEN), spread_act, NT)
    arrived(zh_r, nz - 1, 10)
    parts = zh_r[...].reshape(nslot, pf)
    total = total + dot(parts, wt[pl.ds(0, nslot), :], TN) + dot(parts, wt[pl.ds(nslot, nslot), :], TN)
    total = total.reshape(ncol, 2, FEATS // 2, batch)
    low_lane = iota((ncol, FEATS // 2, hl), 2) < ob
    for k in range(nt // 2):
        ta = total[:, 0, :, hl * k : hl * (k + 1)]
        tb = total[:, 1, :, hl * k : hl * (k + 1)]
        flat = (ncol * FEATS // 2, hl)
        ra = pltpu.roll(ta.reshape(flat), ob, 1).reshape(ta.shape)
        rb = pltpu.roll(tb.reshape(flat), ob, 1).reshape(tb.shape)
        pd_s[:, 2 * k] = jnp.where(low_lane, ta, rb)
        pd_s[:, 2 * k + 1] = jnp.where(low_lane, ra, tb)
    for dev in plane_peers:
        send(pd_s.at[dev["x"] * nc + dev["c"], dev["y"]], pd_r.at[place_of], 11, dev)
    sent(pd_r, ncol * nt - 1, 11)
    pd_r[pl.ds(place_of, 1)] = pd_s[pl.ds(col, 1), pl.ds(y, 1)].reshape(1, FEATS // 2, hl)
    arrived(pd_r, ncol * nt - 1, 11)
    tot = pd_r[0]
    for i in range(1, ncol * nt):
        tot = tot + pd_r[i]
    o_mixed[...] = mid_own + tot

    late.pop()()
    for buf, n, k in pending:
        part = buf.at[pl.ds(0, n)]
        pltpu.make_async_copy(part, part, ssem.at[k]).wait()


def finish(ob, packed, latent, rotkey, o_mixed, o_latent, o_rotkey):
    v = packed[...]
    both = jnp.concatenate([v, pltpu.roll(v, ob, 1)], axis=0)
    o_mixed[...] = both[:, :ob].astype(BF16)
    o_latent[...] = latent[...]
    o_rotkey[...] = rotkey[...]


def body(nz, nx, nc, nt, *args):
    args = list(args)
    ncol = nx * nc
    pf = FEATS * ncol
    rows = SEQS * nz
    batch = rows * ncol
    lq = LATENT // nt
    nslot = nz * SLOTS
    hl = 2 * (batch // nt)
    aw = QW + lq + 128
    for i in (1, 12):
        args[i] = args[i].reshape(nz, pf)
    args[5] = args[5].reshape(1, LATENT)
    args[13], args[14] = args[13].T, args[14].T
    half = HEAD_ROT // 2
    frequency = THETA_BASE ** (-np.arange(half, dtype=np.float64) / half)
    angles = frequency.astype(np.float32)[:, None] * np.arange(CACHE, dtype=np.float32)[None, :]
    trig = jnp.asarray(np.stack([np.cos(angles.astype(np.float64)), np.sin(angles.astype(np.float64))]).astype(np.float32))
    freq = jnp.asarray(np.tile(frequency.astype(np.float32), 128 // half)[None, :])
    vm = pltpu.VMEM
    scratch = [
        vm((ncol, FEATS, QW + lq + batch), BF16),
        vm((ncol, FEATS, nt * HV + 3 * HIDDEN), BF16),
        vm((128, pf), BF16),
        vm((nz, pf), F32), vm((nz, pf), F32), vm((1, LATENT), F32), vm((1, 128), F32),
        vm((LATENT, LOCAL_HEADS * HEAD_KEY), BF16), vm((LATENT, HV), BF16),
        vm((SEQS, CACHE, LATENT), BF16), vm((SEQS, HEAD_ROT, CACHE), BF16),
        pltpu.SMEM((SEQS,), jnp.int32),
        vm((4, batch), jnp.int32), vm((4, batch), F32),
        vm((pf * nz, 2 * HIDDEN), BF16), vm((HIDDEN, pf * nz), BF16),
        vm((2, half, CACHE), F32),
        vm((nz, SEQS, aw), F32), vm((nz, SEQS, aw), F32),
        vm((nt, SEQS, lq), F32),
        vm((SEQS, HV), F32),
        vm((nz, SEQS, HV), F32),
        vm((ncol * nt, SEQS * nz // nt, pf), F32),
        vm((nz, SEQS, 2 * HIDDEN + 128), F32), vm((nz, SEQS, 2 * HIDDEN + 128), F32),
        vm((nz, SLOTS, pf), BF16), vm((nz, SLOTS, pf), BF16),
        vm((nz, SLOTS, pf), BF16), vm((nz, SLOTS, pf), BF16),
        vm((nz, SEQS, HIDDEN), F32),
        vm((ncol, nt, FEATS // 2, hl), F32), vm((ncol * nt, FEATS // 2, hl), F32),
        vm((LATENT + 256, QW), BF16),
        vm((SEQS, HEAD_ROT, CACHE), F32),
        vm((nslot, batch), BF16),
        vm((2 * nslot, batch), BF16),
        vm((rows, pf), F32),
        vm((SEQS * nz // nt, nt * HV), F32),
        vm((rows, HIDDEN), F32),
        vm((rows, aw), F32),
        vm((rows, 2 * HIDDEN + 128), F32),
        pltpu.SemaphoreType.DMA((25,)),
        pltpu.SemaphoreType.DMA((13,)),
        pltpu.SemaphoreType.DMA((13,)),
        pltpu.SemaphoreType.REGULAR((2,)),
    ]
    anywhere = pl.BlockSpec(memory_space=pltpu.HBM)
    packed, latent, rotkey = pl.pallas_call(
        functools.partial(kernel, nz, nx, nc, nt),
        out_shape=(
            jax.ShapeDtypeStruct((FEATS // 2, hl), F32),
            jax.ShapeDtypeStruct((SEQS, LATENT), BF16),
            jax.ShapeDtypeStruct((SEQS, HEAD_ROT), BF16),
        ),
        in_specs=[anywhere] * 23,
        out_specs=(pl.BlockSpec(memory_space=pltpu.VMEM),) * 3,
        scratch_shapes=scratch,
        compiler_params=pltpu.CompilerParams(collective_id=0, has_side_effects=True, vmem_limit_bytes=67043328),
        name="layer",
    )(*args, trig, freq)
    vmem = pl.BlockSpec(memory_space=pltpu.VMEM)
    return pl.pallas_call(
        functools.partial(finish, hl // 2),
        out_shape=(
            jax.ShapeDtypeStruct((FEATS, hl // 2), BF16),
            jax.ShapeDtypeStruct((SEQS, LATENT), BF16),
            jax.ShapeDtypeStruct((SEQS, HEAD_ROT), BF16),
        ),
        in_specs=[vmem] * 3,
        out_specs=(vmem,) * 3,
        name="finish",
    )(packed, latent, rotkey)


EP = ("z", "x", "c")


def build(devices):
    split = Mesh(devices, ("z", "x", "c", "y"))
    return jax.shard_map(
        functools.partial(body, *devices.shape),
        mesh=split,
        in_specs=(
            P(EP, None),
            P(),
            P(EP, "y"),
            P(EP, None),
            P(),
            P(),
            P(None, "y"),
            P(None, "y"),
            P(EP, None),
            P(EP, None, None),
            P(EP, None, None),
            P(EP),
            P(),
            P(),
            P(),
            P(EP, None, "y"),
            P(EP, None, "y"),
            P(EP, "y", None),
            P(EP, "y"),
            P(EP, "y"),
            P(EP, "y"),
        ),
        out_specs=(P(EP, "y"), P(EP, None), P(EP, None)),
        check_vma=False,
    )


def solution(mesh):
    return build(mesh.devices.reshape(16, 4, 2, mesh.shape["tp"]))
```

```python
import functools

import jax
import jax.numpy as jnp
import numpy as np
from jax import lax
from jax.experimental import pallas as pl
from jax.experimental.pallas import tpu as pltpu
from jax.sharding import Mesh
from jax.sharding import PartitionSpec as P

MESH = pl.DeviceIdType.MESH
F32 = jnp.float32
BF16 = jnp.bfloat16
HIGHEST = lax.Precision.HIGHEST
NN = (((1,), (0,)), ((), ()))
NT = (((1,), (1,)), ((), ()))
TN = (((0,), (0,)), ((), ()))

LOCAL_HEADS = 4
HEAD_KEY = 64
HEAD_ROT = 32
HEAD_VAL = 64
PER_HEAD = HEAD_KEY + HEAD_ROT
LATENT = 512
CACHE = 1024
HIDDEN = 128
SLOTS = 16
FEATS = 16
SEQS = 2
EPSILON = 1e-06
THETA_BASE = 10000.0
ROUTED_SCALE = 2.5
QW = LOCAL_HEADS * PER_HEAD
HV = LOCAL_HEADS * HEAD_VAL


def dot(a, b, dims=NN, precision=None):
    return lax.dot_general(a, b, dims, precision=precision, preferred_element_type=F32)


def iota(shape, axis):
    return lax.broadcasted_iota(jnp.int32, shape, axis)


def ones_where(mask, dtype=BF16):
    return jnp.where(mask, 1.0, 0.0).astype(dtype)


def rounded(v):
    return v.astype(BF16).astype(F32)


def log2(n):
    return n.bit_length() - 1


def kernel(nz, nx, nc, nt, *refs):
    (
        hidden, attn_gain, w_query, w_latent, w_rotkey, latent_gain, w_key_up, w_value_up, w_attn_out, cache_latent, cache_rotkey,
        lengths, ffn_gain, route_ids, route_scores, w_exp_gate, w_exp_up, w_exp_down, w_shared_gate, w_shared_up, w_shared_out,
        trig, freq,
        o_mixed, o_latent, o_rotkey,
        crit, so, bgs, aoc, sgc, hc, rotw, again, fgain, lgain, fr, keyup, valup, cache, crot, lens, ids, scores, wgu, wd, trg,
        za_s, za_r, yb, ha, mz, sh_s, sh_r, tk_s, tk_r, zh_s, zh_r, zs, pd_s, pd_r,
        ka, krot, sel_p, wt, h16, s32, pall, sp, gp, tot0,
        lsem, ssem, rsem, ok,
    ) = refs
    ncol = nx * nc
    pf = FEATS * ncol
    rows = SEQS * nz
    batch = rows * ncol
    width = pf * nz
    lq = LATENT // nt
    nslot = nz * SLOTS
    ob = batch // nt
    hl = 2 * ob
    hb = batch // 2
    zy = nz // nt
    tok = ncol * SEQS
    cf = FEATS * zy
    npl = ncol * nt
    z, x, c, y = (lax.axis_index(a) for a in ("z", "x", "c", "y"))
    col = x * nc + c
    place_of = col * nt + y
    y_to = lax.div(z, zy)
    spot = lax.rem(z, zy) * nt + y

    def xdev(p):
        return {"x": lax.div(p, nc), "c": lax.rem(p, nc)}

    z_order = sorted(range(1, nz), key=lambda d: -min(d, nz - d))
    z_peers = [lax.rem(z + d, nz) for d in z_order]
    x_order = sorted(range(1, ncol), key=lambda d: -min(d, ncol - d))
    x_peers = [lax.rem(col + d, ncol) for d in x_order]
    y_peers = [lax.rem(y + d, nt) for d in range(1, nt)]
    plane_order = sorted(
        [(dx, dc, dy) for dx in range(nx) for dc in range(nc) for dy in range(nt) if dx or dc or dy],
        key=lambda t: -(min(t[0], nx - t[0]) + min(t[2], nt - t[2])),
    )
    plane_peers = [
        {"x": lax.rem(x + dx, nx), "c": lax.rem(c + dc, nc), "y": lax.rem(y + dy, nt)} for dx, dc, dy in plane_order
    ]

    bar = pltpu.get_barrier_semaphore()

    def signal(sem, dev):
        pl.semaphore_signal(sem, inc=1, device_id=dev, device_id_type=MESH)

    for d in range(nx - 1, 0, -1):
        signal(bar, {"x": lax.rem(x + d, nx), "c": 0})

    @pl.when(c == 1)
    def _():
        signal(bar, {"c": 0})

    def loads(sem, pairs):
        copies = [pltpu.make_async_copy(s, d, lsem.at[sem + i]) for i, (s, d) in enumerate(pairs)]
        for cp in copies:
            cp.start()
        return copies

    def done(copies):
        for cp in copies:
            cp.wait()

    own_lq = pl.ds(pl.multiple_of(y * lq, lq), lq)
    own_hv = pl.ds(pl.multiple_of(y * HV, HV), HV)
    own_pf = pl.ds(pl.multiple_of(z * pf, pf), pf)
    half = HEAD_ROT // 2
    l_crit = loads(0, [
        (w_query, crit.at[col, :, pl.ds(0, QW)]),
        (w_latent.at[:, own_lq], crit.at[col, :, pl.ds(QW, lq)]),
        (hidden, crit.at[col, :, pl.ds(QW + lq, batch)]),
    ])

    for p in z_peers:
        signal(bar, {"z": p, "c": 1})
    for p in y_peers:
        signal(bar, {"y": p, "c": 1})

    def send(src, dst, k, dev):
        cp = pltpu.make_async_remote_copy(
            src_ref=src, dst_ref=dst, send_sem=ssem.at[k], recv_sem=rsem.at[k], device_id=dev, device_id_type=MESH
        )
        cp.start()

    def take(part, sem):
        pltpu.make_async_copy(part, part, sem).wait()

    def arrived(buf, n, k):
        take(buf.at[pl.ds(0, n)], rsem.at[k])

    pending, late = [], []

    def sent(buf, n, k):
        pending.append((buf, n, k))

    done(l_crit)

    @pl.when(c == 0)
    def _():
        pl.semaphore_wait(bar, nc * nx - 1)
        signal(ok.at[0], {"c": 1})

    @pl.when(c == 1)
    def _():
        pl.semaphore_wait(ok.at[0], 1)

    for p in x_peers:
        send(crit.at[col], crit.at[col], 0, xdev(p))
    sent(crit, ncol - 1, 0)
    l_rot = loads(3, [
        (w_rotkey.at[:, own_pf], rotw.at[pl.ds(0, HEAD_ROT)]),
        (w_rotkey.at[pl.ds(half, half), own_pf], rotw.at[pl.ds(64, half)]),
        (w_rotkey.at[pl.ds(0, half), own_pf], rotw.at[pl.ds(64 + half, half)]),
        (attn_gain, again),
        (ffn_gain, fgain),
        (latent_gain, lgain),
        (freq, fr),
        (lengths, lens),
    ])
    l_tab = loads(11, [
        (w_key_up, keyup), (cache_rotkey, crot), (trig, trg), (route_ids, ids), (route_scores, scores),
    ])
    l_att = loads(16, [(cache_latent, cache), (w_value_up, valup)])
    l_bg = loads(18, [
        (w_attn_out.at[:, own_hv], bgs.at[:, pl.ds(0, HV)]),
        (w_shared_gate, bgs.at[:, pl.ds(HV, HIDDEN)]),
        (w_shared_up, bgs.at[:, pl.ds(HV + HIDDEN, HIDDEN)]),
        (w_shared_out, so.at[col]),
    ])
    l_exp = loads(22, [(w_exp_down.at[0], wd)])
    for i in range(ncol):
        pltpu.make_async_copy(w_exp_gate.at[:, i], wgu.at[i, :, :, pl.ds(0, HIDDEN)], lsem.at[23]).start()
        pltpu.make_async_copy(w_exp_up.at[:, i], wgu.at[i, :, :, pl.ds(HIDDEN, HIDDEN)], lsem.at[23]).start()
    l_gu = pltpu.make_async_copy(wgu, wgu, lsem.at[23])

    done(l_rot)
    done(l_tab)
    cos_t, sin_t = trg[0], trg[1]
    for s in range(SEQS):
        low = crot[s, pl.ds(0, half), :].astype(F32)
        high = crot[s, pl.ds(half, half), :].astype(F32)
        krot[s, pl.ds(0, half), :] = low * cos_t - high * sin_t
        krot[s, pl.ds(half, half), :] = low * sin_t + high * cos_t
    spread_r = iota((LOCAL_HEADS * HEAD_KEY, QW), 0)
    spread = ones_where(iota((LOCAL_HEADS * HEAD_KEY, QW), 1) == spread_r + HEAD_ROT * (spread_r >> log2(HEAD_KEY)))
    ka[pl.ds(0, LATENT), :] = dot(keyup[...], spread).astype(BF16)
    lane_q = iota((256, QW), 1)
    head_q = ones_where(lane_q >= PER_HEAD, jnp.int32)
    for h in range(2, LOCAL_HEADS):
        head_q = head_q + ones_where(lane_q >= h * PER_HEAD, jnp.int32)
    within = lane_q - PER_HEAD * head_q - HEAD_KEY
    row_q = iota((256, QW), 0)
    want = jnp.where(row_q < 128, row_q, (row_q - 128) ^ half)
    limit = jnp.where(row_q < 128, row_q, row_q - 128)
    ka[pl.ds(LATENT, 256), :] = ones_where((within == want) & (limit < HEAD_ROT))
    rot_rows = iota((128, pf), 0)
    rot_w = jnp.where((rot_rows & 63) < HEAD_ROT, rotw[...].astype(F32), 0.0).astype(BF16)

    @pl.when(c == 1)
    def _():
        pl.semaphore_wait(bar, nc * (nz - 1) + nc * (nt - 1))
        signal(ok.at[1], {"c": 0})
        for p in y_peers:
            for core in range(nc):
                signal(ok.at[2], {"y": p, "c": core})

    arrived(crit, ncol - 1, 0)
    r_i, b_i = iota((rows, batch), 0), iota((rows, batch), 1)
    sel_a = ones_where(b_i == (r_i >> 1) * tok + col * SEQS + (r_i & 1))
    hid = crit[:, :, pl.ds(QW + lq, batch)].reshape(pf, batch)
    h_t = dot(sel_a, hid, NT)
    scaled = (h_t * again[pl.ds(z, 1), :]).astype(BF16)
    main = dot(scaled, crit[:, :, pl.ds(0, QW + lq)].reshape(pf, QW + lq))
    rot = dot(scaled, rot_w, NT)
    square = jnp.sum(h_t * h_t, axis=1, keepdims=True)
    rot = jnp.where(iota((rows, 128), 1) == HEAD_ROT, square, rot)
    aw = QW + lq + 128
    pall[:, pl.ds(0, QW + lq)] = main
    pall[:, pl.ds(QW + lq, 128)] = rot
    for i in range(nz):
        za_s[i] = pall[pl.ds(SEQS * i, SEQS), :]

    @pl.when(c == 0)
    def _():
        pl.semaphore_wait(ok.at[1], 1)

    for p in z_peers:
        send(za_s.at[p], za_r.at[z], 2, {"z": p})
    sent(za_s, nz - 1, 2)
    za_r[pl.ds(z, 1)] = za_s[pl.ds(z, 1)]
    pl.semaphore_wait(ok.at[2], nt - 1)
    done(l_bg)

    def chunk_send(src, dst, k):
        for p in z_peers:
            send(src, dst.at[spot], k, {"z": p, "y": y_to})

        @pl.when(y_to == y)
        def _():
            dst[pl.ds(spot, 1)] = src[...].reshape(1, FEATS, HV)

        @pl.when(y_to != y)
        def _():
            send(src, dst.at[spot], k, {"y": y_to})

        def wait(sems, _):
            @pl.when(y_to == y)
            def _():
                take(dst.at[pl.ds(0, nz - 1)], sems.at[k])

            @pl.when(y_to != y)
            def _():
                take(dst.at[pl.ds(0, nz)], sems.at[k])

        late.append((k, wait))
        return wait

    wait_ao = chunk_send(bgs.at[:, pl.ds(0, HV)], aoc, 1)
    hzs = nz // 2

    @pl.when(y_to == y)
    def _():
        for p in z_peers:
            lanes = pl.ds(pl.multiple_of(QW + lq + lax.div(p, hzs) * hb, hb), hb)
            send(crit.at[col, :, lanes], hc.at[lax.rem(z, zy)], 3, {"z": p})
        own = pl.ds(pl.multiple_of(QW + lq + lax.div(z, hzs) * hb, hb), hb)
        hc[pl.ds(lax.rem(z, zy), 1)] = crit[pl.ds(col, 1), :, own]

    def wait_hc(sems, receive):
        @pl.when(y_to == y)
        def _():
            if receive:
                if zy > 1:
                    take(hc.at[pl.ds(0, zy - 1)], sems.at[3])
            else:
                take(aoc.at[pl.ds(0, nz - 1), :, pl.ds(0, hb)], sems.at[3])

        if receive:

            @pl.when(y_to != y)
            def _():
                take(hc.at[pl.ds(0, zy)], sems.at[3])

    late.append((3, wait_hc))
    for p in x_peers:
        send(so.at[col], so.at[col], 4, xdev(p))
    sent(so, ncol - 1, 4)

    arrived(za_r, nz - 1, 2)
    tot = za_r[0]
    for i in range(1, nz):
        tot = tot + za_r[i]
    lane2 = iota((SEQS, 128), 1)
    tail = tot[:, QW + lq : aw]
    sq = jnp.sum(jnp.where(lane2 == HEAD_ROT, tail, 0.0), axis=1, keepdims=True)
    scale = lax.rsqrt(sq / width + EPSILON)
    yb[pl.ds(y, 1)] = rounded(tot[:, QW : QW + lq] * scale).reshape(1, SEQS, lq)
    for p in y_peers:
        send(yb.at[y], yb.at[y], 5, {"y": p})
    sent(yb, nt - 1, 5)
    wait_sg = chunk_send(bgs.at[:, pl.ds(HV, HV)], sgc, 6)
    q = rounded(tot[:, :QW] * scale)
    nrows = SEQS * LOCAL_HEADS
    r8 = iota((nrows, 128), 0)
    first8 = r8 < LOCAL_HEADS

    def per_row(v):
        top = iota((nrows, v.shape[1]), 0) < LOCAL_HEADS
        return jnp.where(top, v[0:1, :], v[1:2, :])

    lane_8 = iota((nrows, QW), 1)
    first = (iota((nrows, QW), 0) & (LOCAL_HEADS - 1)) * PER_HEAD
    q8 = jnp.where((lane_8 >= first) & (lane_8 < first + PER_HEAD), per_row(q), 0.0).astype(BF16)
    qa = dot(q8, ka[...], NT)
    absorbed = qa[:, :LATENT].astype(BF16)
    len8 = jnp.where(first8, lens[0], lens[1])
    angle = len8.astype(F32) * fr[...]
    cos8 = jnp.cos(angle)
    lane8 = iota((nrows, 128), 1)
    sin8 = jnp.where((lane8 & half) == 0, -jnp.sin(angle), jnp.sin(angle))
    q_rot = qa[:, LATENT : LATENT + 128] * cos8 + qa[:, LATENT + 128 : LATENT + 256] * sin8

    done(l_att)
    q32 = q_rot[:, :HEAD_ROT]
    per_seq = [dot(absorbed, cache[s], NT) + dot(q32, krot[s], NN, HIGHEST) for s in range(SEQS)]
    top_rows = iota((nrows, CACHE), 0) < LOCAL_HEADS
    score_scale = PER_HEAD**-0.5
    live = iota((nrows, CACHE), 1) < jnp.where(top_rows, lens[0], lens[1])
    cache_score = jnp.where(live, score_scale * jnp.where(top_rows, per_seq[0], per_seq[1]), -1e30)
    best = jnp.max(cache_score, axis=1, keepdims=True)

    new_rot = rounded(tail * scale)
    o_rotkey[...] = new_rot[:, :HEAD_ROT].astype(BF16)
    new_swap = pltpu.roll(new_rot, 64, 1)
    own_rot = jnp.where(lane8 < HEAD_ROT, per_row(new_rot) * cos8 + per_row(new_swap) * sin8, 0.0)

    arrived(yb, nt - 1, 5)
    raw = jnp.concatenate([yb[i] for i in range(nt)], axis=1)
    new_latent = (
        raw * lax.rsqrt(jnp.mean(raw * raw, axis=1, keepdims=True) + EPSILON) * lgain[...]
    ).astype(BF16)
    o_latent[...] = new_latent
    lat8 = per_row(new_latent.astype(F32))
    own_score = score_scale * (
        jnp.sum(absorbed.astype(F32) * lat8, axis=1, keepdims=True)
        + jnp.sum(q_rot * own_rot, axis=1, keepdims=True)
    )
    top_score = jnp.maximum(best, own_score)
    cache_weight = jnp.exp(cache_score - top_score)
    own_weight = jnp.exp(own_score - top_score)
    denominator = jnp.sum(cache_weight, axis=1, keepdims=True) + own_weight
    prob = (cache_weight / denominator).astype(BF16)
    own_prob = rounded(own_weight / denominator)
    ctx = [dot(prob, cache[s]) for s in range(SEQS)]
    top_rows = iota((nrows, LATENT), 0) < LOCAL_HEADS
    context = jnp.where(top_rows, ctx[0], ctx[1]) + own_prob * lat8
    ho = dot(context.astype(BF16), valup[...])
    r_h = iota((nrows, HV), 0)
    ho = jnp.where((iota((nrows, HV), 1) >> log2(HEAD_VAL)) == (r_h & (LOCAL_HEADS - 1)), ho, 0.0)
    h0 = jnp.sum(jnp.where(r_h < LOCAL_HEADS, ho, 0.0), axis=0, keepdims=True)
    h1 = jnp.sum(jnp.where(r_h < LOCAL_HEADS, 0.0, ho), axis=0, keepdims=True)
    heads = rounded(jnp.where(iota((SEQS, HV), 0) == 0, h0, h1))
    ha[pl.ds(place_of, 1)] = heads.reshape(1, SEQS, HV)
    for dev in plane_peers:
        send(ha.at[place_of], ha.at[place_of], 7, dev)
    sent(ha, npl - 1, 7)

    wait_hc(rsem, True)
    t_i, l_i = iota((tok, hb), 0), iota((tok, hb), 1)
    sel_h = ones_where(l_i == lax.rem(z, hzs) * tok + t_i)
    hcv = hc[...].reshape(cf, hb)
    hid_c = dot(sel_h, jnp.concatenate([hcv, hcv], axis=0), NT)
    rs = scores[...]
    rw = ROUTED_SCALE * rs / jnp.sum(rs, axis=0, keepdims=True)
    idv = ids[...]
    nex = nz + ncol
    which = iota((nex, batch), 0)
    target = jnp.where(which < nz, which * ncol + col, z * ncol + which - nz)
    hit = jnp.zeros((nex, batch), F32)
    wgt = jnp.zeros((nex, batch), F32)
    for k in range(4):
        same = idv[k : k + 1, :] == target
        hit = jnp.where(same, 1.0, hit)
        wgt = jnp.where(same, rw[k : k + 1, :], wgt)
    before = ones_where(iota((batch, batch), 0) < iota((batch, batch), 1))
    rank = dot(hit.astype(BF16), before)
    val = jnp.where(hit > 0.0, rank, -1.0).astype(BF16)
    pslot = ncol * SLOTS
    expand_p = ones_where(iota((pslot, nex), 1) == nz + (iota((pslot, nex), 0) >> log2(SLOTS)))
    sel_p[...] = ones_where(dot(expand_p, val) == (iota((pslot, batch), 0) & (SLOTS - 1)).astype(F32))

    gain_rows = jnp.broadcast_to(fgain[...][:, None, :], (nz, ncol, pf)).reshape(nz * ncol, pf)
    gr = iota((nz * ncol, pf), 0)
    gain_rows = jnp.where((iota((nz * ncol, pf), 1) >> log2(FEATS)) == (gr & (ncol - 1)), gain_rows, 0.0)
    tile_f = jnp.where(
        (iota((pf, 2 * cf), 0) & (FEATS - 1)) == (iota((pf, 2 * cf), 1) & (FEATS - 1)), 1.0, 0.0
    )
    tiled = dot(gain_rows, tile_f, NN, HIGHEST).reshape(nz, ncol, 2 * cf)
    lane_z = iota((ncol, 2 * cf), 1) >> log2(FEATS)
    for k in range(nt // 2):
        g = jnp.zeros((ncol, 2 * cf), F32)
        for i in range(2 * zy):
            g = jnp.where(lane_z == i, tiled[2 * zy * k + i], g)
        gp[k] = g

    wait_ao(rsem, True)
    arrived(ha, npl - 1, 7)
    for i in range(ncol):
        for j in range(nt):
            h16[pl.ds(SEQS * i, SEQS), pl.ds(HV * j, HV)] = ha[i * nt + j]
    attn = jnp.zeros((tok, 2 * cf), F32)
    for j in range(nt):
        w = jnp.concatenate([aoc[i * nt + j] for i in range(zy)] * 2, axis=0)
        attn = attn + dot(h16[:, pl.ds(HV * j, HV)].astype(BF16), w, NT)
    mine = (iota((tok, 2 * cf), 1) >> log2(cf)) == (y & 1)
    mid = jnp.where(mine, rounded(hid_c + rounded(attn)), 0.0)
    mz[pl.ds(z, 1)] = mid.astype(BF16).reshape(1, tok, 2 * cf)
    for p in z_peers:
        send(mz.at[z], mz.at[z], 8, {"z": p})
    sent(mz, nz - 1, 8)

    ffn = (mid * gp[pl.ds(y >> 1, 1), pl.ds(col, 1)].reshape(1, 2 * cf)).astype(BF16)
    square = jnp.broadcast_to(jnp.sum(mid * mid, axis=1, keepdims=True), (tok, 128))
    wait_sg(rsem, True)
    for j in range(nt):
        w = jnp.concatenate([sgc[i * nt + j] for i in range(zy)] * 2, axis=0)
        sp[:, pl.ds(0, 2 * HIDDEN)] = dot(ffn, w)
        sp[:, pl.ds(2 * HIDDEN, 128)] = square
        for i in range(ncol):
            sh_s[i * nt + j] = sp[pl.ds(SEQS * i, SEQS), :]
    for dev in plane_peers:
        send(sh_s.at[(dev["x"] * nc + dev["c"]) * nt + dev["y"]], sh_r.at[place_of], 9, dev)
    sent(sh_s, npl - 1, 9)
    sh_r[pl.ds(place_of, 1)] = sh_s[pl.ds(place_of, 1)]

    expand = ones_where(iota((nslot, nex), 1) == (iota((nslot, nex), 0) >> log2(SLOTS)))
    slot_i = (iota((nslot, batch), 0) & (SLOTS - 1)).astype(F32)
    in_slot = dot(expand, val) == slot_i
    w_hi = wgt.astype(BF16)
    w_lo = (wgt - w_hi.astype(F32)).astype(BF16)
    wt[pl.ds(0, nslot), :] = jnp.where(in_slot, dot(expand, w_hi), 0.0).astype(BF16)
    wt[pl.ds(nslot, nslot), :] = jnp.where(in_slot, dot(expand, w_lo), 0.0).astype(BF16)
    arrived(mz, nz - 1, 8)
    mid_all = mz[...].reshape(batch, 2 * cf)
    tk_s[...] = dot(sel_p[...], mid_all).astype(BF16).reshape(ncol, SLOTS, 2 * cf)
    for dev in plane_peers:
        send(tk_s.at[dev["x"] * nc + dev["c"]], tk_r.at[place_of], 10, dev)
    sent(tk_r, npl - 1, 10)
    tk_r[pl.ds(place_of, 1)] = tk_s[pl.ds(col, 1)]
    f_i, l_i = iota((pf, 2 * cf), 0), iota((pf, 2 * cf), 1)
    own_f = (f_i >> log2(FEATS) == col) & (l_i == (z & (2 * zy - 1)) * FEATS + (f_i & (FEATS - 1))) & (y_to == y)
    tot0[...] = dot(ones_where(own_f), mid_all, NT)

    arrived(sh_r, npl - 1, 9)
    tot = sh_r[0]
    for i in range(1, npl):
        tot = tot + sh_r[i]
    scale = lax.rsqrt(tot[:, 2 * HIDDEN : 2 * HIDDEN + 1] / width + EPSILON)
    gate = scale * tot[:, :HIDDEN]
    act = rounded(gate / (1.0 + jnp.exp(-gate)) * (scale * tot[:, HIDDEN : 2 * HIDDEN]))
    zs[pl.ds(z, 1)] = act.reshape(1, SEQS, HIDDEN)
    for p in z_peers:
        send(zs.at[z], zs.at[z], 11, {"z": p})
    sent(zs, nz - 1, 11)

    done(l_exp)
    done([l_gu])
    arrived(tk_r, npl - 1, 10)
    pieces = []
    sq = jnp.zeros((SLOTS, 2 * cf), F32)
    for i in range(ncol):
        for k in range(nt // 2):
            v = tk_r[i * nt + 2 * k].astype(F32) + tk_r[i * nt + 2 * k + 1].astype(F32)
            sq = sq + v * v
            pieces.append((v * gp[k, pl.ds(i, 1), :]).astype(BF16))
    gu = dot(jnp.concatenate(pieces, axis=1), wgu[...].reshape(width, 2 * HIDDEN))
    scale = lax.rsqrt(jnp.sum(sq, axis=1, keepdims=True) / width + EPSILON)
    gate = scale * gu[:, :HIDDEN]
    act = (gate / (1.0 + jnp.exp(-gate)) * (scale * gu[:, HIDDEN:])).astype(BF16)
    out = dot(act, wd[...])
    for i in range(nz):
        zh_s[i] = out[:, pf * i : pf * (i + 1)].astype(BF16)
    for p in z_peers:
        send(zh_s.at[p], zh_r.at[z], 12, {"z": p})
    sent(zh_s, nz - 1, 12)
    zh_r[pl.ds(z, 1)] = zh_s[pl.ds(z, 1)]

    arrived(so, ncol - 1, 4)
    arrived(zs, nz - 1, 11)
    for i in range(nz):
        s32[pl.ds(SEQS * i, SEQS), :] = zs[i]
    b_i, r_i = iota((batch, rows), 0), iota((batch, rows), 1)
    place = ones_where(b_i == (r_i >> 1) * tok + col * SEQS + (r_i & 1))
    spread_act = dot(place, s32[...].astype(BF16)).astype(BF16)
    total = tot0[...] + dot(so[...].reshape(pf, HIDDEN), spread_act, NT)
    arrived(zh_r, nz - 1, 12)
    parts = zh_r[...].reshape(nslot, pf)
    total = total + dot(parts, wt[pl.ds(0, nslot), :], TN) + dot(parts, wt[pl.ds(nslot, nslot), :], TN)
    total = total.reshape(ncol, 2, FEATS // 2, batch)
    low_lane = iota((ncol, FEATS // 2, hl), 2) < ob
    for k in range(nt // 2):
        ta = total[:, 0, :, hl * k : hl * (k + 1)]
        tb = total[:, 1, :, hl * k : hl * (k + 1)]
        flat = (ncol * FEATS // 2, hl)
        ra = pltpu.roll(ta.reshape(flat), ob, 1).reshape(ta.shape)
        rb = pltpu.roll(tb.reshape(flat), ob, 1).reshape(tb.shape)
        pd_s[:, 2 * k] = jnp.where(low_lane, ta, rb)
        pd_s[:, 2 * k + 1] = jnp.where(low_lane, ra, tb)
    for dev in plane_peers:
        send(pd_s.at[dev["x"] * nc + dev["c"], dev["y"]], pd_r.at[place_of], 13, dev)
    sent(pd_r, npl - 1, 13)
    pd_r[pl.ds(place_of, 1)] = pd_s[pl.ds(col, 1), pl.ds(y, 1)].reshape(1, FEATS // 2, hl)
    arrived(pd_r, npl - 1, 13)
    tot = pd_r[0]
    for i in range(1, npl):
        tot = tot + pd_r[i]
    both = jnp.concatenate([tot, pltpu.roll(tot, ob, 1)], axis=0)
    o_mixed[...] = both[:, :ob].astype(BF16)

    for k, f in late:
        f(ssem, False)
    for buf, n, k in pending:
        take(buf.at[pl.ds(0, n)], ssem.at[k])


def finish(*refs):
    copies = [pltpu.make_async_copy(refs[i], refs[3 + i], refs[6].at[i]) for i in range(3)]
    for cp in copies:
        cp.start()
    for cp in copies:
        cp.wait()


def body(nz, nx, nc, nt, *args):
    args = list(args)
    ncol = nx * nc
    pf = FEATS * ncol
    rows = SEQS * nz
    batch = rows * ncol
    lq = LATENT // nt
    nslot = nz * SLOTS
    hl = 2 * (batch // nt)
    aw = QW + lq + 128
    for i in (1, 12):
        args[i] = args[i].reshape(nz, pf)
    args[5] = args[5].reshape(1, LATENT)
    args[13], args[14] = args[13].T, args[14].T
    for i in (15, 16):
        args[i] = args[i].reshape(nz, ncol, FEATS, HIDDEN)
    half = HEAD_ROT // 2
    frequency = THETA_BASE ** (-np.arange(half, dtype=np.float64) / half)
    angles = frequency.astype(np.float32)[:, None] * np.arange(CACHE, dtype=np.float32)[None, :]
    trig = jnp.asarray(np.stack([np.cos(angles.astype(np.float64)), np.sin(angles.astype(np.float64))]).astype(np.float32))
    freq = jnp.asarray(np.tile(frequency.astype(np.float32), 128 // half)[None, :])
    vm = pltpu.VMEM
    tok = ncol * SEQS
    cf = FEATS * nz // nt
    npl = ncol * nt
    scratch = [
        vm((ncol, FEATS, QW + lq + batch), BF16),
        vm((ncol, FEATS, HIDDEN), BF16),
        vm((FEATS, 2 * HV), BF16),
        vm((nz, FEATS, HV), BF16), vm((nz, FEATS, HV), BF16),
        vm((nz // nt, FEATS, batch // 2), BF16),
        vm((128, pf), BF16),
        vm((nz, pf), F32), vm((nz, pf), F32), vm((1, LATENT), F32), vm((1, 128), F32),
        vm((LATENT, LOCAL_HEADS * HEAD_KEY), BF16), vm((LATENT, HV), BF16),
        vm((SEQS, CACHE, LATENT), BF16), vm((SEQS, HEAD_ROT, CACHE), BF16),
        pltpu.SMEM((SEQS,), jnp.int32),
        vm((4, batch), jnp.int32), vm((4, batch), F32),
        vm((ncol, nz, FEATS, 2 * HIDDEN), BF16), vm((HIDDEN, pf * nz), BF16),
        vm((2, half, CACHE), F32),
        vm((nz, SEQS, aw), F32), vm((nz, SEQS, aw), F32),
        vm((nt, SEQS, lq), F32),
        vm((npl, SEQS, HV), F32),
        vm((nz, tok, 2 * cf), BF16),
        vm((npl, SEQS, 2 * HIDDEN + 128), F32), vm((npl, SEQS, 2 * HIDDEN + 128), F32),
        vm((ncol, SLOTS, 2 * cf), BF16), vm((npl, SLOTS, 2 * cf), BF16),
        vm((nz, SLOTS, pf), BF16), vm((nz, SLOTS, pf), BF16),
        vm((nz, SEQS, HIDDEN), F32),
        vm((ncol, nt, FEATS // 2, hl), F32), vm((npl, FEATS // 2, hl), F32),
        vm((LATENT + 256, QW), BF16),
        vm((SEQS, HEAD_ROT, CACHE), F32),
        vm((ncol * SLOTS, batch), BF16),
        vm((2 * nslot, batch), BF16),
        vm((tok, nt * HV), F32),
        vm((rows, HIDDEN), F32),
        vm((rows, aw), F32),
        vm((tok, 2 * HIDDEN + 128), F32),
        vm((nt // 2, ncol, 2 * cf), F32),
        vm((pf, batch), F32),
        pltpu.SemaphoreType.DMA((24,)),
        pltpu.SemaphoreType.DMA((14,)),
        pltpu.SemaphoreType.DMA((14,)),
        pltpu.SemaphoreType.REGULAR((3,)),
    ]
    anywhere = pl.BlockSpec(memory_space=pltpu.HBM)
    results = pl.pallas_call(
        functools.partial(kernel, nz, nx, nc, nt),
        out_shape=(
            pltpu.VMEM((FEATS, hl // 2), BF16),
            pltpu.VMEM((SEQS, LATENT), BF16),
            pltpu.VMEM((SEQS, HEAD_ROT), BF16),
        ),
        in_specs=[anywhere] * 23,
        out_specs=(pl.BlockSpec(memory_space=pltpu.VMEM),) * 3,
        scratch_shapes=scratch,
        compiler_params=pltpu.CompilerParams(collective_id=0, has_side_effects=True, vmem_limit_bytes=66977792),
        name="layer",
    )(*args, trig, freq)
    results = [pltpu.with_memory_space_constraint(r, pltpu.VMEM) for r in results]
    return pl.pallas_call(
        finish,
        out_shape=(
            jax.ShapeDtypeStruct((FEATS, hl // 2), BF16),
            jax.ShapeDtypeStruct((SEQS, LATENT), BF16),
            jax.ShapeDtypeStruct((SEQS, HEAD_ROT), BF16),
        ),
        in_specs=[pl.BlockSpec(memory_space=pltpu.VMEM)] * 3,
        out_specs=(anywhere,) * 3,
        scratch_shapes=[pltpu.SemaphoreType.DMA((3,))],
        name="finish",
    )(*results)


EP = ("z", "x", "c")


def build(devices):
    split = Mesh(devices, ("z", "x", "c", "y"))
    return jax.shard_map(
        functools.partial(body, *devices.shape),
        mesh=split,
        in_specs=(
            P(EP, None),
            P(),
            P(EP, "y"),
            P(EP, None),
            P(),
            P(),
            P(None, "y"),
            P(None, "y"),
            P(EP, None),
            P(EP, None, None),
            P(EP, None, None),
            P(EP),
            P(),
            P(),
            P(),
            P(EP, None, "y"),
            P(EP, None, "y"),
            P(EP, "y", None),
            P(EP, "y"),
            P(EP, "y"),
            P(EP, "y"),
        ),
        out_specs=(P(EP, "y"), P(EP, None), P(EP, None)),
        check_vma=False,
    )


def solution(mesh):
    return build(mesh.devices.reshape(16, 4, 2, mesh.shape["tp"]))
```

```python
import functools
import math

import jax
import jax.numpy as jnp
import numpy as np
from jax import lax
from jax.experimental import pallas as pl
from jax.experimental.pallas import tpu as pltpu
from jax.sharding import Mesh
from jax.sharding import PartitionSpec as P

MESH = pl.DeviceIdType.MESH
F32 = jnp.float32
BF16 = jnp.bfloat16
HIGHEST = lax.Precision.HIGHEST
NN = (((1,), (0,)), ((), ()))
NT = (((1,), (1,)), ((), ()))
TN = (((0,), (0,)), ((), ()))

LOCAL_HEADS = 4
HEAD_KEY = 64
HEAD_ROT = 32
HEAD_VAL = 64
PER_HEAD = HEAD_KEY + HEAD_ROT
LATENT = 512
CACHE = 1024
HIDDEN = 128
SLOTS = 16
FEATS = 16
SEQS = 2
EPSILON = 1e-06
THETA_BASE = 10000.0
ROUTED_SCALE = 2.5
QW = LOCAL_HEADS * PER_HEAD
HV = LOCAL_HEADS * HEAD_VAL
UNIT = 1024


def dot(a, b, dims=NN, precision=None):
    return lax.dot_general(a, b, dims, precision=precision, preferred_element_type=F32)


def iota(shape, axis):
    return lax.broadcasted_iota(jnp.int32, shape, axis)


def ones_where(mask, dtype=BF16):
    return jnp.where(mask, 1.0, 0.0).astype(dtype)


def rounded(v):
    return v.astype(BF16).astype(F32)


def log2(n):
    return n.bit_length() - 1


def kernel(nz, nx, nc, nt, *refs):
    (
        hidden, attn_gain, w_query, w_latent, w_rotkey, latent_gain, w_key_up, w_value_up, w_attn_out, cache_latent, cache_rotkey,
        lengths, ffn_gain, route_ids, route_scores, w_exp_gate, w_exp_up, w_exp_down, w_shared_gate, w_shared_up, w_shared_out,
        trig, freq,
        o_mixed, o_latent, o_rotkey,
        pack, crit, so, bgs, aoc, sgc, hc, rotw, again, fgain, lgain, fr, keyup, valup, cache, crot, lens, ids, scores, wgu, wd, trg,
        za_s, za_r, zb_r, yb, ha, mz, sh_s, sh_r, tk_s, tk_r, zh_s, zh_r, zs, pd_s, pd_r,
        ka, krot, sel_p, wt, h16, s32, pall, sp, gp, tot0,
        lsem, ssem, rsem, ok, ruler,
    ) = refs
    ncol = nx * nc
    pf = FEATS * ncol
    rows = SEQS * nz
    batch = rows * ncol
    width = pf * nz
    lq = LATENT // nt
    nslot = nz * SLOTS
    ob = batch // nt
    hl = 2 * ob
    wa = 2 * 128
    wb = QW - wa + lq
    zy = nz // nt
    tok = ncol * SEQS
    cf = FEATS * zy
    npl = ncol * nt
    z, x, c, y = (lax.axis_index(a) for a in ("z", "x", "c", "y"))
    col = x * nc + c
    place_of = col * nt + y
    y_to = ((z) >> log2(zy))
    ring = ((z) & (zy - 1))

    def xdev(p):
        return {"x": ((p) >> log2(nc)), "c": ((p) & (nc - 1))}

    z_order = sorted(range(1, nz), key=lambda d: -min(d, nz - d))
    z_peers = [((z + d) & (nz - 1)) for d in z_order]
    x_order = sorted(range(1, ncol), key=lambda d: -min(d, ncol - d))
    x_peers = [((col + d) & (ncol - 1)) for d in x_order]
    y_peers = [((y + d) & (nt - 1)) for d in range(1, nt)]
    plane_order = sorted(
        [(dx, dc, dy) for dx in range(nx) for dc in range(nc) for dy in range(nt) if dx or dc or dy],
        key=lambda t: -(min(t[0], nx - t[0]) + min(t[2], nt - t[2])),
    )
    plane_peers = [
        {"x": ((x + dx) & (nx - 1)), "c": ((c + dc) & (nc - 1)), "y": ((y + dy) & (nt - 1))} for dx, dc, dy in plane_order
    ]

    bar = pltpu.get_barrier_semaphore()

    def signal(sem, dev):
        pl.semaphore_signal(sem, inc=1, device_id=dev, device_id_type=MESH)

    for d in range(nx - 1, 0, -1):
        signal(bar, {"x": ((x + d) & (nx - 1)), "c": 0})

    @pl.when(c == 1)
    def _():
        signal(bar, {"c": 0})

    def nbytes(ref):
        return math.prod(ref.shape) * jnp.dtype(ref.dtype).itemsize

    def rows_of(n):
        assert n % UNIT == 0 and n // UNIT <= ruler.shape[0]
        return ruler.at[pl.ds(0, n // UNIT)]

    def loads(sem, pairs):
        for src, dst in pairs:
            pltpu.make_async_copy(src, dst, lsem.at[sem]).start()
        part = rows_of(sum(nbytes(dst) for _, dst in pairs))
        return [(part, sem)]

    def done(copies):
        for part, sem in copies:
            pltpu.make_async_copy(part, part, lsem.at[sem]).wait()

    own_lq = pl.ds(pl.multiple_of(y * lq, lq), lq)
    own_hv = pl.ds(pl.multiple_of(y * HV, HV), HV)
    own_pf = pl.ds(pl.multiple_of(z * pf, pf), pf)
    half = HEAD_ROT // 2
    l_crit = loads(0, [
        (w_query.at[:, pl.ds(0, wa)], pack.at[0, :, pl.ds(0, wa)]),
        (w_query.at[:, pl.ds(wa, QW - wa)], pack.at[1, :, pl.ds(0, QW - wa)]),
        (w_latent.at[:, own_lq], pack.at[1, :, pl.ds(QW - wa, lq)]),
        (hidden, pack.at[0, :, pl.ds(wa, batch)]),
        (hidden, pack.at[1, :, pl.ds(wb, batch)]),
    ])

    for p in z_peers:
        signal(bar, {"z": p, "c": 1})
    for p in y_peers:
        signal(bar, {"y": p, "c": 1})

    def send(src, dst, k, dev):
        cp = pltpu.make_async_remote_copy(
            src_ref=src, dst_ref=dst, send_sem=ssem.at[0], recv_sem=rsem.at[slot[k]], device_id=dev, device_id_type=MESH
        )
        cp.start()

    def take(part, sem):
        pltpu.make_async_copy(part, part, sem).wait()

    def arrived(buf, n, k):
        take(buf.at[pl.ds(0, n)], rsem.at[slot[k]])

    slot = {0: 0, 1: 1, 3: 1, 6: 1, 2: 2, 14: 2, 5: 3, 7: 4, 15: 5, 17: 5, 16: 6, 4: 6, 8: 7, 9: 8, 10: 9, 11: 10, 12: 11, 13: 12}
    pending = []

    def sent(buf, n):
        pending.append(n * nbytes(buf) // buf.shape[0])

    def take_bytes(n, sem):
        take(rows_of(n), sem)

    done(l_crit)

    @pl.when(c == 0)
    def _():
        pl.semaphore_wait(bar, nc * nx - 1)
        signal(ok.at[0], {"c": 1})

    @pl.when(c == 1)
    def _():
        pl.semaphore_wait(ok.at[0], 1)

    for p in x_peers:
        send(pack.at[((p) & (nc - 1))], crit.at[col], 0, xdev(p))
    sent(crit, ncol - 1)
    crit[pl.ds(col, 1)] = pack[pl.ds(c, 1)]
    l_rot = loads(1, [
        (w_rotkey.at[:, own_pf], rotw.at[pl.ds(0, HEAD_ROT)]),
        (w_rotkey.at[pl.ds(half, half), own_pf], rotw.at[pl.ds(64, half)]),
        (w_rotkey.at[pl.ds(0, half), own_pf], rotw.at[pl.ds(64 + half, half)]),
        (attn_gain, again),
        (ffn_gain, fgain),
        (latent_gain, lgain),
        (w_key_up, keyup), (cache_rotkey, crot), (trig, trg), (route_ids, ids), (route_scores, scores), (freq, fr),
    ])
    l_len = pltpu.make_async_copy(lengths, lens, lsem.at[2])
    l_len.start()
    l_att = loads(3, [(cache_latent, cache), (w_value_up, valup)])
    l_bg = loads(4, [
        (w_attn_out.at[:, own_hv], bgs.at[:, pl.ds(0, HV)]),
        (w_shared_gate, bgs.at[:, pl.ds(HV, HIDDEN)]),
        (w_shared_up, bgs.at[:, pl.ds(HV + HIDDEN, HIDDEN)]),
        (w_shared_out, so.at[col]),
    ])
    l_exp = loads(5, [(w_exp_down.at[0], wd)] + [
        (w.at[:, i], wgu.at[i, :, :, pl.ds(HIDDEN * j, HIDDEN)])
        for i in range(ncol) for j, w in enumerate((w_exp_gate, w_exp_up))
    ])

    done(l_rot)
    l_len.wait()
    cos_t, sin_t = trg[0], trg[1]
    for s in range(SEQS):
        low = crot[s, pl.ds(0, half), :].astype(F32)
        high = crot[s, pl.ds(half, half), :].astype(F32)
        krot[s, pl.ds(0, half), :] = low * cos_t - high * sin_t
        krot[s, pl.ds(half, half), :] = low * sin_t + high * cos_t
    spread_r = iota((LOCAL_HEADS * HEAD_KEY, QW), 0)
    spread = ones_where(iota((LOCAL_HEADS * HEAD_KEY, QW), 1) == spread_r + HEAD_ROT * (spread_r >> log2(HEAD_KEY)))
    ka[pl.ds(0, LATENT), :] = dot(keyup[...], spread).astype(BF16)
    lane_q = iota((256, QW), 1)
    head_q = ones_where(lane_q >= PER_HEAD, jnp.int32)
    for h in range(2, LOCAL_HEADS):
        head_q = head_q + ones_where(lane_q >= h * PER_HEAD, jnp.int32)
    within = lane_q - PER_HEAD * head_q - HEAD_KEY
    row_q = iota((256, QW), 0)
    want = jnp.where(row_q < 128, row_q, (row_q - 128) ^ half)
    limit = jnp.where(row_q < 128, row_q, row_q - 128)
    ka[pl.ds(LATENT, 256), :] = ones_where((within == want) & (limit < HEAD_ROT))
    rot_rows = iota((128, pf), 0)
    rot_w = jnp.where((rot_rows & 63) < HEAD_ROT, rotw[...].astype(F32), 0.0).astype(BF16)

    @pl.when(c == 1)
    def _():
        pl.semaphore_wait(bar, nc * (nz - 1) + nc * (nt - 1))
        signal(ok.at[1], {"c": 0})
        for p in y_peers:
            for core in range(nc):
                signal(ok.at[2], {"y": p, "c": core})

    arrived(crit, ncol - 1, 0)
    r_i, b_i = iota((nc * rows, batch), 0), iota((nc * rows, batch), 1)
    owner = x * nc + (r_i >> log2(rows))
    sel_a = ones_where(b_i == ((r_i & (rows - 1)) >> 1) * tok + owner * SEQS + (r_i & 1))
    hid = crit[:, :, pl.ds(wa, batch)].reshape(pf, batch)
    h_t = dot(sel_a, hid, NT)
    scaled = (h_t * again[pl.ds(z, 1), :]).astype(BF16)
    pall[:, pl.ds(0, wa)] = dot(scaled, crit[:, :, pl.ds(0, wa)].reshape(pf, wa))
    rot = dot(scaled, rot_w, NT)
    square = jnp.sum(h_t * h_t, axis=1, keepdims=True)
    pall[:, pl.ds(wa, 128)] = jnp.where(iota((nc * rows, 128), 1) == HEAD_ROT, square, rot)
    for i in range(nc * nz):
        za_s[i] = pall[pl.ds(SEQS * i, SEQS), :]

    @pl.when(c == 0)
    def _():
        pl.semaphore_wait(ok.at[1], 1)

    zc_peers = [(p, d) for p in z_peers for d in range(nc)] + [(z, 1)]
    for core in range(nc):

        @pl.when(c == core)
        def _():
            lanes = pl.ds(0, wa if core else wa + 128)
            dst = (za_r, zb_r)[core]
            for p, d in zc_peers:
                e = (core + d) % nc
                send(za_s.at[e * nz + p, :, lanes], dst.at[z], 2 + 12 * core, {"z": p, "c": e})
            dst[pl.ds(z, 1)] = za_s[pl.ds(core * nz + z, 1), :, lanes]

    size_a, size_b = nbytes(za_r) // nz, nbytes(zb_r) // nz

    pl.semaphore_wait(ok.at[2], nt - 1)
    done(l_bg)

    groups = sorted(range(nt), key=lambda k: -min(k, nt - k))
    for src, dst, k in ((bgs.at[:, pl.ds(0, HV)], aoc, 1), (bgs.at[:, pl.ds(HV, HV)], sgc, 6)):
        for g in groups:
            dev = {"z": ((z + zy * g) & (nz - 1)), "y": y_to}
            if g:
                send(src, dst.at[ring, y], k, dev)
            else:

                @pl.when(y_to != y)
                def _():
                    send(src, dst.at[ring, y], k, dev)

                @pl.when(y_to == y)
                def _():
                    dst[pl.ds(ring, 1), pl.ds(y, 1)] = src[...].reshape(1, 1, FEATS, HV)

    @pl.when(y_to == y)
    def _():
        for g in groups[:-1]:
            send(pack.at[0, :, pl.ds(wa, batch)], hc.at[ring], 3, {"z": ((z + zy * g) & (nz - 1))})
        hc[pl.ds(ring, 1)] = pack[pl.ds(0, 1), :, pl.ds(wa, batch)]

    for p in x_peers:
        send(so.at[col], so.at[col], 4, xdev(p))
    sent(so, ncol - 1)

    for core in range(nc):

        @pl.when(c == core)
        def _():
            take_bytes((nz - 1 + core) * size_a + (nz - core) * size_b, rsem.at[2])

    tot, tot_b = za_r[0], zb_r[0]
    for i in range(1, nz):
        tot = tot + za_r[i]
        tot_b = tot_b + zb_r[i]
    lane2 = iota((SEQS, 128), 1)
    tail = tot[:, wa:]
    sq = jnp.sum(jnp.where(lane2 == HEAD_ROT, tail, 0.0), axis=1, keepdims=True)
    scale = lax.rsqrt(sq / width + EPSILON)
    yb[pl.ds(y, 1)] = rounded(tot_b[:, QW - wa :] * scale).reshape(1, SEQS, lq)
    for p in y_peers:
        send(yb.at[y], yb.at[y], 5, {"y": p})
    sent(yb, nt - 1)
    q = rounded(jnp.concatenate([tot[:, :wa], tot_b[:, : QW - wa]], axis=1) * scale)
    nrows = SEQS * LOCAL_HEADS
    r8 = iota((nrows, 128), 0)
    first8 = r8 < LOCAL_HEADS

    def per_row(v):
        top = iota((nrows, v.shape[1]), 0) < LOCAL_HEADS
        return jnp.where(top, v[0:1, :], v[1:2, :])

    lane_8 = iota((nrows, QW), 1)
    first = (iota((nrows, QW), 0) & (LOCAL_HEADS - 1)) * PER_HEAD
    q8 = jnp.where((lane_8 >= first) & (lane_8 < first + PER_HEAD), per_row(q), 0.0).astype(BF16)
    qa = dot(q8, ka[...], NT)
    absorbed = qa[:, :LATENT].astype(BF16)
    len8 = jnp.where(first8, lens[0], lens[1])
    angle = len8.astype(F32) * fr[pl.ds(0, 1), :]
    cos8 = jnp.cos(angle)
    lane8 = iota((nrows, 128), 1)
    sin8 = jnp.where((lane8 & half) == 0, -jnp.sin(angle), jnp.sin(angle))
    q_rot = qa[:, LATENT : LATENT + 128] * cos8 + qa[:, LATENT + 128 : LATENT + 256] * sin8

    done(l_att)
    q32 = q_rot[:, :HEAD_ROT]
    per_seq = [dot(absorbed, cache[s], NT) + dot(q32, krot[s], NN, HIGHEST) for s in range(SEQS)]
    top_rows = iota((nrows, CACHE), 0) < LOCAL_HEADS
    score_scale = PER_HEAD**-0.5
    live = iota((nrows, CACHE), 1) < jnp.where(top_rows, lens[0], lens[1])
    cache_score = jnp.where(live, score_scale * jnp.where(top_rows, per_seq[0], per_seq[1]), -1e30)
    best = jnp.max(cache_score, axis=1, keepdims=True)
    cache_weight = jnp.exp(cache_score - best)
    cache_total = jnp.sum(cache_weight, axis=1, keepdims=True)
    cache_weight = cache_weight.astype(BF16)
    ctx = [dot(cache_weight, cache[s]) for s in range(SEQS)]
    ctx = jnp.where(iota((nrows, LATENT), 0) < LOCAL_HEADS, ctx[0], ctx[1])

    new_rot = rounded(tail * scale)
    o_rotkey[...] = new_rot[:, :HEAD_ROT].astype(BF16)
    new_swap = pltpu.roll(new_rot, 64, 1)
    own_rot = jnp.where(lane8 < HEAD_ROT, per_row(new_rot) * cos8 + per_row(new_swap) * sin8, 0.0)

    arrived(yb, nt - 1, 5)
    raw = jnp.concatenate([yb[i] for i in range(nt)], axis=1)
    new_latent = (
        raw * lax.rsqrt(jnp.mean(raw * raw, axis=1, keepdims=True) + EPSILON) * lgain[...]
    ).astype(BF16)
    o_latent[...] = new_latent
    lat8 = per_row(new_latent.astype(F32))
    own_score = score_scale * (
        jnp.sum(absorbed.astype(F32) * lat8, axis=1, keepdims=True)
        + jnp.sum(q_rot * own_rot, axis=1, keepdims=True)
    )
    top_score = jnp.maximum(best, own_score)
    rescale = jnp.exp(best - top_score)
    own_weight = jnp.exp(own_score - top_score)
    denominator = rescale * cache_total + own_weight
    context = (rescale / denominator) * ctx + rounded(own_weight / denominator) * lat8
    ho = dot(context.astype(BF16), valup[...])
    r_h = iota((nrows, HV), 0)
    ho = jnp.where((iota((nrows, HV), 1) >> log2(HEAD_VAL)) == (r_h & (LOCAL_HEADS - 1)), ho, 0.0)
    h0 = jnp.sum(jnp.where(r_h < LOCAL_HEADS, ho, 0.0), axis=0, keepdims=True)
    h1 = jnp.sum(jnp.where(r_h < LOCAL_HEADS, 0.0, ho), axis=0, keepdims=True)
    heads = rounded(jnp.where(iota((SEQS, HV), 0) == 0, h0, h1))
    ha[pl.ds(place_of, 1)] = heads.reshape(1, SEQS, HV)
    for dev in plane_peers:
        send(ha.at[place_of], ha.at[place_of], 7, dev)
    sent(ha, npl - 1)

    size_bg, size_h = nbytes(bgs), nbytes(hc) // zy
    for here in (True, False):

        @pl.when((y_to == y) if here else (y_to != y))
        def _():
            take_bytes((nt - 1) * size_bg if here else nt * size_bg + size_h, rsem.at[1])

    beside = [r if 2 * r <= zy else r - zy for r in range(1, zy)]
    for r in sorted(beside, key=lambda r: -abs(r)):
        dev = {"z": ((z + r + nz) & (nz - 1))}
        send(hc.at[ring], hc.at[ring], 17, dev)
        send(aoc.at[ring], aoc.at[ring], 15, dev)
    for r in sorted(beside, key=lambda r: -abs(r)):
        send(sgc.at[ring], sgc.at[ring], 16, {"z": ((z + r + nz) & (nz - 1))})
    for buf in (hc, aoc, sgc):
        sent(buf, zy - 1)

    rs = scores[...]
    rw = ROUTED_SCALE * rs / jnp.sum(rs, axis=0, keepdims=True)
    idv = ids[...]
    nex = nz + ncol
    which = iota((nex, batch), 0)
    target = jnp.where(which < nz, which * ncol + col, z * ncol + which - nz)
    hit = jnp.zeros((nex, batch), F32)
    wgt = jnp.zeros((nex, batch), F32)
    for k in range(4):
        same = idv[k : k + 1, :] == target
        hit = jnp.where(same, 1.0, hit)
        wgt = jnp.where(same, rw[k : k + 1, :], wgt)
    before = ones_where(iota((batch, batch), 0) < iota((batch, batch), 1))
    rank = dot(hit.astype(BF16), before)
    val = jnp.where(hit > 0.0, rank, -1.0).astype(BF16)
    pslot = ncol * SLOTS
    expand_p = ones_where(iota((pslot, nex), 1) == nz + (iota((pslot, nex), 0) >> log2(SLOTS)))
    sel_p[...] = ones_where(dot(expand_p, val) == (iota((pslot, batch), 0) & (SLOTS - 1)).astype(F32))

    gain_rows = jnp.broadcast_to(fgain[...][:, None, :], (nz, ncol, pf)).reshape(nz * ncol, pf)
    gr = iota((nz * ncol, pf), 0)
    gain_rows = jnp.where((iota((nz * ncol, pf), 1) >> log2(FEATS)) == (gr & (ncol - 1)), gain_rows, 0.0)
    tile_f = jnp.where(
        (iota((pf, 2 * cf), 0) & (FEATS - 1)) == (iota((pf, 2 * cf), 1) & (FEATS - 1)), 1.0, 0.0
    )
    tiled = dot(gain_rows, tile_f, NN, HIGHEST).reshape(nz, ncol, 2 * cf)
    lane_z = iota((ncol, 2 * cf), 1) >> log2(FEATS)
    for k in range(nt // 2):
        g = jnp.zeros((ncol, 2 * cf), F32)
        for i in range(2 * zy):
            g = jnp.where(lane_z == i, tiled[2 * zy * k + i], g)
        gp[k] = g

    if beside:
        take_bytes((zy - 1) * (nbytes(hc) + nbytes(aoc)) // zy, rsem.at[slot[15]])
    t_i, l_i = iota((tok, batch), 0), iota((tok, batch), 1)
    sel_h = ones_where(l_i == z * tok + t_i)
    hcv = hc[...].reshape(cf, batch)
    hid_c = dot(sel_h, jnp.concatenate([hcv, hcv], axis=0), NT)
    arrived(ha, npl - 1, 7)
    for i in range(ncol):
        for j in range(nt):
            h16[pl.ds(SEQS * i, SEQS), pl.ds(HV * j, HV)] = ha[i * nt + j]
    attn = jnp.zeros((tok, 2 * cf), F32)
    for j in range(nt):
        w = jnp.concatenate([aoc[i, j] for i in range(zy)] * 2, axis=0)
        attn = attn + dot(h16[:, pl.ds(HV * j, HV)].astype(BF16), w, NT)
    mine = (iota((tok, 2 * cf), 1) >> log2(cf)) == (y & 1)
    mid = jnp.where(mine, rounded(hid_c + rounded(attn)), 0.0)
    mz[pl.ds(z, 1)] = mid.astype(BF16).reshape(1, tok, 2 * cf)
    for p in z_peers:
        send(mz.at[z], mz.at[z], 8, {"z": p})
    sent(mz, nz - 1)

    ffn = (mid * gp[pl.ds(y >> 1, 1), pl.ds(col, 1)].reshape(1, 2 * cf)).astype(BF16)
    square = jnp.broadcast_to(jnp.sum(mid * mid, axis=1, keepdims=True), (tok, 128))
    take_bytes((zy - 1) * nbytes(sgc) // zy + (ncol - 1) * nbytes(so) // ncol, rsem.at[slot[16]])
    for j in range(nt):
        w = jnp.concatenate([sgc[i, j] for i in range(zy)] * 2, axis=0)
        sp[:, pl.ds(0, 2 * HIDDEN)] = dot(ffn, w)
        sp[:, pl.ds(2 * HIDDEN, 128)] = square
        for i in range(ncol):
            sh_s[i * nt + j] = sp[pl.ds(SEQS * i, SEQS), :]
    for dev in plane_peers:
        send(sh_s.at[(dev["x"] * nc + dev["c"]) * nt + dev["y"]], sh_r.at[place_of], 9, dev)
    sent(sh_s, npl - 1)
    sh_r[pl.ds(place_of, 1)] = sh_s[pl.ds(place_of, 1)]

    expand = ones_where(iota((nslot, nex), 1) == (iota((nslot, nex), 0) >> log2(SLOTS)))
    slot_i = (iota((nslot, batch), 0) & (SLOTS - 1)).astype(F32)
    in_slot = dot(expand, val) == slot_i
    w_hi = wgt.astype(BF16)
    w_lo = (wgt - w_hi.astype(F32)).astype(BF16)
    wt[pl.ds(0, nslot), :] = jnp.where(in_slot, dot(expand, w_hi), 0.0).astype(BF16)
    wt[pl.ds(nslot, nslot), :] = jnp.where(in_slot, dot(expand, w_lo), 0.0).astype(BF16)
    arrived(mz, nz - 1, 8)
    mid_all = mz[...].reshape(batch, 2 * cf)
    tk_s[...] = dot(sel_p[...], mid_all).astype(BF16).reshape(ncol, SLOTS, 2 * cf)
    for dev in plane_peers:
        send(tk_s.at[dev["x"] * nc + dev["c"]], tk_r.at[place_of], 10, dev)
    sent(tk_r, npl - 1)
    tk_r[pl.ds(place_of, 1)] = tk_s[pl.ds(col, 1)]
    f_i, l_i = iota((pf, 2 * cf), 0), iota((pf, 2 * cf), 1)
    own_f = (f_i >> log2(FEATS) == col) & (l_i == (z & (2 * zy - 1)) * FEATS + (f_i & (FEATS - 1))) & (y_to == y)
    tot0[...] = dot(ones_where(own_f), mid_all, NT)

    arrived(sh_r, npl - 1, 9)
    tot = sh_r[0]
    for i in range(1, npl):
        tot = tot + sh_r[i]
    scale = lax.rsqrt(tot[:, 2 * HIDDEN : 2 * HIDDEN + 1] / width + EPSILON)
    gate = scale * tot[:, :HIDDEN]
    act = rounded(gate / (1.0 + jnp.exp(-gate)) * (scale * tot[:, HIDDEN : 2 * HIDDEN]))
    zs[pl.ds(z, 1)] = act.reshape(1, SEQS, HIDDEN)
    for p in z_peers:
        send(zs.at[z], zs.at[z], 11, {"z": p})
    sent(zs, nz - 1)

    done(l_exp)
    arrived(tk_r, npl - 1, 10)
    pieces = []
    sq = jnp.zeros((SLOTS, 2 * cf), F32)
    for i in range(ncol):
        for k in range(nt // 2):
            v = tk_r[i * nt + 2 * k].astype(F32) + tk_r[i * nt + 2 * k + 1].astype(F32)
            sq = sq + v * v
            pieces.append((v * gp[k, pl.ds(i, 1), :]).astype(BF16))
    gu = dot(jnp.concatenate(pieces, axis=1), wgu[...].reshape(width, 2 * HIDDEN))
    scale = lax.rsqrt(jnp.sum(sq, axis=1, keepdims=True) / width + EPSILON)
    gate = scale * gu[:, :HIDDEN]
    act = (gate / (1.0 + jnp.exp(-gate)) * (scale * gu[:, HIDDEN:])).astype(BF16)
    out = dot(act, wd[...])
    for i in range(nz):
        zh_s[i] = out[:, pf * i : pf * (i + 1)].astype(BF16)
    for p in z_peers:
        send(zh_s.at[p], zh_r.at[z], 12, {"z": p})
    sent(zh_s, nz - 1)
    zh_r[pl.ds(z, 1)] = zh_s[pl.ds(z, 1)]

    arrived(zs, nz - 1, 11)
    for i in range(nz):
        s32[pl.ds(SEQS * i, SEQS), :] = zs[i]
    b_i, r_i = iota((batch, rows), 0), iota((batch, rows), 1)
    place = ones_where(b_i == (r_i >> 1) * tok + col * SEQS + (r_i & 1))
    spread_act = dot(place, s32[...].astype(BF16)).astype(BF16)
    total = tot0[...] + dot(so[...].reshape(pf, HIDDEN), spread_act, NT)
    arrived(zh_r, nz - 1, 12)
    parts = zh_r[...].reshape(nslot, pf)
    total = total + dot(parts, wt[pl.ds(0, nslot), :], TN) + dot(parts, wt[pl.ds(nslot, nslot), :], TN)
    total = total.reshape(ncol, 2, FEATS // 2, batch)
    low_lane = iota((ncol, FEATS // 2, hl), 2) < ob
    for k in range(nt // 2):
        ta = total[:, 0, :, hl * k : hl * (k + 1)]
        tb = total[:, 1, :, hl * k : hl * (k + 1)]
        flat = (ncol * FEATS // 2, hl)
        ra = pltpu.roll(ta.reshape(flat), ob, 1).reshape(ta.shape)
        rb = pltpu.roll(tb.reshape(flat), ob, 1).reshape(tb.shape)
        pd_s[:, 2 * k] = jnp.where(low_lane, ta, rb)
        pd_s[:, 2 * k + 1] = jnp.where(low_lane, ra, tb)
    for dev in plane_peers:
        send(pd_s.at[dev["x"] * nc + dev["c"], dev["y"]], pd_r.at[place_of], 13, dev)
    sent(pd_r, npl - 1)
    pd_r[pl.ds(place_of, 1)] = pd_s[pl.ds(col, 1), pl.ds(y, 1)].reshape(1, FEATS // 2, hl)
    arrived(pd_r, npl - 1, 13)
    tot = pd_r[0]
    for i in range(1, npl):
        tot = tot + pd_r[i]
    both = jnp.concatenate([tot, pltpu.roll(tot, ob, 1)], axis=0)
    o_mixed[...] = both[:, :ob].astype(BF16)

    for core in range(nc):
        for here in (True, False):

            @pl.when((c == core) & ((y_to == y) if here else (y_to != y)))
            def _():
                mine = (nc * nz - 1) * (size_b if core else size_a)
                mine += (nt - 1) * (size_bg + size_h) if here else nt * size_bg
                take_bytes(sum(pending) + mine, ssem.at[0])


def finish(*refs):
    copies = [pltpu.make_async_copy(refs[i], refs[3 + i], refs[6].at[i]) for i in range(3)]
    for cp in copies:
        cp.start()
    for cp in copies:
        cp.wait()


def body(nz, nx, nc, nt, *args):
    args = list(args)
    ncol = nx * nc
    pf = FEATS * ncol
    rows = SEQS * nz
    batch = rows * ncol
    lq = LATENT // nt
    nslot = nz * SLOTS
    hl = 2 * (batch // nt)
    wa = 2 * 128
    for i in (1, 12):
        args[i] = args[i].reshape(nz, pf)
    args[5] = args[5].reshape(1, LATENT)
    args[13], args[14] = args[13].T, args[14].T
    for i in (15, 16):
        args[i] = args[i].reshape(nz, ncol, FEATS, HIDDEN)
    half = HEAD_ROT // 2
    frequency = THETA_BASE ** (-np.arange(half, dtype=np.float64) / half)
    angles = frequency.astype(np.float32)[:, None] * np.arange(CACHE, dtype=np.float32)[None, :]
    trig = jnp.asarray(np.stack([np.cos(angles.astype(np.float64)), np.sin(angles.astype(np.float64))]).astype(np.float32))
    freq = jnp.asarray(np.tile(frequency.astype(np.float32), (2, 128 // half)))
    vm = pltpu.VMEM
    tok = ncol * SEQS
    cf = FEATS * nz // nt
    npl = ncol * nt
    scratch = [
        vm((nc, FEATS, wa + batch), BF16), vm((ncol, FEATS, wa + batch), BF16),
        vm((ncol, FEATS, HIDDEN), BF16),
        vm((FEATS, 2 * HV), BF16),
        vm((nz // nt, nt, FEATS, HV), BF16), vm((nz // nt, nt, FEATS, HV), BF16),
        vm((nz // nt, FEATS, batch), BF16),
        vm((128, pf), BF16),
        vm((nz, pf), F32), vm((nz, pf), F32), vm((1, LATENT), F32), vm((2, 128), F32),
        vm((LATENT, LOCAL_HEADS * HEAD_KEY), BF16), vm((LATENT, HV), BF16),
        vm((SEQS, CACHE, LATENT), BF16), vm((SEQS, HEAD_ROT, CACHE), BF16),
        pltpu.SMEM((SEQS,), jnp.int32),
        vm((4, batch), jnp.int32), vm((4, batch), F32),
        vm((ncol, nz, FEATS, 2 * HIDDEN), BF16), vm((HIDDEN, pf * nz), BF16),
        vm((2, half, CACHE), F32),
        vm((nc * nz, SEQS, wa + 128), F32), vm((nz, SEQS, wa + 128), F32), vm((nz, SEQS, wa), F32),
        vm((nt, SEQS, lq), F32),
        vm((npl, SEQS, HV), F32),
        vm((nz, tok, 2 * cf), BF16),
        vm((npl, SEQS, 2 * HIDDEN + 128), F32), vm((npl, SEQS, 2 * HIDDEN + 128), F32),
        vm((ncol, SLOTS, 2 * cf), BF16), vm((npl, SLOTS, 2 * cf), BF16),
        vm((nz, SLOTS, pf), BF16), vm((nz, SLOTS, pf), BF16),
        vm((nz, SEQS, HIDDEN), F32),
        vm((ncol, nt, FEATS // 2, hl), F32), vm((npl, FEATS // 2, hl), F32),
        vm((LATENT + 256, QW), BF16),
        vm((SEQS, HEAD_ROT, CACHE), F32),
        vm((ncol * SLOTS, batch), BF16),
        vm((2 * nslot, batch), BF16),
        vm((tok, nt * HV), F32),
        vm((rows, HIDDEN), F32),
        vm((nc * rows, wa + 128), F32),
        vm((tok, 2 * HIDDEN + 128), F32),
        vm((nt // 2, ncol, 2 * cf), F32),
        vm((pf, batch), F32),
        pltpu.SemaphoreType.DMA((6,)),
        pltpu.SemaphoreType.DMA((1,)),
        pltpu.SemaphoreType.DMA((13,)),
        pltpu.SemaphoreType.REGULAR((3,)),
        vm((2560 * 1024 // UNIT, 2, UNIT // 8), F32),
    ]
    anywhere = pl.BlockSpec(memory_space=pltpu.HBM)
    results = pl.pallas_call(
        functools.partial(kernel, nz, nx, nc, nt),
        out_shape=(
            pltpu.VMEM((FEATS, hl // 2), BF16),
            pltpu.VMEM((SEQS, LATENT), BF16),
            pltpu.VMEM((SEQS, HEAD_ROT), BF16),
        ),
        in_specs=[anywhere] * 23,
        out_specs=(pl.BlockSpec(memory_space=pltpu.VMEM),) * 3,
        scratch_shapes=scratch,
        compiler_params=pltpu.CompilerParams(collective_id=0, has_side_effects=True, vmem_limit_bytes=66977792),
        name="layer",
    )(*args, trig, freq)
    results = [pltpu.with_memory_space_constraint(r, pltpu.VMEM) for r in results]
    return pl.pallas_call(
        finish,
        out_shape=(
            jax.ShapeDtypeStruct((FEATS, hl // 2), BF16),
            jax.ShapeDtypeStruct((SEQS, LATENT), BF16),
            jax.ShapeDtypeStruct((SEQS, HEAD_ROT), BF16),
        ),
        in_specs=[pl.BlockSpec(memory_space=pltpu.VMEM)] * 3,
        out_specs=(anywhere,) * 3,
        scratch_shapes=[pltpu.SemaphoreType.DMA((3,))],
        name="finish",
    )(*results)


EP = ("z", "x", "c")


def build(devices):
    split = Mesh(devices, ("z", "x", "c", "y"))
    return jax.shard_map(
        functools.partial(body, *devices.shape),
        mesh=split,
        in_specs=(
            P(EP, None),
            P(),
            P(EP, "y"),
            P(EP, None),
            P(),
            P(),
            P(None, "y"),
            P(None, "y"),
            P(EP, None),
            P(EP, None, None),
            P(EP, None, None),
            P(EP),
            P(),
            P(),
            P(),
            P(EP, None, "y"),
            P(EP, None, "y"),
            P(EP, "y", None),
            P(EP, "y"),
            P(EP, "y"),
            P(EP, "y"),
        ),
        out_specs=(P(EP, "y"), P(EP, None), P(EP, None)),
        check_vma=False,
    )


def solution(mesh):
    return build(mesh.devices.reshape(16, 4, 2, mesh.shape["tp"]))
```

```python
import functools
import math

import jax
import jax.numpy as jnp
import numpy as np
from jax import lax
from jax.experimental import pallas as pl
from jax.experimental.pallas import tpu as pltpu
from jax.sharding import Mesh
from jax.sharding import PartitionSpec as P

MESH = pl.DeviceIdType.MESH
F32 = jnp.float32
BF16 = jnp.bfloat16
HIGHEST = lax.Precision.HIGHEST
NN = (((1,), (0,)), ((), ()))
NT = (((1,), (1,)), ((), ()))
TN = (((0,), (0,)), ((), ()))

LOCAL_HEADS = 4
HEAD_KEY = 64
HEAD_ROT = 32
HEAD_VAL = 64
PER_HEAD = HEAD_KEY + HEAD_ROT
LATENT = 512
CACHE = 1024
HIDDEN = 128
SLOTS = 16
FEATS = 16
SEQS = 2
EPSILON = 1e-06
THETA_BASE = 10000.0
ROUTED_SCALE = 2.5
QW = LOCAL_HEADS * PER_HEAD
HV = LOCAL_HEADS * HEAD_VAL
UNIT = 1024


def dot(a, b, dims=NN, precision=None):
    return lax.dot_general(a, b, dims, precision=precision, preferred_element_type=F32)


def iota(shape, axis):
    return lax.broadcasted_iota(jnp.int32, shape, axis)


def ones_where(mask, dtype=BF16):
    return jnp.where(mask, 1.0, 0.0).astype(dtype)


def rounded(v):
    return v.astype(BF16).astype(F32)


def log2(n):
    return n.bit_length() - 1


def kernel(nz, nx, nc, nt, *refs):
    (
        hidden, attn_gain, w_query, w_latent, w_rotkey, latent_gain, w_key_up, w_value_up, w_attn_out, cache_latent, cache_rotkey,
        lengths, ffn_gain, route_ids, route_scores, w_exp_gate, w_exp_up, w_exp_down, w_shared_gate, w_shared_up, w_shared_out,
        trig, freq,
        o_mixed, o_latent, o_rotkey,
        pack, crit, hidn, hp_s, hp, so, bgs, aoc, sgc, hc, rotw, again, fgain, lgain, fr, keyup, valup, cache, crot, lens, ids, scores, wgu, wd, trg,
        za_s, za_r, zb_r, yb, ha, mz, sh_s, sh_r, tk_s, tk_r, zh_s, zh_r, zs, pd_s, pd_r,
        ka, krot, sel_p, wt, h16, s32, pall, sp, gp, tot0,
        lsem, ssem, rsem, ok, ruler,
    ) = refs
    ncol = nx * nc
    pf = FEATS * ncol
    rows = SEQS * nz
    batch = rows * ncol
    width = pf * nz
    lq = LATENT // nt
    nslot = nz * SLOTS
    ob = batch // nt
    hl = 2 * ob
    wa = 2 * 128
    hw = max(128, nc * rows)
    zy = nz // nt
    tok = ncol * SEQS
    cf = FEATS * zy
    npl = ncol * nt
    th, sh = tok // 2, SLOTS // 2
    z, x, c, y = (lax.axis_index(a) for a in ("z", "x", "c", "y"))
    col = x * nc + c
    place_of = col * nt + y
    y_to = ((z) >> log2(zy))
    ring = ((z) & (zy - 1))

    def xdev(p):
        return {"x": ((p) >> log2(nc)), "c": ((p) & (nc - 1))}

    z_order = sorted(range(1, nz), key=lambda d: -min(d, nz - d))
    z_peers = [((z + d) & (nz - 1)) for d in z_order]
    x_order = sorted(range(1, ncol), key=lambda d: -min(d, ncol - d))
    x_peers = [((col + d) & (ncol - 1)) for d in x_order]
    y_peers = [((y + d) & (nt - 1)) for d in range(1, nt)]
    plane_order = sorted(
        [(dx, dc, dy) for dx in range(nx) for dc in range(nc) for dy in range(nt) if dx or dc or dy],
        key=lambda t: -(min(t[0], nx - t[0]) + min(t[2], nt - t[2])),
    )
    plane_peers = [
        {"x": ((x + dx) & (nx - 1)), "c": ((c + dc) & (nc - 1)), "y": ((y + dy) & (nt - 1))} for dx, dc, dy in plane_order
    ]

    bar = pltpu.get_barrier_semaphore()

    def signal(sem, dev):
        pl.semaphore_signal(sem, inc=1, device_id=dev, device_id_type=MESH)

    for d in range(nx - 1, 0, -1):
        signal(bar, {"x": ((x + d) & (nx - 1)), "c": 0})

    @pl.when(c == 1)
    def _():
        signal(bar, {"c": 0})

    sig_first = nz // 4
    for p in z_peers[:sig_first]:
        signal(bar, {"z": p, "c": 1})

    def nbytes(ref):
        return math.prod(ref.shape) * jnp.dtype(ref.dtype).itemsize

    def rows_of(n):
        assert n % UNIT == 0 and n // UNIT <= ruler.shape[0]
        return ruler.at[pl.ds(0, n // UNIT)]

    def loads(sem, pairs):
        for src, dst in pairs:
            pltpu.make_async_copy(src, dst, lsem.at[sem]).start()
        part = rows_of(sum(nbytes(dst) for _, dst in pairs))
        return [(part, sem)]

    def done(copies):
        for part, sem in copies:
            pltpu.make_async_copy(part, part, lsem.at[sem]).wait()

    own_lq = pl.ds(pl.multiple_of(y * lq, lq), lq)
    own_hv = pl.ds(pl.multiple_of(y * HV, HV), HV)
    own_pf = pl.ds(pl.multiple_of(z * pf, pf), pf)
    half = HEAD_ROT // 2
    l_crit = loads(0, [
        (w_query.at[:, pl.ds(0, wa)], pack.at[0, :, pl.ds(0, wa)]),
        (w_query.at[:, pl.ds(wa, QW - wa)], pack.at[1, :, pl.ds(0, QW - wa)]),
        (w_latent.at[:, own_lq], pack.at[1, :, pl.ds(QW - wa, lq)]),
        (hidden, hidn),
    ])

    for p in z_peers[sig_first:]:
        signal(bar, {"z": p, "c": 1})
    for p in y_peers:
        signal(bar, {"y": p, "c": 1})

    def send(src, dst, k, dev):
        cp = pltpu.make_async_remote_copy(
            src_ref=src, dst_ref=dst, send_sem=ssem.at[0], recv_sem=rsem.at[slot[k]], device_id=dev, device_id_type=MESH
        )
        cp.start()

    def take(part, sem):
        pltpu.make_async_copy(part, part, sem).wait()

    def arrived(buf, n, k):
        take(buf.at[pl.ds(0, n)], rsem.at[slot[k]])

    slot = {0: 0, 1: 1, 3: 1, 6: 1, 2: 2, 14: 2, 5: 3, 7: 4, 15: 5, 17: 5, 16: 6, 4: 6, 8: 7, 9: 8, 10: 9, 11: 10, 12: 11, 13: 12}
    pending = []

    def sent(buf, n):
        pending.append(n * nbytes(buf) // buf.shape[0])

    def take_bytes(n, sem):
        take(rows_of(n), sem)

    chip = nc * rows
    order = iota((batch, nx * hw), 1)
    place = order & (hw - 1)
    b_i = ((place & (rows - 1)) >> 1) * tok + ((order >> log2(hw)) * nc + (place >> log2(rows))) * SEQS + (place & 1)
    chosen = ones_where((iota((batch, nx * hw), 0) == b_i) & (place < chip))
    done(l_crit)
    cut = dot(hidn[...], chosen).astype(BF16)
    for i in range(nx):
        hp_s[i] = cut[:, hw * i : hw * (i + 1)]

    @pl.when(c == 0)
    def _():
        pl.semaphore_wait(bar, nc * nx - 1)
        signal(ok.at[0], {"c": 1})

    @pl.when(c == 1)
    def _():
        pl.semaphore_wait(ok.at[0], 1)

    for p in x_peers:
        send(hp_s.at[p >> log2(nc)], hp.at[col], 0, xdev(p))
        send(pack.at[p & (nc - 1)], crit.at[col], 0, xdev(p))
    sent(hp, ncol - 1)
    sent(crit, ncol - 1)
    crit[pl.ds(col, 1)] = pack[pl.ds(c, 1)]
    hp[pl.ds(col, 1)] = hp_s[pl.ds(x, 1)]
    l_rot = loads(1, [
        (w_rotkey.at[:, own_pf], rotw.at[pl.ds(0, HEAD_ROT)]),
        (w_rotkey.at[pl.ds(half, half), own_pf], rotw.at[pl.ds(64, half)]),
        (w_rotkey.at[pl.ds(0, half), own_pf], rotw.at[pl.ds(64 + half, half)]),
        (attn_gain, again),
        (ffn_gain, fgain),
        (latent_gain, lgain),
        (w_key_up, keyup), (cache_rotkey, crot), (trig, trg), (route_ids, ids), (route_scores, scores), (freq, fr),
    ])
    l_len = pltpu.make_async_copy(lengths, lens, lsem.at[2])
    l_len.start()
    l_att = loads(3, [(cache_latent, cache), (w_value_up, valup)])
    l_bg = loads(4, [
        (w_attn_out.at[:, own_hv], bgs.at[:, pl.ds(0, HV)]),
        (w_shared_gate, bgs.at[:, pl.ds(HV, HIDDEN)]),
        (w_shared_up, bgs.at[:, pl.ds(HV + HIDDEN, HIDDEN)]),
        (w_shared_out, so.at[col]),
    ])
    l_exp = loads(5, [(w_exp_down.at[0], wd)] + [
        (w.at[:, i], wgu.at[i, :, :, pl.ds(HIDDEN * j, HIDDEN)])
        for i in range(ncol) for j, w in enumerate((w_exp_gate, w_exp_up))
    ])

    done(l_rot)
    l_len.wait()
    cos_t, sin_t = trg[0], trg[1]
    for s in range(SEQS):
        low = crot[s, pl.ds(0, half), :].astype(F32)
        high = crot[s, pl.ds(half, half), :].astype(F32)
        krot[s, pl.ds(0, half), :] = low * cos_t - high * sin_t
        krot[s, pl.ds(half, half), :] = low * sin_t + high * cos_t
    spread_r = iota((LOCAL_HEADS * HEAD_KEY, QW), 0)
    spread = ones_where(iota((LOCAL_HEADS * HEAD_KEY, QW), 1) == spread_r + HEAD_ROT * (spread_r >> log2(HEAD_KEY)))
    ka[pl.ds(0, LATENT), :] = dot(keyup[...], spread).astype(BF16)
    lane_q = iota((256, QW), 1)
    head_q = ones_where(lane_q >= PER_HEAD, jnp.int32)
    for h in range(2, LOCAL_HEADS):
        head_q = head_q + ones_where(lane_q >= h * PER_HEAD, jnp.int32)
    within = lane_q - PER_HEAD * head_q - HEAD_KEY
    row_q = iota((256, QW), 0)
    want = jnp.where(row_q < 128, row_q, (row_q - 128) ^ half)
    limit = jnp.where(row_q < 128, row_q, row_q - 128)
    ka[pl.ds(LATENT, 256), :] = ones_where((within == want) & (limit < HEAD_ROT))
    rot_rows = iota((128, pf), 0)
    rot_w = jnp.where((rot_rows & 63) < HEAD_ROT, rotw[...].astype(F32), 0.0).astype(BF16)

    def others_ready(when):
        @pl.when((c == 1) & when)
        def _():
            pl.semaphore_wait(bar, nc * (nz - 1) + nc * (nt - 1))
            signal(ok.at[1], {"c": 0})
            for p in y_peers:
                for core in range(nc):
                    signal(ok.at[2], {"y": p, "c": core})

    others_ready(z >= nz // 2)

    take_bytes((ncol - 1) * (nbytes(crit) + nbytes(hp)) // ncol, rsem.at[slot[0]])
    sel_a = ones_where(iota((nc * rows, hw), 0) == iota((nc * rows, hw), 1))
    hid = hp[...].reshape(pf, hw)
    h_t = dot(sel_a, hid, NT)
    scaled = (h_t * again[pl.ds(z, 1), :]).astype(BF16)
    pall[:, pl.ds(0, wa)] = dot(scaled, crit[:, :, pl.ds(0, wa)].reshape(pf, wa))
    rot = dot(scaled, rot_w, NT)
    square = jnp.sum(h_t * h_t, axis=1, keepdims=True)
    pall[:, pl.ds(wa, 128)] = jnp.where(iota((nc * rows, 128), 1) == HEAD_ROT, square, rot)
    for i in range(nc * nz):
        za_s[i] = pall[pl.ds(SEQS * i, SEQS), :]

    others_ready(z < nz // 2)

    @pl.when(c == 0)
    def _():
        pl.semaphore_wait(ok.at[1], 1)

    zc_peers = [(p, d) for p in z_peers for d in range(nc)] + [(z, 1)]
    for core in range(nc):

        @pl.when(c == core)
        def _():
            lanes = pl.ds(0, wa if core else wa + 128)
            dst = (za_r, zb_r)[core]
            for p, d in zc_peers:
                e = (core + d) % nc
                send(za_s.at[e * nz + p, :, lanes], dst.at[z], 2 + 12 * core, {"z": p, "c": e})
            dst[pl.ds(z, 1)] = za_s[pl.ds(core * nz + z, 1), :, lanes]

    size_a, size_b = nbytes(za_r) // nz, nbytes(zb_r) // nz

    pl.semaphore_wait(ok.at[2], nt - 1)
    done(l_bg)

    groups = sorted(range(nt), key=lambda k: -min(k, nt - k))
    for src, dst, k in ((bgs.at[:, pl.ds(0, HV)], aoc, 1), (bgs.at[:, pl.ds(HV, HV)], sgc, 6)):
        for g in groups:
            dev = {"z": ((z + zy * g) & (nz - 1)), "y": y_to}
            if g:
                send(src, dst.at[ring, y], k, dev)
            else:

                @pl.when(y_to != y)
                def _():
                    send(src, dst.at[ring, y], k, dev)

                @pl.when(y_to == y)
                def _():
                    dst[pl.ds(ring, 1), pl.ds(y, 1)] = src[...].reshape(1, 1, FEATS, HV)

    @pl.when(y_to == y)
    def _():
        for g in groups[:-1]:
            send(hidn, hc.at[ring], 3, {"z": ((z + zy * g) & (nz - 1))})
        hc[pl.ds(ring, 1)] = hidn[...].reshape(1, FEATS, batch)

    for p in x_peers:
        send(so.at[col], so.at[col], 4, xdev(p))
    sent(so, ncol - 1)

    for core in range(nc):

        @pl.when(c == core)
        def _():
            take_bytes((nz - 1 + core) * size_a + (nz - core) * size_b, rsem.at[2])

    tot, tot_b = za_r[0], zb_r[0]
    for i in range(1, nz):
        tot = tot + za_r[i]
        tot_b = tot_b + zb_r[i]
    lane2 = iota((SEQS, 128), 1)
    tail = tot[:, wa:]
    sq = jnp.sum(jnp.where(lane2 == HEAD_ROT, tail, 0.0), axis=1, keepdims=True)
    scale = lax.rsqrt(sq / width + EPSILON)
    yb[pl.ds(y, 1)] = rounded(tot_b[:, QW - wa :] * scale).reshape(1, SEQS, lq)
    for p in y_peers:
        send(yb.at[y], yb.at[y], 5, {"y": p})
    sent(yb, nt - 1)
    q = rounded(jnp.concatenate([tot[:, :wa], tot_b[:, : QW - wa]], axis=1) * scale)
    nrows = SEQS * LOCAL_HEADS
    r8 = iota((nrows, 128), 0)
    first8 = r8 < LOCAL_HEADS

    def per_row(v):
        top = iota((nrows, v.shape[1]), 0) < LOCAL_HEADS
        return jnp.where(top, v[0:1, :], v[1:2, :])

    lane_8 = iota((nrows, QW), 1)
    first = (iota((nrows, QW), 0) & (LOCAL_HEADS - 1)) * PER_HEAD
    q8 = jnp.where((lane_8 >= first) & (lane_8 < first + PER_HEAD), per_row(q), 0.0).astype(BF16)
    qa = dot(q8, ka[...], NT)
    absorbed = qa[:, :LATENT].astype(BF16)
    len8 = jnp.where(first8, lens[0], lens[1])
    angle = len8.astype(F32) * fr[pl.ds(0, 1), :]
    cos8 = jnp.cos(angle)
    lane8 = iota((nrows, 128), 1)
    sin8 = jnp.where((lane8 & half) == 0, -jnp.sin(angle), jnp.sin(angle))
    q_rot = qa[:, LATENT : LATENT + 128] * cos8 + qa[:, LATENT + 128 : LATENT + 256] * sin8

    done(l_att)
    q32 = q_rot[:, :HEAD_ROT]
    per_seq = [dot(absorbed, cache[s], NT) + dot(q32, krot[s], NN, HIGHEST) for s in range(SEQS)]
    top_rows = iota((nrows, CACHE), 0) < LOCAL_HEADS
    score_scale = PER_HEAD**-0.5
    live = iota((nrows, CACHE), 1) < jnp.where(top_rows, lens[0], lens[1])
    cache_score = jnp.where(live, score_scale * jnp.where(top_rows, per_seq[0], per_seq[1]), -1e30)
    best = jnp.max(cache_score, axis=1, keepdims=True)
    cache_weight = jnp.exp(cache_score - best)
    cache_total = jnp.sum(cache_weight, axis=1, keepdims=True)
    cache_weight = cache_weight.astype(BF16)
    ctx = [dot(cache_weight, cache[s]) for s in range(SEQS)]
    ctx = jnp.where(iota((nrows, LATENT), 0) < LOCAL_HEADS, ctx[0], ctx[1])

    new_rot = rounded(tail * scale)
    o_rotkey[...] = new_rot[:, :HEAD_ROT].astype(BF16)
    new_swap = pltpu.roll(new_rot, 64, 1)
    own_rot = jnp.where(lane8 < HEAD_ROT, per_row(new_rot) * cos8 + per_row(new_swap) * sin8, 0.0)

    arrived(yb, nt - 1, 5)
    raw = jnp.concatenate([yb[i] for i in range(nt)], axis=1)
    new_latent = (
        raw * lax.rsqrt(jnp.mean(raw * raw, axis=1, keepdims=True) + EPSILON) * lgain[...]
    ).astype(BF16)
    o_latent[...] = new_latent
    lat8 = per_row(new_latent.astype(F32))
    own_score = score_scale * (
        jnp.sum(absorbed.astype(F32) * lat8, axis=1, keepdims=True)
        + jnp.sum(q_rot * own_rot, axis=1, keepdims=True)
    )
    top_score = jnp.maximum(best, own_score)
    rescale = jnp.exp(best - top_score)
    own_weight = jnp.exp(own_score - top_score)
    denominator = rescale * cache_total + own_weight
    context = (rescale / denominator) * ctx + rounded(own_weight / denominator) * lat8
    ho = dot(context.astype(BF16), valup[...])
    r_h = iota((nrows, HV), 0)
    ho = jnp.where((iota((nrows, HV), 1) >> log2(HEAD_VAL)) == (r_h & (LOCAL_HEADS - 1)), ho, 0.0)
    h0 = jnp.sum(jnp.where(r_h < LOCAL_HEADS, ho, 0.0), axis=0, keepdims=True)
    h1 = jnp.sum(jnp.where(r_h < LOCAL_HEADS, 0.0, ho), axis=0, keepdims=True)
    heads = rounded(jnp.where(iota((SEQS, HV), 0) == 0, h0, h1))
    ha[pl.ds(place_of, 1)] = heads.astype(BF16).reshape(1, SEQS, HV)
    for dev in plane_peers:
        send(ha.at[place_of], ha.at[place_of], 7, dev)
    sent(ha, npl - 1)

    size_bg, size_h = nbytes(bgs), nbytes(hc) // zy
    for here in (True, False):

        @pl.when((y_to == y) if here else (y_to != y))
        def _():
            take_bytes((nt - 1) * size_bg if here else nt * size_bg + size_h, rsem.at[1])

    beside = [r if 2 * r <= zy else r - zy for r in range(1, zy)]
    for r in sorted(beside, key=lambda r: -abs(r)):
        dev = {"z": ((z + r + nz) & (nz - 1))}
        send(hc.at[ring], hc.at[ring], 17, dev)
        send(aoc.at[ring], aoc.at[ring], 15, dev)
    for r in sorted(beside, key=lambda r: -abs(r)):
        send(sgc.at[ring], sgc.at[ring], 16, {"z": ((z + r + nz) & (nz - 1))})
    for buf in (hc, aoc, sgc):
        sent(buf, zy - 1)

    rs = scores[...]
    rw = ROUTED_SCALE * rs / jnp.sum(rs, axis=0, keepdims=True)
    idv = ids[...]
    nex = nz + ncol
    which = iota((nex, batch), 0)
    target = jnp.where(which < nz, which * ncol + col, z * ncol + which - nz)
    hit = jnp.zeros((nex, batch), F32)
    wgt = jnp.zeros((nex, batch), F32)
    for k in range(4):
        same = idv[k : k + 1, :] == target
        hit = jnp.where(same, 1.0, hit)
        wgt = jnp.where(same, rw[k : k + 1, :], wgt)
    before = ones_where(iota((batch, batch), 0) < iota((batch, batch), 1))
    rank = dot(hit.astype(BF16), before)
    val = jnp.where(hit > 0.0, rank, -1.0).astype(BF16)
    pslot = ncol * SLOTS

    def pick(upper, shape, token_axis):
        t, p = iota(shape, token_axis), iota(shape, 1 - token_axis)
        return ones_where((t >> log2(th)) == 2 * (p >> log2(th)) + upper, jnp.int32) * ones_where(
            (t & (th - 1)) == (p & (th - 1)), jnp.int32
        )

    expand_p = ones_where(iota((pslot, nex), 1) == nz + (iota((pslot, nex), 0) >> log2(SLOTS)))
    slot_p = (iota((pslot, nz * th), 0) & (SLOTS - 1)).astype(F32)
    for i in range(2):
        part = dot(val, pick(i, (batch, nz * th), 0).astype(F32).astype(BF16)).astype(BF16)
        sel_p[i] = ones_where(dot(expand_p, part) == slot_p)

    gain_rows = jnp.broadcast_to(fgain[...][:, None, :], (nz, ncol, pf)).reshape(nz * ncol, pf)
    gr = iota((nz * ncol, pf), 0)
    gain_rows = jnp.where((iota((nz * ncol, pf), 1) >> log2(FEATS)) == (gr & (ncol - 1)), gain_rows, 0.0)
    tile_f = jnp.where(
        (iota((pf, 2 * cf), 0) & (FEATS - 1)) == (iota((pf, 2 * cf), 1) & (FEATS - 1)), 1.0, 0.0
    )
    tiled = dot(gain_rows, tile_f, NN, HIGHEST).reshape(nz, ncol, 2 * cf)
    lane_z = iota((ncol, 2 * cf), 1) >> log2(FEATS)
    for k in range(nt // 2):
        g = jnp.zeros((ncol, 2 * cf), F32)
        for i in range(2 * zy):
            g = jnp.where(lane_z == i, tiled[2 * zy * k + i], g)
        gp[k] = g

    if beside:
        take_bytes((zy - 1) * (nbytes(hc) + nbytes(aoc)) // zy, rsem.at[slot[15]])
    t_i, l_i = iota((tok, batch), 0), iota((tok, batch), 1)
    sel_h = ones_where(l_i == z * tok + t_i)
    hcv = hc[...].reshape(cf, batch)
    hid_c = dot(sel_h, jnp.concatenate([hcv, hcv], axis=0), NT)
    arrived(ha, npl - 1, 7)
    for i in range(ncol):
        for j in range(nt):
            h16[pl.ds(SEQS * i, SEQS), pl.ds(HV * j, HV)] = ha[i * nt + j].astype(F32)
    attn = jnp.zeros((tok, 2 * cf), F32)
    for j in range(nt):
        w = jnp.concatenate([aoc[i, j] for i in range(zy)] * 2, axis=0)
        attn = attn + dot(h16[:, pl.ds(HV * j, HV)].astype(BF16), w, NT)
    mid = rounded(hid_c + rounded(attn))
    low8 = iota((th, 2 * cf), 1) < cf
    mz[pl.ds(z, 1)] = jnp.where(low8, mid[:th], mid[th:]).astype(BF16).reshape(1, th, 2 * cf)
    for p in z_peers:
        send(mz.at[z], mz.at[z], 8, {"z": p})
    sent(mz, nz - 1)

    mine = (iota((tok, 2 * cf), 1) >> log2(cf)) == (y & 1)
    mid = jnp.where(mine, mid, 0.0)
    ffn = (mid * gp[pl.ds(y >> 1, 1), pl.ds(col, 1)].reshape(1, 2 * cf)).astype(BF16)
    square = jnp.broadcast_to(jnp.sum(mid * mid, axis=1, keepdims=True), (tok, 128))
    take_bytes((zy - 1) * nbytes(sgc) // zy + (ncol - 1) * nbytes(so) // ncol, rsem.at[slot[16]])
    for j in range(nt):
        w = jnp.concatenate([sgc[i, j] for i in range(zy)] * 2, axis=0)
        sp[:, pl.ds(0, 2 * HIDDEN)] = dot(ffn, w)
        sp[:, pl.ds(2 * HIDDEN, 128)] = square
        for i in range(ncol):
            sh_s[i * nt + j] = sp[pl.ds(SEQS * i, SEQS), :]
    for dev in plane_peers:
        send(sh_s.at[(dev["x"] * nc + dev["c"]) * nt + dev["y"]], sh_r.at[place_of], 9, dev)
    sent(sh_s, npl - 1)
    sh_r[pl.ds(place_of, 1)] = sh_s[pl.ds(place_of, 1)]

    expand = ones_where(iota((nslot, nex), 1) == (iota((nslot, nex), 0) >> log2(SLOTS)))
    slot_i = (iota((nslot, batch), 0) & (SLOTS - 1)).astype(F32)
    in_slot = dot(expand, val) == slot_i
    w_hi = wgt.astype(BF16)
    w_lo = (wgt - w_hi.astype(F32)).astype(BF16)
    wt[pl.ds(0, nslot), :] = jnp.where(in_slot, dot(expand, w_hi), 0.0).astype(BF16)
    wt[pl.ds(nslot, nslot), :] = jnp.where(in_slot, dot(expand, w_lo), 0.0).astype(BF16)
    arrived(mz, nz - 1, 8)
    mid_all = mz[...].reshape(nz * th, 2 * cf)
    low = iota((pslot, 2 * cf), 1) < cf
    tk = jnp.where(low, dot(sel_p[0], mid_all), dot(sel_p[1], mid_all))
    tk = (tk + pltpu.roll(tk, cf, 1)).reshape(ncol, 2, sh, 2 * cf)
    tk_s[...] = jnp.where(iota((ncol, sh, 2 * cf), 2) < cf, tk[:, 0], tk[:, 1]).astype(BF16)
    for dev in plane_peers:
        send(tk_s.at[dev["x"] * nc + dev["c"]], tk_r.at[place_of], 10, dev)
    sent(tk_r, npl - 1)
    tk_r[pl.ds(place_of, 1)] = tk_s[pl.ds(col, 1)]
    f_i, l_i = iota((pf, 2 * cf), 0), iota((pf, 2 * cf), 1)
    own_f = ((f_i >> log2(FEATS)) == col) & (y_to == y)
    own_l = ring * FEATS + (f_i & (FEATS - 1))
    tot0[...] = jnp.zeros((pf, batch), F32)
    for i in range(2):
        part = dot(ones_where(own_f & (l_i == own_l + cf * i)), mid_all, NT).astype(BF16)
        tot0[...] += dot(part, pick(i, (nz * th, batch), 1).astype(F32).astype(BF16))

    arrived(sh_r, npl - 1, 9)
    tot = sh_r[0]
    for i in range(1, npl):
        tot = tot + sh_r[i]
    scale = lax.rsqrt(tot[:, 2 * HIDDEN : 2 * HIDDEN + 1] / width + EPSILON)
    gate = scale * tot[:, :HIDDEN]
    act = rounded(gate / (1.0 + jnp.exp(-gate)) * (scale * tot[:, HIDDEN : 2 * HIDDEN]))
    zs[pl.ds(z, 1)] = act.reshape(1, SEQS, HIDDEN)
    for p in z_peers:
        send(zs.at[z], zs.at[z], 11, {"z": p})
    sent(zs, nz - 1)

    done(l_exp)
    arrived(tk_r, npl - 1, 10)
    pieces = []
    low_s = iota((sh, 2 * cf), 1) < cf
    sq = jnp.zeros((SLOTS, 2 * cf), F32)
    for i in range(ncol):
        for k in range(nt // 2):
            va = tk_r[i * nt + 2 * k].astype(F32)
            vb = tk_r[i * nt + 2 * k + 1].astype(F32)
            v = jnp.concatenate(
                [jnp.where(low_s, va, pltpu.roll(vb, cf, 1)), jnp.where(low_s, pltpu.roll(va, cf, 1), vb)], axis=0
            )
            sq = sq + v * v
            pieces.append((v * gp[k, pl.ds(i, 1), :]).astype(BF16))
    gu = dot(jnp.concatenate(pieces, axis=1), wgu[...].reshape(width, 2 * HIDDEN))
    scale = lax.rsqrt(jnp.sum(sq, axis=1, keepdims=True) / width + EPSILON)
    gate = scale * gu[:, :HIDDEN]
    act = (gate / (1.0 + jnp.exp(-gate)) * (scale * gu[:, HIDDEN:])).astype(BF16)
    for p in z_peers + [z]:
        zh_s[pl.ds(p, 1)] = dot(act, wd[:, pl.ds(pl.multiple_of(p * pf, pf), pf)]).astype(BF16).reshape(1, SLOTS, pf)
        if p is not z:
            send(zh_s.at[p], zh_r.at[z], 12, {"z": p})
    sent(zh_s, nz - 1)
    zh_r[pl.ds(z, 1)] = zh_s[pl.ds(z, 1)]

    arrived(zs, nz - 1, 11)
    for i in range(nz):
        s32[pl.ds(SEQS * i, SEQS), :] = zs[i]
    b_i, r_i = iota((batch, rows), 0), iota((batch, rows), 1)
    place = ones_where(b_i == (r_i >> 1) * tok + col * SEQS + (r_i & 1))
    spread_act = dot(place, s32[...].astype(BF16)).astype(BF16)
    total = tot0[...] + dot(so[...].reshape(pf, HIDDEN), spread_act, NT)
    arrived(zh_r, nz - 1, 12)
    parts = zh_r[...].reshape(nslot, pf)
    total = total + dot(parts, wt[pl.ds(0, nslot), :], TN) + dot(parts, wt[pl.ds(nslot, nslot), :], TN)
    total = total.reshape(ncol, 2, FEATS // 2, batch)
    low_lane = iota((ncol, FEATS // 2, hl), 2) < ob
    for k in range(nt // 2):
        ta = total[:, 0, :, hl * k : hl * (k + 1)]
        tb = total[:, 1, :, hl * k : hl * (k + 1)]
        flat = (ncol * FEATS // 2, hl)
        ra = pltpu.roll(ta.reshape(flat), ob, 1).reshape(ta.shape)
        rb = pltpu.roll(tb.reshape(flat), ob, 1).reshape(tb.shape)
        pd_s[:, 2 * k] = jnp.where(low_lane, ta, rb)
        pd_s[:, 2 * k + 1] = jnp.where(low_lane, ra, tb)
    for dev in plane_peers:
        send(pd_s.at[dev["x"] * nc + dev["c"], dev["y"]], pd_r.at[place_of], 13, dev)
    sent(pd_r, npl - 1)
    pd_r[pl.ds(place_of, 1)] = pd_s[pl.ds(col, 1), pl.ds(y, 1)].reshape(1, FEATS // 2, hl)
    arrived(pd_r, npl - 1, 13)
    tot = pd_r[0]
    for i in range(1, npl):
        tot = tot + pd_r[i]
    both = jnp.concatenate([tot, pltpu.roll(tot, ob, 1)], axis=0)
    o_mixed[...] = both[:, :ob].astype(BF16)

    for core in range(nc):
        for here in (True, False):

            @pl.when((c == core) & ((y_to == y) if here else (y_to != y)))
            def _():
                mine = (nc * nz - 1) * (size_b if core else size_a)
                mine += (nt - 1) * (size_bg + size_h) if here else nt * size_bg
                take_bytes(sum(pending) + mine, ssem.at[0])


def finish(*refs):
    copies = [pltpu.make_async_copy(refs[i], refs[3 + i], refs[6].at[i]) for i in range(3)]
    for cp in copies:
        cp.start()
    for cp in copies:
        cp.wait()


def body(nz, nx, nc, nt, *args):
    args = list(args)
    ncol = nx * nc
    pf = FEATS * ncol
    rows = SEQS * nz
    batch = rows * ncol
    lq = LATENT // nt
    nslot = nz * SLOTS
    hl = 2 * (batch // nt)
    wa = 2 * 128
    for i in (1, 12):
        args[i] = args[i].reshape(nz, pf)
    args[5] = args[5].reshape(1, LATENT)
    args[13], args[14] = args[13].T, args[14].T
    for i in (15, 16):
        args[i] = args[i].reshape(nz, ncol, FEATS, HIDDEN)
    half = HEAD_ROT // 2
    frequency = THETA_BASE ** (-np.arange(half, dtype=np.float64) / half)
    angles = frequency.astype(np.float32)[:, None] * np.arange(CACHE, dtype=np.float32)[None, :]
    trig = jnp.asarray(np.stack([np.cos(angles.astype(np.float64)), np.sin(angles.astype(np.float64))]).astype(np.float32))
    freq = jnp.asarray(np.tile(frequency.astype(np.float32), (2, 128 // half)))
    vm = pltpu.VMEM
    tok = ncol * SEQS
    cf = FEATS * nz // nt
    npl = ncol * nt
    scratch = [
        vm((nc, FEATS, wa), BF16), vm((ncol, FEATS, wa), BF16),
        vm((FEATS, batch), BF16), vm((nx, FEATS, max(128, nc * rows)), BF16), vm((ncol, FEATS, max(128, nc * rows)), BF16),
        vm((ncol, FEATS, HIDDEN), BF16),
        vm((FEATS, 2 * HV), BF16),
        vm((nz // nt, nt, FEATS, HV), BF16), vm((nz // nt, nt, FEATS, HV), BF16),
        vm((nz // nt, FEATS, batch), BF16),
        vm((128, pf), BF16),
        vm((nz, pf), F32), vm((nz, pf), F32), vm((1, LATENT), F32), vm((2, 128), F32),
        vm((LATENT, LOCAL_HEADS * HEAD_KEY), BF16), vm((LATENT, HV), BF16),
        vm((SEQS, CACHE, LATENT), BF16), vm((SEQS, HEAD_ROT, CACHE), BF16),
        pltpu.SMEM((SEQS,), jnp.int32),
        vm((4, batch), jnp.int32), vm((4, batch), F32),
        vm((ncol, nz, FEATS, 2 * HIDDEN), BF16), vm((HIDDEN, pf * nz), BF16),
        vm((2, half, CACHE), F32),
        vm((nc * nz, SEQS, wa + 128), F32), vm((nz, SEQS, wa + 128), F32), vm((nz, SEQS, wa), F32),
        vm((nt, SEQS, lq), F32),
        vm((npl, SEQS, HV), BF16),
        vm((nz, tok // 2, 2 * cf), BF16),
        vm((npl, SEQS, 2 * HIDDEN + 128), F32), vm((npl, SEQS, 2 * HIDDEN + 128), F32),
        vm((ncol, SLOTS // 2, 2 * cf), BF16), vm((npl, SLOTS // 2, 2 * cf), BF16),
        vm((nz, SLOTS, pf), BF16), vm((nz, SLOTS, pf), BF16),
        vm((nz, SEQS, HIDDEN), F32),
        vm((ncol, nt, FEATS // 2, hl), F32), vm((npl, FEATS // 2, hl), F32),
        vm((LATENT + 256, QW), BF16),
        vm((SEQS, HEAD_ROT, CACHE), F32),
        vm((2, ncol * SLOTS, batch // 2), BF16),
        vm((2 * nslot, batch), BF16),
        vm((tok, nt * HV), F32),
        vm((rows, HIDDEN), F32),
        vm((nc * rows, wa + 128), F32),
        vm((tok, 2 * HIDDEN + 128), F32),
        vm((nt // 2, ncol, 2 * cf), F32),
        vm((pf, batch), F32),
        pltpu.SemaphoreType.DMA((6,)),
        pltpu.SemaphoreType.DMA((1,)),
        pltpu.SemaphoreType.DMA((13,)),
        pltpu.SemaphoreType.REGULAR((3,)),
        vm((2560 * 1024 // UNIT, 2, UNIT // 8), F32),
    ]
    anywhere = pl.BlockSpec(memory_space=pltpu.HBM)
    results = pl.pallas_call(
        functools.partial(kernel, nz, nx, nc, nt),
        out_shape=(
            pltpu.VMEM((FEATS, hl // 2), BF16),
            pltpu.VMEM((SEQS, LATENT), BF16),
            pltpu.VMEM((SEQS, HEAD_ROT), BF16),
        ),
        in_specs=[anywhere] * 23,
        out_specs=(pl.BlockSpec(memory_space=pltpu.VMEM),) * 3,
        scratch_shapes=scratch,
        compiler_params=pltpu.CompilerParams(collective_id=0, has_side_effects=True, vmem_limit_bytes=66977792),
        name="layer",
    )(*args, trig, freq)
    results = [pltpu.with_memory_space_constraint(r, pltpu.VMEM) for r in results]
    return pl.pallas_call(
        finish,
        out_shape=(
            jax.ShapeDtypeStruct((FEATS, hl // 2), BF16),
            jax.ShapeDtypeStruct((SEQS, LATENT), BF16),
            jax.ShapeDtypeStruct((SEQS, HEAD_ROT), BF16),
        ),
        in_specs=[pl.BlockSpec(memory_space=pltpu.VMEM)] * 3,
        out_specs=(anywhere,) * 3,
        scratch_shapes=[pltpu.SemaphoreType.DMA((3,))],
        name="finish",
    )(*results)


EP = ("z", "x", "c")


def build(devices):
    split = Mesh(devices, ("z", "x", "c", "y"))
    return jax.shard_map(
        functools.partial(body, *devices.shape),
        mesh=split,
        in_specs=(
            P(EP, None),
            P(),
            P(EP, "y"),
            P(EP, None),
            P(),
            P(),
            P(None, "y"),
            P(None, "y"),
            P(EP, None),
            P(EP, None, None),
            P(EP, None, None),
            P(EP),
            P(),
            P(),
            P(),
            P(EP, None, "y"),
            P(EP, None, "y"),
            P(EP, "y", None),
            P(EP, "y"),
            P(EP, "y"),
            P(EP, "y"),
        ),
        out_specs=(P(EP, "y"), P(EP, None), P(EP, None)),
        check_vma=False,
    )


def solution(mesh):
    return build(mesh.devices.reshape(16, 4, 2, mesh.shape["tp"]))
```

```python
import functools
import math

import jax
import jax.numpy as jnp
import numpy as np
from jax import lax
from jax.experimental import pallas as pl
from jax.experimental.pallas import tpu as pltpu
from jax.sharding import Mesh
from jax.sharding import PartitionSpec as P

MESH = pl.DeviceIdType.MESH
F32 = jnp.float32
BF16 = jnp.bfloat16
HIGHEST = lax.Precision.HIGHEST
NN = (((1,), (0,)), ((), ()))
NT = (((1,), (1,)), ((), ()))
TN = (((0,), (0,)), ((), ()))

LOCAL_HEADS = 4
HEAD_KEY = 64
HEAD_ROT = 32
HEAD_VAL = 64
PER_HEAD = HEAD_KEY + HEAD_ROT
LATENT = 512
CACHE = 1024
HIDDEN = 128
SLOTS = 16
FEATS = 16
SEQS = 2
EPSILON = 1e-06
THETA_BASE = 10000.0
ROUTED_SCALE = 2.5
QW = LOCAL_HEADS * PER_HEAD
HV = LOCAL_HEADS * HEAD_VAL
UNIT = 1024


def dot(a, b, dims=NN, precision=None):
    return lax.dot_general(a, b, dims, precision=precision, preferred_element_type=F32)


def iota(shape, axis):
    return lax.broadcasted_iota(jnp.int32, shape, axis)


def ones_where(mask, dtype=BF16):
    return jnp.where(mask, 1.0, 0.0).astype(dtype)


def rounded(v):
    return v.astype(BF16).astype(F32)


def log2(n):
    return n.bit_length() - 1


def kernel(nz, nx, nc, nt, *refs):
    (
        hidden, attn_gain, w_query, w_latent, w_rotkey, latent_gain, w_key_up, w_value_up, w_attn_out, cache_latent, cache_rotkey,
        lengths, ffn_gain, route_ids, route_scores, w_exp_gate, w_exp_up, w_exp_down, w_shared_gate, w_shared_up, w_shared_out,
        trig, freq,
        o_mixed, o_latent, o_rotkey,
        pack, crit, hidn, hp_s, hp, so, bgs, aoc, sgc, hc, rotw, again, fgain, lgain, fr, keyup, valup, cache, crot, lens, ids, scores, wgu, wd, trg,
        za_s, za_r, zb_r, yb, ha, mz, sh_s, sh_r, tk_s, tk_r, zh_s, zh_r, zs, pd_s, pd_r,
        ka, krot, sel_p, wt, h16, s32, pall, sp, gp, tot0,
        lsem, ssem, rsem, ok, ruler,
    ) = refs
    ncol = nx * nc
    pf = FEATS * ncol
    rows = SEQS * nz
    batch = rows * ncol
    width = pf * nz
    lq = LATENT // nt
    nslot = nz * SLOTS
    ob = batch // nt
    hl = 2 * ob
    wa = 2 * 128
    hw = max(128, nc * rows)
    zy = nz // nt
    tok = ncol * SEQS
    cf = FEATS * zy
    npl = ncol * nt
    th, sh = tok // 2, SLOTS // 2
    z, x, c, y = (lax.axis_index(a) for a in ("z", "x", "c", "y"))
    col = x * nc + c
    place_of = col * nt + y
    y_to = ((z) >> log2(zy))
    ring = ((z) & (zy - 1))

    def xdev(p):
        return {"x": ((p) >> log2(nc)), "c": ((p) & (nc - 1))}

    z_order = sorted(range(1, nz), key=lambda d: -min(d, nz - d))
    z_peers = [((z + d) & (nz - 1)) for d in z_order]
    x_order = sorted(range(1, ncol), key=lambda d: -min(d, ncol - d))
    x_peers = [((col + d) & (ncol - 1)) for d in x_order]
    y_peers = [((y + d) & (nt - 1)) for d in range(1, nt)]
    plane_order = sorted(
        [(dx, dc, dy) for dx in range(nx) for dc in range(nc) for dy in range(nt) if dx or dc or dy],
        key=lambda t: -(min(t[0], nx - t[0]) + min(t[2], nt - t[2])),
    )
    plane_peers = [
        {"x": ((x + dx) & (nx - 1)), "c": ((c + dc) & (nc - 1)), "y": ((y + dy) & (nt - 1))} for dx, dc, dy in plane_order
    ]

    bar = pltpu.get_barrier_semaphore()

    def signal(sem, dev):
        pl.semaphore_signal(sem, inc=1, device_id=dev, device_id_type=MESH)

    for d in range(nx - 1, 0, -1):
        signal(bar, {"x": ((x + d) & (nx - 1)), "c": 0})

    @pl.when(c == 1)
    def _():
        signal(bar, {"c": 0})

    sig_first = nz // 4
    for p in z_peers[:sig_first]:
        signal(bar, {"z": p, "c": 1})

    def nbytes(ref):
        return math.prod(ref.shape) * jnp.dtype(ref.dtype).itemsize

    def rows_of(n):
        assert n % UNIT == 0 and n // UNIT <= ruler.shape[0]
        return ruler.at[pl.ds(0, n // UNIT)]

    def loads(sem, pairs):
        for src, dst in pairs:
            pltpu.make_async_copy(src, dst, lsem.at[sem]).start()
        part = rows_of(sum(nbytes(dst) for _, dst in pairs))
        return [(part, sem)]

    def done(copies):
        for part, sem in copies:
            pltpu.make_async_copy(part, part, lsem.at[sem]).wait()

    own_lq = pl.ds(pl.multiple_of(y * lq, lq), lq)
    own_hv = pl.ds(pl.multiple_of(y * HV, HV), HV)
    own_pf = pl.ds(pl.multiple_of(z * pf, pf), pf)
    half = HEAD_ROT // 2
    l_crit = loads(0, [
        (w_query.at[:, pl.ds(0, wa)], pack.at[0, :, pl.ds(0, wa)]),
        (w_query.at[:, pl.ds(wa, QW - wa)], pack.at[1, :, pl.ds(0, QW - wa)]),
        (w_latent.at[:, own_lq], pack.at[1, :, pl.ds(QW - wa, lq)]),
        (hidden, hidn),
    ])

    for p in z_peers[sig_first:]:
        signal(bar, {"z": p, "c": 1})
    for p in y_peers:
        signal(bar, {"y": p, "c": 1})

    def send(src, dst, k, dev):
        cp = pltpu.make_async_remote_copy(
            src_ref=src, dst_ref=dst, send_sem=ssem.at[0], recv_sem=rsem.at[slot[k]], device_id=dev, device_id_type=MESH
        )
        cp.start()

    def take(part, sem):
        pltpu.make_async_copy(part, part, sem).wait()

    def arrived(buf, n, k):
        take(buf.at[pl.ds(0, n)], rsem.at[slot[k]])

    slot = {0: 0, 1: 1, 3: 1, 6: 13, 2: 2, 14: 2, 5: 3, 7: 4, 15: 5, 17: 5, 16: 6, 4: 6, 8: 7, 9: 8, 10: 9, 11: 10, 12: 11, 13: 12}
    pending = []

    def sent(buf, n):
        pending.append(n * nbytes(buf) // buf.shape[0])

    def take_bytes(n, sem):
        take(rows_of(n), sem)

    chip = nc * rows
    order = iota((batch, nx * hw), 1)
    place = order & (hw - 1)
    b_i = ((place & (rows - 1)) >> 1) * tok + ((order >> log2(hw)) * nc + (place >> log2(rows))) * SEQS + (place & 1)
    chosen = ones_where((iota((batch, nx * hw), 0) == b_i) & (place < chip))
    done(l_crit)
    cut = dot(hidn[...], chosen).astype(BF16)
    for i in range(nx):
        hp_s[i] = cut[:, hw * i : hw * (i + 1)]

    @pl.when(c == 0)
    def _():
        pl.semaphore_wait(bar, nc * nx - 1)
        signal(ok.at[0], {"c": 1})

    @pl.when(c == 1)
    def _():
        pl.semaphore_wait(ok.at[0], 1)

    for p in x_peers:
        send(hp_s.at[p >> log2(nc)], hp.at[col], 0, xdev(p))
        send(pack.at[p & (nc - 1)], crit.at[col], 0, xdev(p))
    sent(hp, ncol - 1)
    sent(crit, ncol - 1)
    crit[pl.ds(col, 1)] = pack[pl.ds(c, 1)]
    hp[pl.ds(col, 1)] = hp_s[pl.ds(x, 1)]
    l_rot = loads(1, [
        (w_rotkey.at[:, own_pf], rotw.at[pl.ds(0, HEAD_ROT)]),
        (w_rotkey.at[pl.ds(half, half), own_pf], rotw.at[pl.ds(64, half)]),
        (w_rotkey.at[pl.ds(0, half), own_pf], rotw.at[pl.ds(64 + half, half)]),
        (attn_gain, again),
        (ffn_gain, fgain),
        (latent_gain, lgain),
        (w_key_up, keyup), (cache_rotkey, crot), (trig, trg), (route_ids, ids), (route_scores, scores), (freq, fr),
    ])
    l_len = pltpu.make_async_copy(lengths, lens, lsem.at[2])
    l_len.start()
    l_att = loads(3, [(cache_latent, cache), (w_value_up, valup)])
    l_bg = loads(4, [
        (w_attn_out.at[:, own_hv], bgs.at[:, pl.ds(0, HV)]),
        (w_shared_gate, bgs.at[:, pl.ds(HV, HIDDEN)]),
        (w_shared_up, bgs.at[:, pl.ds(HV + HIDDEN, HIDDEN)]),
        (w_shared_out, so.at[col]),
    ])
    l_exp = loads(5, [(w_exp_down.at[0], wd)] + [
        (w.at[:, i], wgu.at[i, :, :, pl.ds(HIDDEN * j, HIDDEN)])
        for i in range(ncol) for j, w in enumerate((w_exp_gate, w_exp_up))
    ])

    done(l_rot)
    l_len.wait()
    cos_t, sin_t = trg[0], trg[1]
    for s in range(SEQS):
        low = crot[s, pl.ds(0, half), :].astype(F32)
        high = crot[s, pl.ds(half, half), :].astype(F32)
        krot[s, pl.ds(0, half), :] = low * cos_t - high * sin_t
        krot[s, pl.ds(half, half), :] = low * sin_t + high * cos_t
    spread_r = iota((LOCAL_HEADS * HEAD_KEY, QW), 0)
    spread = ones_where(iota((LOCAL_HEADS * HEAD_KEY, QW), 1) == spread_r + HEAD_ROT * (spread_r >> log2(HEAD_KEY)))
    ka[pl.ds(0, LATENT), :] = dot(keyup[...], spread).astype(BF16)
    lane_q = iota((256, QW), 1)
    head_q = ones_where(lane_q >= PER_HEAD, jnp.int32)
    for h in range(2, LOCAL_HEADS):
        head_q = head_q + ones_where(lane_q >= h * PER_HEAD, jnp.int32)
    within = lane_q - PER_HEAD * head_q - HEAD_KEY
    row_q = iota((256, QW), 0)
    want = jnp.where(row_q < 128, row_q, (row_q - 128) ^ half)
    limit = jnp.where(row_q < 128, row_q, row_q - 128)
    ka[pl.ds(LATENT, 256), :] = ones_where((within == want) & (limit < HEAD_ROT))
    rot_rows = iota((128, pf), 0)
    rot_w = jnp.where((rot_rows & 63) < HEAD_ROT, rotw[...].astype(F32), 0.0).astype(BF16)

    def others_ready(when):
        @pl.when((c == 1) & when)
        def _():
            pl.semaphore_wait(bar, nc * (nz - 1) + nc * (nt - 1))
            signal(ok.at[1], {"c": 0})
            for p in y_peers:
                for core in range(nc):
                    signal(ok.at[2], {"y": p, "c": core})

    others_ready(z >= nz // 2)

    take_bytes((ncol - 1) * (nbytes(crit) + nbytes(hp)) // ncol, rsem.at[slot[0]])
    sel_a = ones_where(iota((nc * rows, hw), 0) == iota((nc * rows, hw), 1))
    hid = hp[...].reshape(pf, hw)
    h_t = dot(sel_a, hid, NT)
    scaled = (h_t * again[pl.ds(z, 1), :]).astype(BF16)
    pall[:, pl.ds(0, wa)] = dot(scaled, crit[:, :, pl.ds(0, wa)].reshape(pf, wa))
    rot = dot(scaled, rot_w, NT)
    square = jnp.sum(h_t * h_t, axis=1, keepdims=True)
    pall[:, pl.ds(wa, 128)] = jnp.where(iota((nc * rows, 128), 1) == HEAD_ROT, square, rot)
    for i in range(nc * nz):
        za_s[i] = pall[pl.ds(SEQS * i, SEQS), :]

    others_ready(z < nz // 2)

    @pl.when(c == 0)
    def _():
        pl.semaphore_wait(ok.at[1], 1)

    zc_peers = [(p, d) for p in z_peers for d in range(nc)] + [(z, 1)]
    for core in range(nc):

        @pl.when(c == core)
        def _():
            lanes = pl.ds(0, wa if core else wa + 128)
            dst = (za_r, zb_r)[core]
            for p, d in zc_peers:
                e = (core + d) % nc
                send(za_s.at[e * nz + p, :, lanes], dst.at[z], 2 + 12 * core, {"z": p, "c": e})
            dst[pl.ds(z, 1)] = za_s[pl.ds(core * nz + z, 1), :, lanes]

    size_a, size_b = nbytes(za_r) // nz, nbytes(zb_r) // nz

    pl.semaphore_wait(ok.at[2], nt - 1)
    done(l_bg)

    groups = sorted(range(nt), key=lambda k: -min(k, nt - k))
    def first_stage(src, dst, k):
        for g in groups:
            dev = {"z": (z + zy * g) & (nz - 1), "y": y_to}
            if g:
                send(src, dst.at[ring, y], k, dev)
            else:

                @pl.when(y_to != y)
                def _():
                    send(src, dst.at[ring, y], k, dev)

                @pl.when(y_to == y)
                def _():
                    dst[pl.ds(ring, 1), pl.ds(y, 1)] = src[...].reshape(1, 1, FEATS, HV)

    first_stage(bgs.at[:, pl.ds(0, HV)], aoc, 1)

    @pl.when(y_to == y)
    def _():
        for g in groups[:-1]:
            send(hidn, hc.at[ring], 3, {"z": ((z + zy * g) & (nz - 1))})
        hc[pl.ds(ring, 1)] = hidn[...].reshape(1, FEATS, batch)

    for p in x_peers:
        send(so.at[col], so.at[col], 4, xdev(p))
    sent(so, ncol - 1)

    for core in range(nc):

        @pl.when(c == core)
        def _():
            take_bytes((nz - 1 + core) * size_a + (nz - core) * size_b, rsem.at[2])

    tot, tot_b = za_r[0], zb_r[0]
    for i in range(1, nz):
        tot = tot + za_r[i]
        tot_b = tot_b + zb_r[i]
    lane2 = iota((SEQS, 128), 1)
    tail = tot[:, wa:]
    sq = jnp.sum(jnp.where(lane2 == HEAD_ROT, tail, 0.0), axis=1, keepdims=True)
    scale = lax.rsqrt(sq / width + EPSILON)
    yb[pl.ds(y, 1)] = rounded(tot_b[:, QW - wa :] * scale).reshape(1, SEQS, lq)
    for p in y_peers:
        send(yb.at[y], yb.at[y], 5, {"y": p})
    sent(yb, nt - 1)
    first_stage(bgs.at[:, pl.ds(HV, HV)], sgc, 6)
    q = rounded(jnp.concatenate([tot[:, :wa], tot_b[:, : QW - wa]], axis=1) * scale)
    nrows = SEQS * LOCAL_HEADS
    r8 = iota((nrows, 128), 0)
    first8 = r8 < LOCAL_HEADS

    def per_row(v):
        top = iota((nrows, v.shape[1]), 0) < LOCAL_HEADS
        return jnp.where(top, v[0:1, :], v[1:2, :])

    lane_8 = iota((nrows, QW), 1)
    first = (iota((nrows, QW), 0) & (LOCAL_HEADS - 1)) * PER_HEAD
    q8 = jnp.where((lane_8 >= first) & (lane_8 < first + PER_HEAD), per_row(q), 0.0).astype(BF16)
    qa = dot(q8, ka[...], NT)
    absorbed = qa[:, :LATENT].astype(BF16)
    len8 = jnp.where(first8, lens[0], lens[1])
    angle = len8.astype(F32) * fr[pl.ds(0, 1), :]
    cos8 = jnp.cos(angle)
    lane8 = iota((nrows, 128), 1)
    sin8 = jnp.where((lane8 & half) == 0, -jnp.sin(angle), jnp.sin(angle))
    q_rot = qa[:, LATENT : LATENT + 128] * cos8 + qa[:, LATENT + 128 : LATENT + 256] * sin8

    done(l_att)
    q32 = q_rot[:, :HEAD_ROT]
    per_seq = [dot(absorbed, cache[s], NT) + dot(q32, krot[s], NN, HIGHEST) for s in range(SEQS)]
    top_rows = iota((nrows, CACHE), 0) < LOCAL_HEADS
    score_scale = PER_HEAD**-0.5
    live = iota((nrows, CACHE), 1) < jnp.where(top_rows, lens[0], lens[1])
    cache_score = jnp.where(live, score_scale * jnp.where(top_rows, per_seq[0], per_seq[1]), -1e30)
    best = jnp.max(cache_score, axis=1, keepdims=True)
    cache_weight = jnp.exp(cache_score - best)
    cache_total = jnp.sum(cache_weight, axis=1, keepdims=True)
    cache_weight = cache_weight.astype(BF16)
    ctx = [dot(cache_weight, cache[s]) for s in range(SEQS)]
    ctx = jnp.where(iota((nrows, LATENT), 0) < LOCAL_HEADS, ctx[0], ctx[1])

    new_rot = rounded(tail * scale)
    o_rotkey[...] = new_rot[:, :HEAD_ROT].astype(BF16)
    new_swap = pltpu.roll(new_rot, 64, 1)
    own_rot = jnp.where(lane8 < HEAD_ROT, per_row(new_rot) * cos8 + per_row(new_swap) * sin8, 0.0)

    size_bg, size_h = nbytes(bgs) // 2, nbytes(hc) // zy
    beside = [r if 2 * r <= zy else r - zy for r in range(1, zy)]
    far = ((y_to - y) & (nt - 1)) == nt // 2

    def forward_rows(when):
        for here in (True, False):

            @pl.when(when & ((y_to == y) if here else (y_to != y)))
            def _():
                take_bytes((nt - 1) * size_bg if here else nt * size_bg + size_h, rsem.at[1])

        @pl.when(when)
        def _():
            for r in sorted(beside, key=lambda r: -abs(r)):
                dev = {"z": (z + r + nz) & (nz - 1)}
                send(hc.at[ring], hc.at[ring], 17, dev)
                send(aoc.at[ring], aoc.at[ring], 15, dev)

    def forward_shared(when):
        for here in (True, False):

            @pl.when(when & ((y_to == y) if here else (y_to != y)))
            def _():
                take_bytes((nt - 1 if here else nt) * size_bg, rsem.at[slot[6]])

        @pl.when(when)
        def _():
            for r in sorted(beside, key=lambda r: -abs(r)):
                send(sgc.at[ring], sgc.at[ring], 16, {"z": (z + r + nz) & (nz - 1)})

    forward_rows(jnp.logical_not(far))
    arrived(yb, nt - 1, 5)
    raw = jnp.concatenate([yb[i] for i in range(nt)], axis=1)
    new_latent = (
        raw * lax.rsqrt(jnp.mean(raw * raw, axis=1, keepdims=True) + EPSILON) * lgain[...]
    ).astype(BF16)
    o_latent[...] = new_latent
    lat8 = per_row(new_latent.astype(F32))
    own_score = score_scale * (
        jnp.sum(absorbed.astype(F32) * lat8, axis=1, keepdims=True)
        + jnp.sum(q_rot * own_rot, axis=1, keepdims=True)
    )
    top_score = jnp.maximum(best, own_score)
    rescale = jnp.exp(best - top_score)
    own_weight = jnp.exp(own_score - top_score)
    denominator = rescale * cache_total + own_weight
    context = (rescale / denominator) * ctx + rounded(own_weight / denominator) * lat8
    ho = dot(context.astype(BF16), valup[...])
    r_h = iota((nrows, HV), 0)
    ho = jnp.where((iota((nrows, HV), 1) >> log2(HEAD_VAL)) == (r_h & (LOCAL_HEADS - 1)), ho, 0.0)
    h0 = jnp.sum(jnp.where(r_h < LOCAL_HEADS, ho, 0.0), axis=0, keepdims=True)
    h1 = jnp.sum(jnp.where(r_h < LOCAL_HEADS, 0.0, ho), axis=0, keepdims=True)
    heads = rounded(jnp.where(iota((SEQS, HV), 0) == 0, h0, h1))
    ha[pl.ds(place_of, 1)] = heads.astype(BF16).reshape(1, SEQS, HV)
    for dev in plane_peers:
        send(ha.at[place_of], ha.at[place_of], 7, dev)
    sent(ha, npl - 1)

    forward_rows(far)
    for buf in (hc, aoc, sgc):
        sent(buf, zy - 1)

    rs = scores[...]
    rw = ROUTED_SCALE * rs / jnp.sum(rs, axis=0, keepdims=True)
    idv = ids[...]
    nex = nz + ncol
    which = iota((nex, batch), 0)
    target = jnp.where(which < nz, which * ncol + col, z * ncol + which - nz)
    hit = jnp.zeros((nex, batch), F32)
    wgt = jnp.zeros((nex, batch), F32)
    for k in range(4):
        same = idv[k : k + 1, :] == target
        hit = jnp.where(same, 1.0, hit)
        wgt = jnp.where(same, rw[k : k + 1, :], wgt)
    before = ones_where(iota((batch, batch), 0) < iota((batch, batch), 1))
    rank = dot(hit.astype(BF16), before)
    val = jnp.where(hit > 0.0, rank, -1.0).astype(BF16)
    pslot = ncol * SLOTS

    def pick(upper, shape, token_axis):
        t, p = iota(shape, token_axis), iota(shape, 1 - token_axis)
        return ones_where((t >> log2(th)) == 2 * (p >> log2(th)) + upper, jnp.int32) * ones_where(
            (t & (th - 1)) == (p & (th - 1)), jnp.int32
        )

    expand_p = ones_where(iota((pslot, nex), 1) == nz + (iota((pslot, nex), 0) >> log2(SLOTS)))
    slot_p = (iota((pslot, nz * th), 0) & (SLOTS - 1)).astype(F32)
    for i in range(2):
        part = dot(val, pick(i, (batch, nz * th), 0).astype(F32).astype(BF16)).astype(BF16)
        sel_p[i] = ones_where(dot(expand_p, part) == slot_p)

    gain_rows = jnp.broadcast_to(fgain[...][:, None, :], (nz, ncol, pf)).reshape(nz * ncol, pf)
    gr = iota((nz * ncol, pf), 0)
    gain_rows = jnp.where((iota((nz * ncol, pf), 1) >> log2(FEATS)) == (gr & (ncol - 1)), gain_rows, 0.0)
    tile_f = jnp.where(
        (iota((pf, 2 * cf), 0) & (FEATS - 1)) == (iota((pf, 2 * cf), 1) & (FEATS - 1)), 1.0, 0.0
    )
    tiled = dot(gain_rows, tile_f, NN, HIGHEST).reshape(nz, ncol, 2 * cf)
    lane_z = iota((ncol, 2 * cf), 1) >> log2(FEATS)
    for k in range(nt // 2):
        g = jnp.zeros((ncol, 2 * cf), F32)
        for i in range(2 * zy):
            g = jnp.where(lane_z == i, tiled[2 * zy * k + i], g)
        gp[k] = g

    forward_shared(jnp.logical_not(far))
    if beside:
        take_bytes((zy - 1) * (nbytes(hc) + nbytes(aoc)) // zy, rsem.at[slot[15]])
    t_i, l_i = iota((tok, batch), 0), iota((tok, batch), 1)
    sel_h = ones_where(l_i == z * tok + t_i)
    hcv = hc[...].reshape(cf, batch)
    hid_c = dot(sel_h, jnp.concatenate([hcv, hcv], axis=0), NT)
    arrived(ha, npl - 1, 7)
    for i in range(ncol):
        for j in range(nt):
            h16[pl.ds(SEQS * i, SEQS), pl.ds(HV * j, HV)] = ha[i * nt + j].astype(F32)
    attn = jnp.zeros((tok, 2 * cf), F32)
    for j in range(nt):
        w = jnp.concatenate([aoc[i, j] for i in range(zy)] * 2, axis=0)
        attn = attn + dot(h16[:, pl.ds(HV * j, HV)].astype(BF16), w, NT)
    mid = rounded(hid_c + rounded(attn))
    low8 = iota((th, 2 * cf), 1) < cf
    mz[pl.ds(z, 1)] = jnp.where(low8, mid[:th], mid[th:]).astype(BF16).reshape(1, th, 2 * cf)
    for p in z_peers:
        send(mz.at[z], mz.at[z], 8, {"z": p})
    sent(mz, nz - 1)

    forward_shared(far)

    mine = (iota((tok, 2 * cf), 1) >> log2(cf)) == (y & 1)
    mid = jnp.where(mine, mid, 0.0)
    ffn = (mid * gp[pl.ds(y >> 1, 1), pl.ds(col, 1)].reshape(1, 2 * cf)).astype(BF16)
    square = jnp.broadcast_to(jnp.sum(mid * mid, axis=1, keepdims=True), (tok, 128))
    take_bytes((zy - 1) * nbytes(sgc) // zy + (ncol - 1) * nbytes(so) // ncol, rsem.at[slot[16]])
    for j in range(nt):
        w = jnp.concatenate([sgc[i, j] for i in range(zy)] * 2, axis=0)
        sp[:, pl.ds(0, 2 * HIDDEN)] = dot(ffn, w)
        sp[:, pl.ds(2 * HIDDEN, 128)] = square
        for i in range(ncol):
            sh_s[i * nt + j] = sp[pl.ds(SEQS * i, SEQS), :]
    for dev in plane_peers:
        send(sh_s.at[(dev["x"] * nc + dev["c"]) * nt + dev["y"]], sh_r.at[place_of], 9, dev)
    sent(sh_s, npl - 1)
    sh_r[pl.ds(place_of, 1)] = sh_s[pl.ds(place_of, 1)]

    expand = ones_where(iota((nslot, nex), 1) == (iota((nslot, nex), 0) >> log2(SLOTS)))
    slot_i = (iota((nslot, batch), 0) & (SLOTS - 1)).astype(F32)
    in_slot = dot(expand, val) == slot_i
    w_hi = wgt.astype(BF16)
    w_lo = (wgt - w_hi.astype(F32)).astype(BF16)
    wt[pl.ds(0, nslot), :] = jnp.where(in_slot, dot(expand, w_hi), 0.0).astype(BF16)
    wt[pl.ds(nslot, nslot), :] = jnp.where(in_slot, dot(expand, w_lo), 0.0).astype(BF16)
    arrived(mz, nz - 1, 8)
    mid_all = mz[...].reshape(nz * th, 2 * cf)
    low = iota((pslot, 2 * cf), 1) < cf
    tk = jnp.where(low, dot(sel_p[0], mid_all), dot(sel_p[1], mid_all))
    tk = (tk + pltpu.roll(tk, cf, 1)).reshape(ncol, 2, sh, 2 * cf)
    tk_s[...] = jnp.where(iota((ncol, sh, 2 * cf), 2) < cf, tk[:, 0], tk[:, 1]).astype(BF16)
    for dev in plane_peers:
        send(tk_s.at[dev["x"] * nc + dev["c"]], tk_r.at[place_of], 10, dev)
    sent(tk_r, npl - 1)
    tk_r[pl.ds(place_of, 1)] = tk_s[pl.ds(col, 1)]
    f_i, l_i = iota((pf, 2 * cf), 0), iota((pf, 2 * cf), 1)
    own_f = ((f_i >> log2(FEATS)) == col) & (y_to == y)
    own_l = ring * FEATS + (f_i & (FEATS - 1))
    tot0[...] = jnp.zeros((pf, batch), F32)
    for i in range(2):
        part = dot(ones_where(own_f & (l_i == own_l + cf * i)), mid_all, NT).astype(BF16)
        tot0[...] += dot(part, pick(i, (nz * th, batch), 1).astype(F32).astype(BF16))

    arrived(sh_r, npl - 1, 9)
    tot = sh_r[0]
    for i in range(1, npl):
        tot = tot + sh_r[i]
    scale = lax.rsqrt(tot[:, 2 * HIDDEN : 2 * HIDDEN + 1] / width + EPSILON)
    gate = scale * tot[:, :HIDDEN]
    act = rounded(gate / (1.0 + jnp.exp(-gate)) * (scale * tot[:, HIDDEN : 2 * HIDDEN]))
    zs[pl.ds(z, 1)] = act.reshape(1, SEQS, HIDDEN)
    for p in z_peers:
        send(zs.at[z], zs.at[z], 11, {"z": p})
    sent(zs, nz - 1)

    done(l_exp)
    arrived(tk_r, npl - 1, 10)
    pieces = []
    low_s = iota((sh, 2 * cf), 1) < cf
    sq = jnp.zeros((SLOTS, 2 * cf), F32)
    for i in range(ncol):
        for k in range(nt // 2):
            va = tk_r[i * nt + 2 * k].astype(F32)
            vb = tk_r[i * nt + 2 * k + 1].astype(F32)
            v = jnp.concatenate(
                [jnp.where(low_s, va, pltpu.roll(vb, cf, 1)), jnp.where(low_s, pltpu.roll(va, cf, 1), vb)], axis=0
            )
            sq = sq + v * v
            pieces.append((v * gp[k, pl.ds(i, 1), :]).astype(BF16))
    gu = dot(jnp.concatenate(pieces, axis=1), wgu[...].reshape(width, 2 * HIDDEN))
    scale = lax.rsqrt(jnp.sum(sq, axis=1, keepdims=True) / width + EPSILON)
    gate = scale * gu[:, :HIDDEN]
    act = (gate / (1.0 + jnp.exp(-gate)) * (scale * gu[:, HIDDEN:])).astype(BF16)
    for p in z_peers + [z]:
        zh_s[pl.ds(p, 1)] = dot(act, wd[:, pl.ds(pl.multiple_of(p * pf, pf), pf)]).astype(BF16).reshape(1, SLOTS, pf)
        if p is not z:
            send(zh_s.at[p], zh_r.at[z], 12, {"z": p})
    sent(zh_s, nz - 1)
    zh_r[pl.ds(z, 1)] = zh_s[pl.ds(z, 1)]

    arrived(zs, nz - 1, 11)
    for i in range(nz):
        s32[pl.ds(SEQS * i, SEQS), :] = zs[i]
    b_i, r_i = iota((batch, rows), 0), iota((batch, rows), 1)
    place = ones_where(b_i == (r_i >> 1) * tok + col * SEQS + (r_i & 1))
    spread_act = dot(place, s32[...].astype(BF16)).astype(BF16)
    total = tot0[...] + dot(so[...].reshape(pf, HIDDEN), spread_act, NT)
    arrived(zh_r, nz - 1, 12)
    parts = zh_r[...].reshape(nslot, pf)
    total = total + dot(parts, wt[pl.ds(0, nslot), :], TN) + dot(parts, wt[pl.ds(nslot, nslot), :], TN)
    total = total.reshape(ncol, 2, FEATS // 2, batch)
    low_lane = iota((ncol, FEATS // 2, hl), 2) < ob
    for k in range(nt // 2):
        ta = total[:, 0, :, hl * k : hl * (k + 1)]
        tb = total[:, 1, :, hl * k : hl * (k + 1)]
        flat = (ncol * FEATS // 2, hl)
        ra = pltpu.roll(ta.reshape(flat), ob, 1).reshape(ta.shape)
        rb = pltpu.roll(tb.reshape(flat), ob, 1).reshape(tb.shape)
        pd_s[:, 2 * k] = jnp.where(low_lane, ta, rb)
        pd_s[:, 2 * k + 1] = jnp.where(low_lane, ra, tb)
    for dev in plane_peers:
        send(pd_s.at[dev["x"] * nc + dev["c"], dev["y"]], pd_r.at[place_of], 13, dev)
    sent(pd_r, npl - 1)
    pd_r[pl.ds(place_of, 1)] = pd_s[pl.ds(col, 1), pl.ds(y, 1)].reshape(1, FEATS // 2, hl)
    arrived(pd_r, npl - 1, 13)
    tot = pd_r[0]
    for i in range(1, npl):
        tot = tot + pd_r[i]
    both = jnp.concatenate([tot, pltpu.roll(tot, ob, 1)], axis=0)
    o_mixed[...] = both[:, :ob].astype(BF16)

    for core in range(nc):
        for here in (True, False):

            @pl.when((c == core) & ((y_to == y) if here else (y_to != y)))
            def _():
                mine = (nc * nz - 1) * (size_b if core else size_a)
                mine += (nt - 1) * (2 * size_bg + size_h) if here else nt * 2 * size_bg
                take_bytes(sum(pending) + mine, ssem.at[0])


def finish(*refs):
    copies = [pltpu.make_async_copy(refs[i], refs[3 + i], refs[6].at[i]) for i in range(3)]
    for cp in copies:
        cp.start()
    for cp in copies:
        cp.wait()


def body(nz, nx, nc, nt, *args):
    args = list(args)
    ncol = nx * nc
    pf = FEATS * ncol
    rows = SEQS * nz
    batch = rows * ncol
    lq = LATENT // nt
    nslot = nz * SLOTS
    hl = 2 * (batch // nt)
    wa = 2 * 128
    for i in (1, 12):
        args[i] = args[i].reshape(nz, pf)
    args[5] = args[5].reshape(1, LATENT)
    args[13], args[14] = args[13].T, args[14].T
    for i in (15, 16):
        args[i] = args[i].reshape(nz, ncol, FEATS, HIDDEN)
    half = HEAD_ROT // 2
    frequency = THETA_BASE ** (-np.arange(half, dtype=np.float64) / half)
    angles = frequency.astype(np.float32)[:, None] * np.arange(CACHE, dtype=np.float32)[None, :]
    trig = jnp.asarray(np.stack([np.cos(angles.astype(np.float64)), np.sin(angles.astype(np.float64))]).astype(np.float32))
    freq = jnp.asarray(np.tile(frequency.astype(np.float32), (2, 128 // half)))
    vm = pltpu.VMEM
    tok = ncol * SEQS
    cf = FEATS * nz // nt
    npl = ncol * nt
    scratch = [
        vm((nc, FEATS, wa), BF16), vm((ncol, FEATS, wa), BF16),
        vm((FEATS, batch), BF16), vm((nx, FEATS, max(128, nc * rows)), BF16), vm((ncol, FEATS, max(128, nc * rows)), BF16),
        vm((ncol, FEATS, HIDDEN), BF16),
        vm((FEATS, 2 * HV), BF16),
        vm((nz // nt, nt, FEATS, HV), BF16), vm((nz // nt, nt, FEATS, HV), BF16),
        vm((nz // nt, FEATS, batch), BF16),
        vm((128, pf), BF16),
        vm((nz, pf), F32), vm((nz, pf), F32), vm((1, LATENT), F32), vm((2, 128), F32),
        vm((LATENT, LOCAL_HEADS * HEAD_KEY), BF16), vm((LATENT, HV), BF16),
        vm((SEQS, CACHE, LATENT), BF16), vm((SEQS, HEAD_ROT, CACHE), BF16),
        pltpu.SMEM((SEQS,), jnp.int32),
        vm((4, batch), jnp.int32), vm((4, batch), F32),
        vm((ncol, nz, FEATS, 2 * HIDDEN), BF16), vm((HIDDEN, pf * nz), BF16),
        vm((2, half, CACHE), F32),
        vm((nc * nz, SEQS, wa + 128), F32), vm((nz, SEQS, wa + 128), F32), vm((nz, SEQS, wa), F32),
        vm((nt, SEQS, lq), F32),
        vm((npl, SEQS, HV), BF16),
        vm((nz, tok // 2, 2 * cf), BF16),
        vm((npl, SEQS, 2 * HIDDEN + 128), F32), vm((npl, SEQS, 2 * HIDDEN + 128), F32),
        vm((ncol, SLOTS // 2, 2 * cf), BF16), vm((npl, SLOTS // 2, 2 * cf), BF16),
        vm((nz, SLOTS, pf), BF16), vm((nz, SLOTS, pf), BF16),
        vm((nz, SEQS, HIDDEN), F32),
        vm((ncol, nt, FEATS // 2, hl), F32), vm((npl, FEATS // 2, hl), F32),
        vm((LATENT + 256, QW), BF16),
        vm((SEQS, HEAD_ROT, CACHE), F32),
        vm((2, ncol * SLOTS, batch // 2), BF16),
        vm((2 * nslot, batch), BF16),
        vm((tok, nt * HV), F32),
        vm((rows, HIDDEN), F32),
        vm((nc * rows, wa + 128), F32),
        vm((tok, 2 * HIDDEN + 128), F32),
        vm((nt // 2, ncol, 2 * cf), F32),
        vm((pf, batch), F32),
        pltpu.SemaphoreType.DMA((6,)),
        pltpu.SemaphoreType.DMA((1,)),
        pltpu.SemaphoreType.DMA((14,)),
        pltpu.SemaphoreType.REGULAR((3,)),
        vm((2560 * 1024 // UNIT, 2, UNIT // 8), F32),
    ]
    anywhere = pl.BlockSpec(memory_space=pltpu.HBM)
    results = pl.pallas_call(
        functools.partial(kernel, nz, nx, nc, nt),
        out_shape=(
            pltpu.VMEM((FEATS, hl // 2), BF16),
            pltpu.VMEM((SEQS, LATENT), BF16),
            pltpu.VMEM((SEQS, HEAD_ROT), BF16),
        ),
        in_specs=[anywhere] * 23,
        out_specs=(pl.BlockSpec(memory_space=pltpu.VMEM),) * 3,
        scratch_shapes=scratch,
        compiler_params=pltpu.CompilerParams(collective_id=0, has_side_effects=True, vmem_limit_bytes=66977792),
        name="layer",
    )(*args, trig, freq)
    results = [pltpu.with_memory_space_constraint(r, pltpu.VMEM) for r in results]
    return pl.pallas_call(
        finish,
        out_shape=(
            jax.ShapeDtypeStruct((FEATS, hl // 2), BF16),
            jax.ShapeDtypeStruct((SEQS, LATENT), BF16),
            jax.ShapeDtypeStruct((SEQS, HEAD_ROT), BF16),
        ),
        in_specs=[pl.BlockSpec(memory_space=pltpu.VMEM)] * 3,
        out_specs=(anywhere,) * 3,
        scratch_shapes=[pltpu.SemaphoreType.DMA((3,))],
        name="finish",
    )(*results)


EP = ("z", "x", "c")


def build(devices):
    split = Mesh(devices, ("z", "x", "c", "y"))
    return jax.shard_map(
        functools.partial(body, *devices.shape),
        mesh=split,
        in_specs=(
            P(EP, None),
            P(),
            P(EP, "y"),
            P(EP, None),
            P(),
            P(),
            P(None, "y"),
            P(None, "y"),
            P(EP, None),
            P(EP, None, None),
            P(EP, None, None),
            P(EP),
            P(),
            P(),
            P(),
            P(EP, None, "y"),
            P(EP, None, "y"),
            P(EP, "y", None),
            P(EP, "y"),
            P(EP, "y"),
            P(EP, "y"),
        ),
        out_specs=(P(EP, "y"), P(EP, None), P(EP, None)),
        check_vma=False,
    )


def solution(mesh):
    return build(mesh.devices.reshape(16, 4, 2, mesh.shape["tp"]))
```

```python
import functools
import math

import jax
import jax.numpy as jnp
import numpy as np
from jax import lax
from jax.experimental import pallas as pl
from jax.experimental.pallas import tpu as pltpu
from jax.sharding import Mesh
from jax.sharding import PartitionSpec as P

MESH = pl.DeviceIdType.MESH
F32 = jnp.float32
BF16 = jnp.bfloat16
HIGHEST = lax.Precision.HIGHEST
NN = (((1,), (0,)), ((), ()))
NT = (((1,), (1,)), ((), ()))
TN = (((0,), (0,)), ((), ()))

LOCAL_HEADS = 4
HEAD_KEY = 64
HEAD_ROT = 32
HEAD_VAL = 64
PER_HEAD = HEAD_KEY + HEAD_ROT
LATENT = 512
CACHE = 1024
HIDDEN = 128
SLOTS = 16
FEATS = 16
SEQS = 2
EPSILON = 1e-06
THETA_BASE = 10000.0
ROUTED_SCALE = 2.5
QW = LOCAL_HEADS * PER_HEAD
HV = LOCAL_HEADS * HEAD_VAL
UNIT = 1024


def dot(a, b, dims=NN, precision=None):
    return lax.dot_general(a, b, dims, precision=precision, preferred_element_type=F32)


def iota(shape, axis):
    return lax.broadcasted_iota(jnp.int32, shape, axis)


def ones_where(mask, dtype=BF16):
    return jnp.where(mask, 1.0, 0.0).astype(dtype)


def rounded(v):
    return v.astype(BF16).astype(F32)


def log2(n):
    return n.bit_length() - 1


def kernel(nz, nx, nc, nt, *refs):
    (
        hidden, attn_gain, w_query, w_latent, w_rotkey, latent_gain, w_key_up, w_value_up, w_attn_out, cache_latent, cache_rotkey,
        lengths, ffn_gain, route_ids, route_scores, w_exp_gate, w_exp_up, w_exp_down, w_shared_gate, w_shared_up, w_shared_out,
        trig, freq,
        o_mixed, o_latent, o_rotkey,
        pack, crit, hidn, hp_s, hp, so, bgs, aoc, sgc, hc, rotw, again, fgain, lgain, fr, keyup, valup, cache, crot, lens, ids, scores, wgu, wd, trg,
        za_s, za_r, zb_r, yb, ha, mz, sh_s, sh_r, tk_s, tk_r, zh_s, zh_r, zs, pd_s, pd_r,
        ka, krot, sel_p, wt, h16, s32, pall, sp, gp, tot0,
        lsem, ssem, rsem, ok, ruler,
    ) = refs
    ncol = nx * nc
    pf = FEATS * ncol
    rows = SEQS * nz
    batch = rows * ncol
    width = pf * nz
    lq = LATENT // nt
    nslot = nz * SLOTS
    ob = batch // nt
    hl = 2 * ob
    wa = 2 * 128
    hw = max(128, nc * rows)
    zy = nz // nt
    tok = ncol * SEQS
    cf = FEATS * zy
    npl = ncol * nt
    th, sh = tok // 2, SLOTS // 2
    z, x, c, y = (lax.axis_index(a) for a in ("z", "x", "c", "y"))
    col = x * nc + c
    place_of = col * nt + y
    y_to = ((z) >> log2(zy))
    ring = ((z) & (zy - 1))

    def xdev(p):
        return {"x": ((p) >> log2(nc)), "c": ((p) & (nc - 1))}

    z_order = sorted(range(1, nz), key=lambda d: -min(d, nz - d))
    z_peers = [((z + d) & (nz - 1)) for d in z_order]
    x_order = sorted(range(1, ncol), key=lambda d: -min(d, ncol - d))
    x_peers = [((col + d) & (ncol - 1)) for d in x_order]
    y_peers = [((y + d) & (nt - 1)) for d in range(1, nt)]
    plane_order = sorted(
        [(dx, dc, dy) for dx in range(nx) for dc in range(nc) for dy in range(nt) if dx or dc or dy],
        key=lambda t: -(min(t[0], nx - t[0]) + min(t[2], nt - t[2])),
    )
    plane_peers = [
        {"x": ((x + dx) & (nx - 1)), "c": ((c + dc) & (nc - 1)), "y": ((y + dy) & (nt - 1))} for dx, dc, dy in plane_order
    ]

    bar = pltpu.get_barrier_semaphore()

    def signal(sem, dev):
        pl.semaphore_signal(sem, inc=1, device_id=dev, device_id_type=MESH)

    for d in range(nx - 1, 0, -1):
        signal(bar, {"x": ((x + d) & (nx - 1)), "c": 0})

    @pl.when(c == 1)
    def _():
        signal(bar, {"c": 0})

    sig_first = nz // 4
    for p in z_peers[:sig_first]:
        signal(bar, {"z": p, "c": 1})

    def nbytes(ref):
        return math.prod(ref.shape) * jnp.dtype(ref.dtype).itemsize

    def rows_of(n):
        assert n % UNIT == 0 and n // UNIT <= ruler.shape[0]
        return ruler.at[pl.ds(0, n // UNIT)]

    def loads(sem, pairs):
        for src, dst in pairs:
            pltpu.make_async_copy(src, dst, lsem.at[sem]).start()
        part = rows_of(sum(nbytes(dst) for _, dst in pairs))
        return [(part, sem)]

    def done(copies):
        for part, sem in copies:
            pltpu.make_async_copy(part, part, lsem.at[sem]).wait()

    own_lq = pl.ds(pl.multiple_of(y * lq, lq), lq)
    own_hv = pl.ds(pl.multiple_of(y * HV, HV), HV)
    own_pf = pl.ds(pl.multiple_of(z * pf, pf), pf)
    half = HEAD_ROT // 2
    l_crit = loads(0, [
        (w_query.at[:, pl.ds(0, wa)], pack.at[0, :, pl.ds(0, wa)]),
        (w_query.at[:, pl.ds(wa, QW - wa)], pack.at[1, :, pl.ds(0, QW - wa)]),
        (w_latent.at[:, own_lq], pack.at[1, :, pl.ds(QW - wa, lq)]),
        (hidden, hidn),
    ])

    for p in z_peers[sig_first:]:
        signal(bar, {"z": p, "c": 1})
    for p in y_peers:
        signal(bar, {"y": p, "c": 1})

    def send(src, dst, k, dev):
        cp = pltpu.make_async_remote_copy(
            src_ref=src, dst_ref=dst, send_sem=ssem.at[0], recv_sem=rsem.at[slot[k]], device_id=dev, device_id_type=MESH
        )
        cp.start()

    def take(part, sem):
        pltpu.make_async_copy(part, part, sem).wait()

    def arrived(buf, n, k):
        take(buf.at[pl.ds(0, n)], rsem.at[slot[k]])

    slot = {0: 0, 1: 1, 3: 1, 6: 13, 2: 2, 14: 2, 5: 3, 7: 4, 15: 5, 17: 5, 16: 6, 4: 6, 8: 7, 9: 8, 10: 9, 11: 10, 12: 11, 13: 12}
    pending = []

    def sent(buf, n):
        pending.append(n * nbytes(buf) // buf.shape[0])

    def take_bytes(n, sem):
        take(rows_of(n), sem)

    chip = nc * rows
    order = iota((batch, nx * hw), 1)
    place = order & (hw - 1)
    b_i = ((place & (rows - 1)) >> 1) * tok + ((order >> log2(hw)) * nc + (place >> log2(rows))) * SEQS + (place & 1)
    chosen = ones_where((iota((batch, nx * hw), 0) == b_i) & (place < chip))
    done(l_crit)
    cut = dot(hidn[...], chosen).astype(BF16)
    for i in range(nx):
        hp_s[i] = cut[:, hw * i : hw * (i + 1)]

    @pl.when(c == 0)
    def _():
        pl.semaphore_wait(bar, nc * nx - 1)
        signal(ok.at[0], {"c": 1})

    @pl.when(c == 1)
    def _():
        pl.semaphore_wait(ok.at[0], 1)

    for p in x_peers:
        send(hp_s.at[p >> log2(nc)], hp.at[col], 0, xdev(p))
        send(pack.at[p & (nc - 1)], crit.at[col], 0, xdev(p))
    sent(hp, ncol - 1)
    sent(crit, ncol - 1)
    crit[pl.ds(col, 1)] = pack[pl.ds(c, 1)]
    hp[pl.ds(col, 1)] = hp_s[pl.ds(x, 1)]
    l_rot = loads(1, [
        (w_rotkey.at[:, own_pf], rotw.at[pl.ds(0, HEAD_ROT)]),
        (w_rotkey.at[pl.ds(half, half), own_pf], rotw.at[pl.ds(64, half)]),
        (w_rotkey.at[pl.ds(0, half), own_pf], rotw.at[pl.ds(64 + half, half)]),
        (attn_gain, again),
        (ffn_gain, fgain),
        (latent_gain, lgain),
        (w_key_up, keyup), (cache_rotkey, crot), (trig, trg), (route_ids, ids), (route_scores, scores), (freq, fr),
    ])
    l_len = pltpu.make_async_copy(lengths, lens, lsem.at[2])
    l_len.start()
    l_att = loads(3, [(cache_latent, cache), (w_value_up, valup)])
    l_bg = loads(4, [
        (w_attn_out.at[:, own_hv], bgs.at[:, pl.ds(0, HV)]),
        (w_shared_gate, bgs.at[:, pl.ds(HV, HIDDEN)]),
        (w_shared_up, bgs.at[:, pl.ds(HV + HIDDEN, HIDDEN)]),
        (w_shared_out, so.at[col]),
    ])
    l_exp = loads(5, [(w_exp_down.at[0], wd)] + [
        (w.at[:, i], wgu.at[i, :, :, pl.ds(HIDDEN * j, HIDDEN)])
        for i in range(ncol) for j, w in enumerate((w_exp_gate, w_exp_up))
    ])

    done(l_rot)
    l_len.wait()
    cos_t, sin_t = trg[0], trg[1]
    for s in range(SEQS):
        low = crot[s, pl.ds(0, half), :].astype(F32)
        high = crot[s, pl.ds(half, half), :].astype(F32)
        krot[s, pl.ds(0, half), :] = low * cos_t - high * sin_t
        krot[s, pl.ds(half, half), :] = low * sin_t + high * cos_t
    spread_r = iota((LOCAL_HEADS * HEAD_KEY, QW), 0)
    spread = ones_where(iota((LOCAL_HEADS * HEAD_KEY, QW), 1) == spread_r + HEAD_ROT * (spread_r >> log2(HEAD_KEY)))
    ka[pl.ds(0, LATENT), :] = dot(keyup[...], spread).astype(BF16)
    lane_q = iota((256, QW), 1)
    head_q = ones_where(lane_q >= PER_HEAD, jnp.int32)
    for h in range(2, LOCAL_HEADS):
        head_q = head_q + ones_where(lane_q >= h * PER_HEAD, jnp.int32)
    within = lane_q - PER_HEAD * head_q - HEAD_KEY
    row_q = iota((256, QW), 0)
    want = jnp.where(row_q < 128, row_q, (row_q - 128) ^ half)
    limit = jnp.where(row_q < 128, row_q, row_q - 128)
    ka[pl.ds(LATENT, 256), :] = ones_where((within == want) & (limit < HEAD_ROT))
    rot_rows = iota((128, pf), 0)
    rot_w = jnp.where((rot_rows & 63) < HEAD_ROT, rotw[...].astype(F32), 0.0).astype(BF16)

    def others_ready(when):
        @pl.when((c == 1) & when)
        def _():
            pl.semaphore_wait(bar, nc * (nz - 1) + nc * (nt - 1))
            signal(ok.at[1], {"c": 0})
            for p in y_peers:
                for core in range(nc):
                    signal(ok.at[2], {"y": p, "c": core})

    others_ready(z >= nz // 2)

    take_bytes((ncol - 1) * (nbytes(crit) + nbytes(hp)) // ncol, rsem.at[slot[0]])
    sel_a = ones_where(iota((nc * rows, hw), 0) == iota((nc * rows, hw), 1))
    hid = hp[...].reshape(pf, hw)
    h_t = dot(sel_a, hid, NT)
    scaled = (h_t * again[pl.ds(z, 1), :]).astype(BF16)
    pall[:, pl.ds(0, wa)] = dot(scaled, crit[:, :, pl.ds(0, wa)].reshape(pf, wa))
    rot = dot(scaled, rot_w, NT)
    square = jnp.sum(h_t * h_t, axis=1, keepdims=True)
    pall[:, pl.ds(wa, 128)] = jnp.where(iota((nc * rows, 128), 1) == HEAD_ROT, square, rot)
    for i in range(nc * nz):
        za_s[i] = pall[pl.ds(SEQS * i, SEQS), :]

    others_ready(z < nz // 2)

    @pl.when(c == 0)
    def _():
        pl.semaphore_wait(ok.at[1], 1)

    zc_peers = [(p, d) for p in z_peers for d in range(nc)] + [(z, 1)]
    for core in range(nc):

        @pl.when(c == core)
        def _():
            lanes = pl.ds(0, wa if core else wa + 128)
            dst = (za_r, zb_r)[core]
            for p, d in zc_peers:
                e = (core + d) % nc
                send(za_s.at[e * nz + p, :, lanes], dst.at[z], 2 + 12 * core, {"z": p, "c": e})
            dst[pl.ds(z, 1)] = za_s[pl.ds(core * nz + z, 1), :, lanes]

    size_a, size_b = nbytes(za_r) // nz, nbytes(zb_r) // nz

    pl.semaphore_wait(ok.at[2], nt - 1)
    done(l_bg)

    groups = sorted(range(nt), key=lambda k: -min(k, nt - k))
    def first_stage(src, dst, k):
        for g in groups:
            dev = {"z": (z + zy * g) & (nz - 1), "y": y_to}
            if g:
                send(src, dst.at[ring, y], k, dev)
            else:

                @pl.when(y_to != y)
                def _():
                    send(src, dst.at[ring, y], k, dev)

                @pl.when(y_to == y)
                def _():
                    dst[pl.ds(ring, 1), pl.ds(y, 1)] = src[...].reshape(1, 1, FEATS, HV)

    first_stage(bgs.at[:, pl.ds(0, HV)], aoc, 1)

    @pl.when(y_to == y)
    def _():
        for g in groups[:-1]:
            send(hidn, hc.at[ring], 3, {"z": ((z + zy * g) & (nz - 1))})
        hc[pl.ds(ring, 1)] = hidn[...].reshape(1, FEATS, batch)

    for p in x_peers:
        send(so.at[col], so.at[col], 4, xdev(p))
    sent(so, ncol - 1)

    for core in range(nc):

        @pl.when(c == core)
        def _():
            take_bytes((nz - 1 + core) * size_a + (nz - core) * size_b, rsem.at[2])

    tot, tot_b = za_r[0], zb_r[0]
    for i in range(1, nz):
        tot = tot + za_r[i]
        tot_b = tot_b + zb_r[i]
    lane2 = iota((SEQS, 128), 1)
    tail = tot[:, wa:]
    sq = jnp.sum(jnp.where(lane2 == HEAD_ROT, tail, 0.0), axis=1, keepdims=True)
    scale = lax.rsqrt(sq / width + EPSILON)
    yb[pl.ds(y, 1)] = rounded(tot_b[:, QW - wa :] * scale).reshape(1, SEQS, lq)
    for p in y_peers:
        send(yb.at[y], yb.at[y], 5, {"y": p})
    sent(yb, nt - 1)
    first_stage(bgs.at[:, pl.ds(HV, HV)], sgc, 6)
    q = rounded(jnp.concatenate([tot[:, :wa], tot_b[:, : QW - wa]], axis=1) * scale)
    nrows = SEQS * LOCAL_HEADS
    r8 = iota((nrows, 128), 0)
    first8 = r8 < LOCAL_HEADS

    def per_row(v):
        top = iota((nrows, v.shape[1]), 0) < LOCAL_HEADS
        return jnp.where(top, v[0:1, :], v[1:2, :])

    lane_8 = iota((nrows, QW), 1)
    first = (iota((nrows, QW), 0) & (LOCAL_HEADS - 1)) * PER_HEAD
    q8 = jnp.where((lane_8 >= first) & (lane_8 < first + PER_HEAD), per_row(q), 0.0).astype(BF16)
    qa = dot(q8, ka[...], NT)
    absorbed = qa[:, :LATENT].astype(BF16)
    len8 = jnp.where(first8, lens[0], lens[1])
    angle = len8.astype(F32) * fr[pl.ds(0, 1), :]
    cos8 = jnp.cos(angle)
    lane8 = iota((nrows, 128), 1)
    sin8 = jnp.where((lane8 & half) == 0, -jnp.sin(angle), jnp.sin(angle))
    q_rot = qa[:, LATENT : LATENT + 128] * cos8 + qa[:, LATENT + 128 : LATENT + 256] * sin8

    done(l_att)
    q32 = q_rot[:, :HEAD_ROT]
    per_seq = [dot(absorbed, cache[s], NT) + dot(q32, krot[s], NN, HIGHEST) for s in range(SEQS)]
    top_rows = iota((nrows, CACHE), 0) < LOCAL_HEADS
    score_scale = PER_HEAD**-0.5
    live = iota((nrows, CACHE), 1) < jnp.where(top_rows, lens[0], lens[1])
    cache_score = jnp.where(live, score_scale * jnp.where(top_rows, per_seq[0], per_seq[1]), -1e30)
    best = jnp.max(cache_score, axis=1, keepdims=True)
    cache_weight = jnp.exp(cache_score - best)
    cache_total = jnp.sum(cache_weight, axis=1, keepdims=True)
    cache_weight = cache_weight.astype(BF16)
    ctx = [dot(cache_weight, cache[s]) for s in range(SEQS)]
    ctx = jnp.where(iota((nrows, LATENT), 0) < LOCAL_HEADS, ctx[0], ctx[1])

    new_rot = rounded(tail * scale)
    o_rotkey[...] = new_rot[:, :HEAD_ROT].astype(BF16)
    new_swap = pltpu.roll(new_rot, 64, 1)
    own_rot = jnp.where(lane8 < HEAD_ROT, per_row(new_rot) * cos8 + per_row(new_swap) * sin8, 0.0)

    size_bg, size_h = nbytes(bgs) // 2, nbytes(hc) // zy
    beside = [r if 2 * r <= zy else r - zy for r in range(1, zy)]
    far = ((y_to - y) & (nt - 1)) == nt // 2

    def forward_rows(when):
        for here in (True, False):

            @pl.when(when & ((y_to == y) if here else (y_to != y)))
            def _():
                take_bytes((nt - 1) * size_bg if here else nt * size_bg + size_h, rsem.at[1])

        @pl.when(when)
        def _():
            for r in sorted(beside, key=lambda r: -abs(r)):
                dev = {"z": (z + r + nz) & (nz - 1)}
                send(hc.at[ring], hc.at[ring], 17, dev)
                send(aoc.at[ring], aoc.at[ring], 15, dev)

    def forward_shared(when):
        for here in (True, False):

            @pl.when(when & ((y_to == y) if here else (y_to != y)))
            def _():
                take_bytes((nt - 1 if here else nt) * size_bg, rsem.at[slot[6]])

        @pl.when(when)
        def _():
            for r in sorted(beside, key=lambda r: -abs(r)):
                send(sgc.at[ring], sgc.at[ring], 16, {"z": (z + r + nz) & (nz - 1)})

    forward_rows(jnp.logical_not(far))
    arrived(yb, nt - 1, 5)
    raw = jnp.concatenate([yb[i] for i in range(nt)], axis=1)
    new_latent = (
        raw * lax.rsqrt(jnp.mean(raw * raw, axis=1, keepdims=True) + EPSILON) * lgain[...]
    ).astype(BF16)
    o_latent[...] = new_latent
    lat8 = per_row(new_latent.astype(F32))
    own_score = score_scale * (
        jnp.sum(absorbed.astype(F32) * lat8, axis=1, keepdims=True)
        + jnp.sum(q_rot * own_rot, axis=1, keepdims=True)
    )
    top_score = jnp.maximum(best, own_score)
    rescale = jnp.exp(best - top_score)
    own_weight = jnp.exp(own_score - top_score)
    denominator = rescale * cache_total + own_weight
    context = (rescale / denominator) * ctx + rounded(own_weight / denominator) * lat8
    ho = dot(context.astype(BF16), valup[...])
    r_h = iota((nrows, HV), 0)
    ho = jnp.where((iota((nrows, HV), 1) >> log2(HEAD_VAL)) == (r_h & (LOCAL_HEADS - 1)), ho, 0.0)
    h0 = jnp.sum(jnp.where(r_h < LOCAL_HEADS, ho, 0.0), axis=0, keepdims=True)
    h1 = jnp.sum(jnp.where(r_h < LOCAL_HEADS, 0.0, ho), axis=0, keepdims=True)
    heads = rounded(jnp.where(iota((SEQS, HV), 0) == 0, h0, h1))
    ha[pl.ds(place_of, 1)] = heads.astype(BF16).reshape(1, SEQS, HV)
    for dev in plane_peers:
        send(ha.at[place_of], ha.at[place_of], 7, dev)
    sent(ha, npl - 1)

    forward_rows(far)
    for buf in (hc, aoc, sgc):
        sent(buf, zy - 1)

    rs = scores[...]
    rw = ROUTED_SCALE * rs / jnp.sum(rs, axis=0, keepdims=True)
    idv = ids[...]
    nex = nz + ncol
    which = iota((nex, batch), 0)
    target = jnp.where(which < nz, which * ncol + col, z * ncol + which - nz)
    hit = jnp.zeros((nex, batch), F32)
    wgt = jnp.zeros((nex, batch), F32)
    for k in range(4):
        same = idv[k : k + 1, :] == target
        hit = jnp.where(same, 1.0, hit)
        wgt = jnp.where(same, rw[k : k + 1, :], wgt)
    before = ones_where(iota((batch, batch), 0) < iota((batch, batch), 1))
    rank = dot(hit.astype(BF16), before)
    val = jnp.where(hit > 0.0, rank, -1.0).astype(BF16)
    pslot = ncol * SLOTS

    def pick(upper, shape, token_axis):
        t, p = iota(shape, token_axis), iota(shape, 1 - token_axis)
        return ones_where((t >> log2(th)) == 2 * (p >> log2(th)) + upper, jnp.int32) * ones_where(
            (t & (th - 1)) == (p & (th - 1)), jnp.int32
        )

    expand_p = ones_where(iota((pslot, nex), 1) == nz + (iota((pslot, nex), 0) >> log2(SLOTS)))
    slot_p = (iota((pslot, nz * th), 0) & (SLOTS - 1)).astype(F32)
    for i in range(2):
        part = dot(val, pick(i, (batch, nz * th), 0).astype(F32).astype(BF16)).astype(BF16)
        sel_p[i] = ones_where(dot(expand_p, part) == slot_p)

    gain_rows = jnp.broadcast_to(fgain[...][:, None, :], (nz, ncol, pf)).reshape(nz * ncol, pf)
    gr = iota((nz * ncol, pf), 0)
    gain_rows = jnp.where((iota((nz * ncol, pf), 1) >> log2(FEATS)) == (gr & (ncol - 1)), gain_rows, 0.0)
    tile_f = jnp.where(
        (iota((pf, 2 * cf), 0) & (FEATS - 1)) == (iota((pf, 2 * cf), 1) & (FEATS - 1)), 1.0, 0.0
    )
    tiled = dot(gain_rows, tile_f, NN, HIGHEST).reshape(nz, ncol, 2 * cf)
    lane_z = iota((ncol, 2 * cf), 1) >> log2(FEATS)
    for k in range(nt // 2):
        g = jnp.zeros((ncol, 2 * cf), F32)
        for i in range(2 * zy):
            g = jnp.where(lane_z == i, tiled[2 * zy * k + i], g)
        gp[k] = g

    forward_shared(jnp.logical_not(far))
    if beside:
        take_bytes((zy - 1) * (nbytes(hc) + nbytes(aoc)) // zy, rsem.at[slot[15]])
    t_i, l_i = iota((tok, batch), 0), iota((tok, batch), 1)
    sel_h = ones_where(l_i == z * tok + t_i)
    hcv = hc[...].reshape(cf, batch)
    hid_c = dot(sel_h, jnp.concatenate([hcv, hcv], axis=0), NT)
    arrived(ha, npl - 1, 7)
    for i in range(ncol):
        for j in range(nt):
            h16[pl.ds(SEQS * i, SEQS), pl.ds(HV * j, HV)] = ha[i * nt + j].astype(F32)
    attn = jnp.zeros((tok, 2 * cf), F32)
    for j in range(nt):
        w = jnp.concatenate([aoc[i, j] for i in range(zy)] * 2, axis=0)
        attn = attn + dot(h16[:, pl.ds(HV * j, HV)].astype(BF16), w, NT)
    mid = rounded(hid_c + rounded(attn))
    low8 = iota((th, 2 * cf), 1) < cf
    mz[pl.ds(z, 1)] = jnp.where(low8, mid[:th], mid[th:]).astype(BF16).reshape(1, th, 2 * cf)
    for p in z_peers:
        send(mz.at[z], mz.at[z], 8, {"z": p})
    sent(mz, nz - 1)

    forward_shared(far)

    mine = (iota((tok, 2 * cf), 1) >> log2(cf)) == (y & 1)
    mid = jnp.where(mine, mid, 0.0)
    ffn = (mid * gp[pl.ds(y >> 1, 1), pl.ds(col, 1)].reshape(1, 2 * cf)).astype(BF16)
    square = jnp.broadcast_to(jnp.sum(mid * mid, axis=1, keepdims=True), (tok, 128))
    take_bytes((zy - 1) * nbytes(sgc) // zy + (ncol - 1) * nbytes(so) // ncol, rsem.at[slot[16]])
    for j in range(nt):
        w = jnp.concatenate([sgc[i, j] for i in range(zy)] * 2, axis=0)
        sp[:, pl.ds(0, 2 * HIDDEN)] = dot(ffn, w)
        sp[:, pl.ds(2 * HIDDEN, 128)] = square
        for i in range(ncol):
            sh_s[i * nt + j] = sp[pl.ds(SEQS * i, SEQS), :]
    for dev in plane_peers:
        send(sh_s.at[(dev["x"] * nc + dev["c"]) * nt + dev["y"]], sh_r.at[place_of], 9, dev)
    sent(sh_s, npl - 1)
    sh_r[pl.ds(place_of, 1)] = sh_s[pl.ds(place_of, 1)]

    expand = ones_where(iota((nslot, nex), 1) == (iota((nslot, nex), 0) >> log2(SLOTS)))
    slot_i = (iota((nslot, batch), 0) & (SLOTS - 1)).astype(F32)
    in_slot = dot(expand, val) == slot_i
    w_hi = wgt.astype(BF16)
    w_lo = (wgt - w_hi.astype(F32)).astype(BF16)
    wt[pl.ds(0, nslot), :] = jnp.where(in_slot, dot(expand, w_hi), 0.0).astype(BF16)
    wt[pl.ds(nslot, nslot), :] = jnp.where(in_slot, dot(expand, w_lo), 0.0).astype(BF16)
    arrived(mz, nz - 1, 8)
    mid_all = mz[...].reshape(nz * th, 2 * cf)
    group = nc * SLOTS
    low = iota((group, 2 * cf), 1) < cf
    for dx in sorted(range(nx), key=lambda d: -min(d, nx - d)):
        chip_x = (x + dx) & (nx - 1)
        mine_of = pl.ds(pl.multiple_of(chip_x * group, group), group)
        tk = jnp.where(low, dot(sel_p[0, mine_of, :], mid_all), dot(sel_p[1, mine_of, :], mid_all))
        tk = (tk + pltpu.roll(tk, cf, 1)).reshape(nc, 2, sh, 2 * cf)
        tk = jnp.where(iota((nc, sh, 2 * cf), 2) < cf, tk[:, 0], tk[:, 1]).astype(BF16)
        tk_s[pl.ds(chip_x * nc, nc)] = tk
        for (ex, _, _), dev in zip(plane_order, plane_peers):
            if ex == dx:
                send(tk_s.at[chip_x * nc + dev["c"]], tk_r.at[place_of], 10, dev)
    sent(tk_r, npl - 1)
    tk_r[pl.ds(place_of, 1)] = tk_s[pl.ds(col, 1)]
    f_i, l_i = iota((pf, 2 * cf), 0), iota((pf, 2 * cf), 1)
    own_f = ((f_i >> log2(FEATS)) == col) & (y_to == y)
    own_l = ring * FEATS + (f_i & (FEATS - 1))
    tot0[...] = jnp.zeros((pf, batch), F32)
    for i in range(2):
        part = dot(ones_where(own_f & (l_i == own_l + cf * i)), mid_all, NT).astype(BF16)
        tot0[...] += dot(part, pick(i, (nz * th, batch), 1).astype(F32).astype(BF16))

    arrived(sh_r, npl - 1, 9)
    tot = sh_r[0]
    for i in range(1, npl):
        tot = tot + sh_r[i]
    scale = lax.rsqrt(tot[:, 2 * HIDDEN : 2 * HIDDEN + 1] / width + EPSILON)
    gate = scale * tot[:, :HIDDEN]
    act = rounded(gate / (1.0 + jnp.exp(-gate)) * (scale * tot[:, HIDDEN : 2 * HIDDEN]))
    zs[pl.ds(z, 1)] = act.reshape(1, SEQS, HIDDEN)
    for p in z_peers:
        send(zs.at[z], zs.at[z], 11, {"z": p})
    sent(zs, nz - 1)

    done(l_exp)
    arrived(tk_r, npl - 1, 10)
    pieces = []
    low_s = iota((sh, 2 * cf), 1) < cf
    sq = jnp.zeros((SLOTS, 2 * cf), F32)
    for i in range(ncol):
        for k in range(nt // 2):
            va = tk_r[i * nt + 2 * k].astype(F32)
            vb = tk_r[i * nt + 2 * k + 1].astype(F32)
            v = jnp.concatenate(
                [jnp.where(low_s, va, pltpu.roll(vb, cf, 1)), jnp.where(low_s, pltpu.roll(va, cf, 1), vb)], axis=0
            )
            sq = sq + v * v
            pieces.append((v * gp[k, pl.ds(i, 1), :]).astype(BF16))
    gu = dot(jnp.concatenate(pieces, axis=1), wgu[...].reshape(width, 2 * HIDDEN))
    scale = lax.rsqrt(jnp.sum(sq, axis=1, keepdims=True) / width + EPSILON)
    gate = scale * gu[:, :HIDDEN]
    act = (gate / (1.0 + jnp.exp(-gate)) * (scale * gu[:, HIDDEN:])).astype(BF16)
    for p in z_peers + [z]:
        zh_s[pl.ds(p, 1)] = dot(act, wd[:, pl.ds(pl.multiple_of(p * pf, pf), pf)]).astype(BF16).reshape(1, SLOTS, pf)
        if p is not z:
            send(zh_s.at[p], zh_r.at[z], 12, {"z": p})
    sent(zh_s, nz - 1)
    zh_r[pl.ds(z, 1)] = zh_s[pl.ds(z, 1)]

    arrived(zs, nz - 1, 11)
    for i in range(nz):
        s32[pl.ds(SEQS * i, SEQS), :] = zs[i]
    b_i, r_i = iota((batch, rows), 0), iota((batch, rows), 1)
    place = ones_where(b_i == (r_i >> 1) * tok + col * SEQS + (r_i & 1))
    spread_act = dot(place, s32[...].astype(BF16)).astype(BF16)
    tot0[...] += dot(so[...].reshape(pf, HIDDEN), spread_act, NT)
    arrived(zh_r, nz - 1, 12)
    parts = zh_r[...].reshape(nslot, pf)
    flat = (ncol * FEATS // 2, hl)
    low_lane = iota((ncol, FEATS // 2, hl), 2) < ob
    far_first = sorted(
        [(dx, dc) for dx in range(nx) for dc in range(nc)], key=lambda t: -(2 * min(t[0], nx - t[0]) + t[1])
    )
    for near in range(2):
        side = (y >> 1) if near else 1 - (y >> 1)
        lanes = pl.ds(pl.multiple_of(side * hl, hl), hl)
        total = tot0[:, lanes] + dot(parts, wt[pl.ds(0, nslot), lanes], TN) + dot(parts, wt[pl.ds(nslot, nslot), lanes], TN)
        total = total.reshape(ncol, 2, FEATS // 2, hl)
        ta, tb = total[:, 0], total[:, 1]
        ra = pltpu.roll(ta.reshape(flat), ob, 1).reshape(ta.shape)
        rb = pltpu.roll(tb.reshape(flat), ob, 1).reshape(tb.shape)
        pd_s[:, pl.ds(2 * side, 1)] = jnp.where(low_lane, ta, rb).reshape(ncol, 1, FEATS // 2, hl)
        pd_s[:, pl.ds(2 * side + 1, 1)] = jnp.where(low_lane, ra, tb).reshape(ncol, 1, FEATS // 2, hl)
        for dx, dc in far_first:
            px, pc = (x + dx) & (nx - 1), (c + dc) & (nc - 1)
            for e in range(2):
                dev = {"x": px, "c": pc, "y": 2 * side + e}

                def out():
                    send(pd_s.at[px * nc + pc, 2 * side + e], pd_r.at[place_of], 13, dev)

                if dx or dc or not near:
                    out()
                else:
                    pl.when((y & 1) != e)(out)
    sent(pd_r, npl - 1)
    pd_r[pl.ds(place_of, 1)] = pd_s[pl.ds(col, 1), pl.ds(y, 1)].reshape(1, FEATS // 2, hl)
    arrived(pd_r, npl - 1, 13)
    tot = pd_r[0]
    for i in range(1, npl):
        tot = tot + pd_r[i]
    both = jnp.concatenate([tot, pltpu.roll(tot, ob, 1)], axis=0)
    o_mixed[...] = both[:, :ob].astype(BF16)

    for core in range(nc):
        for here in (True, False):

            @pl.when((c == core) & ((y_to == y) if here else (y_to != y)))
            def _():
                mine = (nc * nz - 1) * (size_b if core else size_a)
                mine += (nt - 1) * (2 * size_bg + size_h) if here else nt * 2 * size_bg
                take_bytes(sum(pending) + mine, ssem.at[0])


def finish(*refs):
    copies = [pltpu.make_async_copy(refs[i], refs[3 + i], refs[6].at[i]) for i in range(3)]
    for cp in copies:
        cp.start()
    for cp in copies:
        cp.wait()


def body(nz, nx, nc, nt, *args):
    args = list(args)
    ncol = nx * nc
    pf = FEATS * ncol
    rows = SEQS * nz
    batch = rows * ncol
    lq = LATENT // nt
    nslot = nz * SLOTS
    hl = 2 * (batch // nt)
    wa = 2 * 128
    for i in (1, 12):
        args[i] = args[i].reshape(nz, pf)
    args[5] = args[5].reshape(1, LATENT)
    args[13], args[14] = args[13].T, args[14].T
    for i in (15, 16):
        args[i] = args[i].reshape(nz, ncol, FEATS, HIDDEN)
    half = HEAD_ROT // 2
    frequency = THETA_BASE ** (-np.arange(half, dtype=np.float64) / half)
    angles = frequency.astype(np.float32)[:, None] * np.arange(CACHE, dtype=np.float32)[None, :]
    trig = jnp.asarray(np.stack([np.cos(angles.astype(np.float64)), np.sin(angles.astype(np.float64))]).astype(np.float32))
    freq = jnp.asarray(np.tile(frequency.astype(np.float32), (2, 128 // half)))
    vm = pltpu.VMEM
    tok = ncol * SEQS
    cf = FEATS * nz // nt
    npl = ncol * nt
    scratch = [
        vm((nc, FEATS, wa), BF16), vm((ncol, FEATS, wa), BF16),
        vm((FEATS, batch), BF16), vm((nx, FEATS, max(128, nc * rows)), BF16), vm((ncol, FEATS, max(128, nc * rows)), BF16),
        vm((ncol, FEATS, HIDDEN), BF16),
        vm((FEATS, 2 * HV), BF16),
        vm((nz // nt, nt, FEATS, HV), BF16), vm((nz // nt, nt, FEATS, HV), BF16),
        vm((nz // nt, FEATS, batch), BF16),
        vm((128, pf), BF16),
        vm((nz, pf), F32), vm((nz, pf), F32), vm((1, LATENT), F32), vm((2, 128), F32),
        vm((LATENT, LOCAL_HEADS * HEAD_KEY), BF16), vm((LATENT, HV), BF16),
        vm((SEQS, CACHE, LATENT), BF16), vm((SEQS, HEAD_ROT, CACHE), BF16),
        pltpu.SMEM((SEQS,), jnp.int32),
        vm((4, batch), jnp.int32), vm((4, batch), F32),
        vm((ncol, nz, FEATS, 2 * HIDDEN), BF16), vm((HIDDEN, pf * nz), BF16),
        vm((2, half, CACHE), F32),
        vm((nc * nz, SEQS, wa + 128), F32), vm((nz, SEQS, wa + 128), F32), vm((nz, SEQS, wa), F32),
        vm((nt, SEQS, lq), F32),
        vm((npl, SEQS, HV), BF16),
        vm((nz, tok // 2, 2 * cf), BF16),
        vm((npl, SEQS, 2 * HIDDEN + 128), F32), vm((npl, SEQS, 2 * HIDDEN + 128), F32),
        vm((ncol, SLOTS // 2, 2 * cf), BF16), vm((npl, SLOTS // 2, 2 * cf), BF16),
        vm((nz, SLOTS, pf), BF16), vm((nz, SLOTS, pf), BF16),
        vm((nz, SEQS, HIDDEN), F32),
        vm((ncol, nt, FEATS // 2, hl), F32), vm((npl, FEATS // 2, hl), F32),
        vm((LATENT + 256, QW), BF16),
        vm((SEQS, HEAD_ROT, CACHE), F32),
        vm((2, ncol * SLOTS, batch // 2), BF16),
        vm((2 * nslot, batch), BF16),
        vm((tok, nt * HV), F32),
        vm((rows, HIDDEN), F32),
        vm((nc * rows, wa + 128), F32),
        vm((tok, 2 * HIDDEN + 128), F32),
        vm((nt // 2, ncol, 2 * cf), F32),
        vm((pf, batch), F32),
        pltpu.SemaphoreType.DMA((6,)),
        pltpu.SemaphoreType.DMA((1,)),
        pltpu.SemaphoreType.DMA((14,)),
        pltpu.SemaphoreType.REGULAR((3,)),
        vm((2560 * 1024 // UNIT, 2, UNIT // 8), F32),
    ]
    anywhere = pl.BlockSpec(memory_space=pltpu.HBM)
    results = pl.pallas_call(
        functools.partial(kernel, nz, nx, nc, nt),
        out_shape=(
            pltpu.VMEM((FEATS, hl // 2), BF16),
            pltpu.VMEM((SEQS, LATENT), BF16),
            pltpu.VMEM((SEQS, HEAD_ROT), BF16),
        ),
        in_specs=[anywhere] * 23,
        out_specs=(pl.BlockSpec(memory_space=pltpu.VMEM),) * 3,
        scratch_shapes=scratch,
        compiler_params=pltpu.CompilerParams(collective_id=0, has_side_effects=True, vmem_limit_bytes=66977792),
        name="layer",
    )(*args, trig, freq)
    results = [pltpu.with_memory_space_constraint(r, pltpu.VMEM) for r in results]
    return pl.pallas_call(
        finish,
        out_shape=(
            jax.ShapeDtypeStruct((FEATS, hl // 2), BF16),
            jax.ShapeDtypeStruct((SEQS, LATENT), BF16),
            jax.ShapeDtypeStruct((SEQS, HEAD_ROT), BF16),
        ),
        in_specs=[pl.BlockSpec(memory_space=pltpu.VMEM)] * 3,
        out_specs=(anywhere,) * 3,
        scratch_shapes=[pltpu.SemaphoreType.DMA((3,))],
        name="finish",
    )(*results)


EP = ("z", "x", "c")


def build(devices):
    split = Mesh(devices, ("z", "x", "c", "y"))
    return jax.shard_map(
        functools.partial(body, *devices.shape),
        mesh=split,
        in_specs=(
            P(EP, None),
            P(),
            P(EP, "y"),
            P(EP, None),
            P(),
            P(),
            P(None, "y"),
            P(None, "y"),
            P(EP, None),
            P(EP, None, None),
            P(EP, None, None),
            P(EP),
            P(),
            P(),
            P(),
            P(EP, None, "y"),
            P(EP, None, "y"),
            P(EP, "y", None),
            P(EP, "y"),
            P(EP, "y"),
            P(EP, "y"),
        ),
        out_specs=(P(EP, "y"), P(EP, None), P(EP, None)),
        check_vma=False,
    )


def solution(mesh):
    return build(mesh.devices.reshape(16, 4, 2, mesh.shape["tp"]))
```
